512 devices in a mesh: sp: 32 (over z, core), tp: 16 (over y, x).
Axes of the slice: x: 4, y: 4, z: 16, core: 2. Of those that a mesh axis runs over, the one named last changes fastest.
Arguments:
- layer_input: bfloat16 [32768, 4096], P('sp', 'tp'), may hold values from -6 to 6
- key_weight: bfloat16 [4096, 4096], P(None, 'tp'), may hold values from -0.09375 to 0.09375
- value_weight: bfloat16 [4096, 4096], P(None, 'tp'), may hold values from -0.09375 to 0.09375
- decay_exponent: float32 [32], P('tp'), may hold values from -0.077 to -4.2114258e-05, as said below
- query_new: bfloat16 [2, 4096], P(None, 'tp'), may hold values from -6 to 6
- key_new: bfloat16 [2, 4096], P(None, 'tp'), may hold values from -6 to 6
- value_new: bfloat16 [2, 4096], P(None, 'tp'), may hold values from -6 to 6
- norm_gain: float32 [4096], P('tp'), may hold values from 0.1 to 1.9
Outputs:
- state_cache: bfloat16 [2, 32, 128, 128], P(None, 'tp', 'sp')
- first_read: bfloat16 [2, 4096], P(None, 'tp')
The draws below stay inside these ranges and needn't reach their ends.
Inputs may be any that keep to these rules, and one draw needn't show every extreme that they name: decay_exponent is negative.
All inputs are finite; a program needn't handle non-finite values.
Results may differ from the reference program's by a relative error of at most 0.011.
Values may be sent and summed in bfloat16 or wider, within the bound.
A program may use at most 64 MiB of HBM per device.

```python
import jax
import jax.numpy as jnp
from jax import lax

D = 4096
HEADS = 32
DK = 128
DV = 128
SEQS = 2
TOKENS = 32768
LEN = 16384


def draw_decay_exponent(key, part):
    first_key = jax.random.fold_in(key, 11)
    second_key = jax.random.fold_in(key, 12)
    third_key = jax.random.fold_in(key, 13)
    slow_share = 0.5
    slow_flag = jax.random.uniform(first_key, (HEADS,), jnp.float32) < slow_share
    fast_rate = jax.random.uniform(second_key, (HEADS,), jnp.float32, 2.3026 / 100.0, 2.3026 / 30.0)
    slow_rate = jax.random.uniform(third_key, (HEADS,), jnp.float32, 0.3, 1.0) * (2.3026 / LEN)
    return -jnp.where(slow_flag, slow_rate, fast_rate)


def levels(rng, dims, shards, least, largest):
    def one(dim, parts):
        draws = jax.random.uniform(jax.random.fold_in(jax.random.fold_in(rng, 6), dim), (parts,), jnp.float32, least / len(shards), largest / len(shards))
        return jnp.repeat(jnp.exp(draws), dims[dim] // parts).reshape((-1,) + (1,) * (len(dims) - dim - 1))

    gain = one(*shards[0])
    for cut in shards[1:]:
        gain = gain * one(*cut)
    return gain


def bell_draw(stream_key, extent, spread, most, split=(), kind=jnp.bfloat16):
    result = spread * jax.random.normal(stream_key, extent, jnp.float32)
    if split:
        result = result * levels(stream_key, extent, split, -0.22, 0.18)
    return jnp.clip(result, -most, most).astype(kind)


def setup_inputs(seed: int = 0) -> dict:
    key_of = jax.random.split(jax.random.key(seed), 9)
    return {
        "layer_input": bell_draw(key_of[0], (TOKENS, D), 1.0, 6.0, ((0, 32), (1, 16))),
        "key_weight": bell_draw(key_of[1], (D, HEADS * DK), D ** -0.5, 0.09375, ((1, 16),)),
        "value_weight": bell_draw(key_of[2], (D, HEADS * DV), D ** -0.5, 0.09375, ((1, 16),)),
        "decay_exponent": draw_decay_exponent(jax.random.fold_in(key_of[8], 71), 0),
        "query_new": bell_draw(key_of[4], (SEQS, HEADS * DK), 1.0, 6.0, ((1, 16),)),
        "key_new": bell_draw(key_of[5], (SEQS, HEADS * DK), 1.0, 6.0, ((1, 16),)),
        "value_new": bell_draw(key_of[6], (SEQS, HEADS * DV), 1.0, 6.0, ((1, 16),)),
        "norm_gain": jnp.clip(1.0 + 0.18 * jax.random.normal(key_of[7], (HEADS * DV,), jnp.float32), 0.1, 1.9),
    }


def rotate(projected, position):
    half_width = projected.shape[-1] // 2
    inverse = 1.0 / 10000.0 ** jnp.linspace(0.0, 1.0, half_width, dtype=jnp.float32)
    angle = position[:, None] * inverse[None, :]
    cosine = jnp.cos(angle)[:, None, :]
    sine = jnp.sin(angle)[:, None, :]
    first = projected[..., :half_width]
    second = projected[..., half_width:]
    return jnp.concatenate([first * cosine - second * sine, first * sine + second * cosine], axis=-1)

def reference(layer_input, key_weight, value_weight, decay_exponent, query_new, key_new, value_new, norm_gain):
    key_proj = jnp.dot(layer_input, key_weight, preferred_element_type=jnp.float32)
    value_proj = jnp.dot(layer_input, value_weight, preferred_element_type=jnp.float32)
    position = (jnp.arange(TOKENS, dtype=jnp.int32) % LEN).astype(jnp.float32)
    keys = (rotate(key_proj.reshape(TOKENS, HEADS, DK), position) * DK ** (-0.5)).astype(jnp.bfloat16)
    values = value_proj.astype(jnp.bfloat16).reshape(TOKENS, HEADS, DV)
    distance = LEN - 1.0 - position
    weighting = jnp.exp(decay_exponent[None, :] * distance[:, None])
    weighted = (keys.astype(jnp.float32) * weighting[:, :, None]).astype(jnp.bfloat16)
    final = jnp.einsum('slhd,slhe->shde', weighted.astype(jnp.float32).reshape(SEQS, LEN, HEADS, DK), values.astype(jnp.float32).reshape(SEQS, LEN, HEADS, DV), precision=lax.Precision.HIGHEST)
    state_cache = final.astype(jnp.bfloat16)
    queries = query_new.astype(jnp.float32).reshape(SEQS, HEADS, DK)
    keys_next = key_new.astype(jnp.float32).reshape(SEQS, HEADS, DK)
    values_next = value_new.astype(jnp.float32).reshape(SEQS, HEADS, DV)
    carried = jnp.einsum('shd,shde->she', queries, final, precision=lax.Precision.HIGHEST)
    own_term = lax.optimization_barrier(jnp.sum(queries * keys_next, axis=2))[:, :, None] * values_next
    mixed = jnp.exp(decay_exponent)[None, :, None] * carried + own_term
    normed = mixed * lax.rsqrt(lax.optimization_barrier(jnp.mean(mixed * mixed, axis=2, keepdims=True)) + 1e-06)
    normed = normed * norm_gain.reshape(HEADS, DV)[None, :, :]
    return (state_cache, normed.reshape(SEQS, HEADS * DV).astype(jnp.bfloat16))
```

```python
import jax
import jax.numpy as jnp
from jax import lax
from jax.experimental import pallas as pl
from jax.experimental.pallas import tpu as pltpu
from jax.sharding import PartitionSpec as P

MESH = pl.DeviceIdType.MESH
N = 4
TOK = 1024
FEAT = 256
PIECE = TOK // N
SP = 32
Z = 16

ORDER = [
    (0, 0), (1, 0), (2, 0), (3, 0),
    (1, 1), (2, 1), (2, 2), (3, 1), (3, 2), (3, 4),
    (2, 3), (3, 3), (3, 5), (3, 6),
    (3, 7),
]


def turn(mask, j):
    return ((mask << j) | (mask >> (N - j))) & (2**N - 1)


def select(d, values):
    total = 0
    for i, value in enumerate(values):
        if value:
            total = total + jnp.where(d == i, value, 0)
    return total


def flip1(v):
    return v + 1 - 2 * (v % 2)


def cos_sin(position, inverse):
    angle = position * inverse
    lane = lax.broadcasted_iota(jnp.int32, angle.shape, 1)
    quarter = jnp.floor(angle * 0.6366197723675814 + 0.5)
    rest = ((angle - quarter * 1.5703125) - quarter * 4.837512969970703125e-4) - quarter * 7.54978995489188e-8
    turns = quarter.astype(jnp.int32) - jnp.where(lane >= 64, 1, 0)
    turns = jnp.bitwise_and(turns, 3)
    square = rest * rest
    sine = rest + rest * square * (-1.6666654611e-1 + square * (8.3321608736e-3 - square * 1.9515295891e-4))
    cosine = 1.0 - 0.5 * square + square * square * (
        4.166664568298827e-2 + square * (-1.388731625493765e-3 + square * 2.443315711809948e-5)
    )
    value = jnp.where(jnp.bitwise_and(turns, 1) == 1, sine, cosine)
    negative = jnp.logical_or(turns == 1, turns == 2)
    return jnp.where(negative, -value, value)


def kernel(
    decay, x_hbm, wk_hbm, wv_hbm, query, key_new, value_new, gain, inverse,
    state_out, read_out,
    xbuf, wk, wv, acc, cosine, sine, weight, send_state, send_read, got_state, got_read,
    own_sem, w_sem, recv_sem, send_sem, tail_send, tail_send2, tail_recv, tail_recv2, self_sem, chain,
):
    sp = lax.axis_index("sp")
    tp = lax.axis_index("tp")
    z, core = sp // 2, sp % 2
    y, x = tp // 4, tp % 4
    links = [
        (sp, y * 4 + flip1(x)),
        (sp, y * 4 + 3 - x),
        (sp, flip1(y) * 4 + x),
        (sp, (3 - y) * 4 + x),
    ]
    sibling = (z * 2 + 1 - core, tp)

    def along_z(step):
        return ((z + step + Z) % Z * 2 + core, tp)

    def signal(semaphore, device):
        pl.semaphore_signal(semaphore, inc=1, device_id=device, device_id_type=MESH)

    own = [
        pltpu.make_async_copy(
            x_hbm.at[pl.ds(j * PIECE, PIECE)], xbuf.at[0, pl.ds(j * PIECE, PIECE)], own_sem.at[j]
        )
        for j in range(N)
    ]
    for copy in own:
        copy.start()
    wcopies = [
        pltpu.make_async_copy(wk_hbm, wk, w_sem.at[0]),
        pltpu.make_async_copy(wv_hbm, wv, w_sem.at[1]),
    ]
    for copy in wcopies:
        copy.start()

    barrier = pltpu.get_barrier_semaphore()
    near = links + [sibling, along_z(1), along_z(-1)]
    for device in near:
        signal(barrier, device)
    pl.semaphore_wait(barrier, len(near))

    def message(d, k, r):
        j = (d - k) % N
        m = turn(r, j)
        rows = pl.ds(j * PIECE, PIECE)
        arrives = m | (1 << d)
        return pltpu.make_async_remote_copy(
            src_ref=xbuf.at[m, rows],
            dst_ref=xbuf.at[arrives, rows],
            send_sem=send_sem,
            recv_sem=recv_sem.at[arrives, j],
            device_id=links[d],
            device_id_type=MESH,
        )

    for copy in own:
        copy.wait()
    for k, r in ORDER[:N]:
        for d in range(N):
            message(d, k, r).start()

    for j in range(N):
        rows = pl.ds(j * PIECE, PIECE)
        first = (sp % 16) * TOK + j * PIECE
        position = (
            lax.broadcasted_iota(jnp.int32, (PIECE, 128), 0) + first
        ).astype(jnp.float32)
        table = cos_sin(position, inverse[...])
        swapped = pltpu.roll(table, 64, axis=1)
        low = lax.broadcasted_iota(jnp.int32, (PIECE, 128), 1) < 64
        cosine[rows, :] = jnp.where(low, table, swapped)
        sine[rows, :] = jnp.where(low, -swapped, table)
        distance = 16384 - 1.0 - position
        for h in range(2):
            weight[h, rows, :] = jnp.exp(decay[h] * distance)

    for copy in wcopies:
        copy.wait()

    def column_of(m):
        b = [m // 2**i % 2 for i in range(N)]
        cx = x + b[0] * (1 - 2 * (x % 2))
        cx = cx + b[1] * (3 - 2 * cx)
        cy = y + b[2] * (1 - 2 * (y % 2))
        cy = cy + b[3] * (3 - 2 * cy)
        return cy * 4 + cx

    def add_product(m, j, first):
        t = column_of(m)
        wrows = pl.ds(pl.multiple_of(t * FEAT, FEAT), FEAT)
        rows = pl.ds(pl.multiple_of(j * PIECE, PIECE), PIECE)
        block = xbuf[m, rows, :]
        for i, w in enumerate((wk, wv)):
            part = jnp.dot(block, w[wrows, :], preferred_element_type=jnp.float32)
            if first:
                acc[i, rows, :] = part
            else:
                acc[i, rows, :] += part

    @pl.loop(0, N)
    def _(j):
        add_product(0, j, True)

    chain_steps = {0: [sibling, along_z(1), along_z(-1)], 2: [along_z(2), along_z(-2)],
                   4: [along_z(3), along_z(-3)], 6: [along_z(6), along_z(-6)]}
    pending = None

    for slot, (k, r) in enumerate(ORDER):
        for d in range(N):
            message(d, k, r).wait_recv()
        here = [q for q, (kk, rr) in enumerate(ORDER) if q >= N and forwards_after(kk, rr) == slot]
        for q in here:
            for d in range(N):
                message(d, *ORDER[q]).start()
        if slot in chain_steps:
            if pending is not None:
                pl.semaphore_wait(chain.at[pending[0]], pending[1])
            number = sorted(chain_steps).index(slot)
            for device in chain_steps[slot]:
                signal(chain.at[number], device)
            pending = (number, len(chain_steps[slot]))
        js = [(d - k) % N for d in range(N)]
        ms = [turn(r | (1 << k), j) for j in js]

        @pl.loop(0, N)
        def _(d):
            add_product(select(d, ms), select(d, js), False)

    pl.semaphore_wait(chain.at[pending[0]], pending[1])

    scale = 128 ** (-0.5)
    states = []
    for h in range(2):
        cols = pl.ds(h * 128, 128)
        k = acc[0, :, cols]
        turned = k * cosine[...] + pltpu.roll(k, 64, axis=1) * sine[...]
        keys = (turned * scale).astype(jnp.bfloat16)
        weighted = (keys.astype(jnp.float32) * weight[h]).astype(jnp.bfloat16)
        values = acc[1, :, cols].astype(jnp.bfloat16)
        states.append(
            lax.dot_general(
                weighted, values, (((0,), (0,)), ((), ())), preferred_element_type=jnp.float32
            )
        )
    top = lax.broadcasted_iota(jnp.int32, (8, 128), 0) < 4
    for i in range(16):
        a = states[0][8 * i : 8 * i + 8]
        b = states[1][8 * i : 8 * i + 8]
        send_state[2 * i] = jnp.where(top, a, pltpu.roll(b, 4, axis=0)).astype(jnp.bfloat16)
        send_state[2 * i + 1] = jnp.where(top, pltpu.roll(a, 4, axis=0), b).astype(jnp.bfloat16)
    prompt = z // 8
    for h in range(2):
        q = query[:, h * 128 : h * 128 + 128].astype(jnp.float32)
        both = jnp.dot(q, states[h], precision=lax.Precision.HIGHEST, preferred_element_type=jnp.float32)
        send_read[h : h + 1, :] = jnp.where(prompt == 0, both[0:1], both[1:2])

    def tail(step, other):
        target = (z + step + Z) % Z * 2 + (1 - core if other else core)
        state_copy = pltpu.make_async_remote_copy(
            src_ref=send_state.at[target], dst_ref=got_state.at[sp],
            send_sem=tail_send, recv_sem=tail_recv, device_id=(target, tp), device_id_type=MESH,
        )
        read_copy = pltpu.make_async_remote_copy(
            src_ref=send_read, dst_ref=got_read.at[sp],
            send_sem=tail_send2, recv_sem=tail_recv2, device_id=(target, tp), device_id_type=MESH,
        )
        return state_copy, read_copy

    steps = [8]
    for s in range(7, 0, -1):
        steps += [s, -s]
    for step in steps:
        for other in (False, True):
            for copy in tail(step, other):
                copy.start()
    for copy in tail(0, True):
        copy.start()
    pltpu.make_async_copy(send_state.at[sp], got_state.at[sp], tail_recv).start()
    pltpu.make_async_copy(send_read, got_read.at[sp], tail_recv2).start()

    queries = query[...].astype(jnp.float32)
    dots = queries * key_new[...].astype(jnp.float32)
    news = value_new[...].astype(jnp.float32)
    own_terms = [
        jnp.sum(dots[:, h * 128 : h * 128 + 128], axis=1, keepdims=True) * news[:, h * 128 : h * 128 + 128]
        for h in range(2)
    ]

    pltpu.make_async_copy(got_read, got_read, tail_recv2).wait()
    carried = [jnp.sum(got_read[16 * s : 16 * s + 16], axis=0) for s in range(2)]
    for h in range(2):
        scaled = jnp.exp(jnp.full((1, 128), decay[h], jnp.float32))
        rows = jnp.concatenate([carried[0][h : h + 1], carried[1][h : h + 1]], axis=0)
        mixed = scaled * rows + own_terms[h]
        normed = mixed * lax.rsqrt(jnp.mean(mixed * mixed, axis=1, keepdims=True) + 1e-06)
        read_out[:, h * 128 : h * 128 + 128] = normed * gain[:, h * 128 : h * 128 + 128]
    pltpu.make_async_copy(got_state, got_state, tail_recv).wait()
    for s in range(2):
        total = jnp.zeros((8, 128), jnp.float32)
        for i in range(16):
            total = total + got_state[16 * s + i].astype(jnp.float32)
        state_out[s] = total

    blocks = pl.ds(0, 15)
    pltpu.make_async_copy(xbuf.at[blocks], xbuf.at[blocks], send_sem).wait()
    others = pl.ds(0, SP - 1)
    pltpu.make_async_copy(got_state.at[others], got_state.at[others], tail_send).wait()
    pltpu.make_async_copy(got_read.at[others], got_read.at[others], tail_send2).wait()


def forwards_after(k, r):
    top = r.bit_length() - 1
    return ORDER.index((top, r - (1 << top)))


def on_device(
    layer_input, key_weight, value_weight, decay_exponent, query_new, key_new, value_new, norm_gain
):
    inverse = 1.0 / 10000.0 ** jnp.linspace(0.0, 1.0, 64, dtype=jnp.float32)
    inverse = jnp.concatenate([inverse, inverse])[None, :]
    vmem = pl.BlockSpec(memory_space=pltpu.VMEM)
    anywhere = pl.BlockSpec(memory_space=pl.ANY)
    state, read = pl.pallas_call(
        kernel,
        name="gather_project_reduce",
        out_shape=(
            jax.ShapeDtypeStruct((2, 8, 128), jnp.float32),
            jax.ShapeDtypeStruct((2, 256), jnp.float32),
        ),
        in_specs=[
            pl.BlockSpec(memory_space=pltpu.SMEM), anywhere, anywhere, anywhere,
            vmem, vmem, vmem, vmem, vmem,
        ],
        out_specs=(vmem, vmem),
        scratch_shapes=[
            pltpu.VMEM((16, TOK, FEAT), jnp.bfloat16),
            pltpu.VMEM((4096, 256), jnp.bfloat16),
            pltpu.VMEM((4096, 256), jnp.bfloat16),
            pltpu.VMEM((2, TOK, 256), jnp.float32),
            pltpu.VMEM((TOK, 128), jnp.float32),
            pltpu.VMEM((TOK, 128), jnp.float32),
            pltpu.VMEM((2, TOK, 128), jnp.float32),
            pltpu.VMEM((SP, 8, 128), jnp.bfloat16),
            pltpu.VMEM((2, 128), jnp.float32),
            pltpu.VMEM((SP, 8, 128), jnp.bfloat16),
            pltpu.VMEM((SP, 2, 128), jnp.float32),
            pltpu.SemaphoreType.DMA((N,)),
            pltpu.SemaphoreType.DMA((2,)),
            pltpu.SemaphoreType.DMA((16, N)),
            pltpu.SemaphoreType.DMA,
            pltpu.SemaphoreType.DMA,
            pltpu.SemaphoreType.DMA,
            pltpu.SemaphoreType.DMA,
            pltpu.SemaphoreType.DMA,
            pltpu.SemaphoreType.DMA,
            pltpu.SemaphoreType.REGULAR((4,)),
        ],
        compiler_params=pltpu.CompilerParams(collective_id=0, has_side_effects=True),
    )(
        decay_exponent, layer_input, key_weight, value_weight,
        query_new, key_new, value_new, norm_gain[None, :], inverse,
    )
    return (
        state.reshape(2, 2, 4, 128).astype(jnp.bfloat16),
        read.astype(jnp.bfloat16),
    )


def solution(mesh):
    in_specs = (
        P("sp", "tp"), P(None, "tp"), P(None, "tp"), P("tp"),
        P(None, "tp"), P(None, "tp"), P(None, "tp"), P("tp"),
    )
    out_specs = (P(None, "tp", "sp", None), P(None, "tp"))
    return jax.shard_map(
        on_device, mesh=mesh, in_specs=in_specs, out_specs=out_specs, check_vma=False
    )
```

```python
import jax
import jax.numpy as jnp
import numpy as np
from jax import lax
from jax.experimental import pallas as pl
from jax.experimental.pallas import tpu as pltpu
from jax.sharding import PartitionSpec as P

MESH = pl.DeviceIdType.MESH
N = 3
TOK = 1024
FEAT = 256
STARTS = (0, 352, 688, 1024)
SP = 32
Z = 16

NATIVE_ORDER = [[(0, 0), (1, 0), (2, 0), (1, 1), (2, 1), (2, 2), (2, 3)]] * 3
FOREIGN_ORDER = [
    [(0, 0), (2, 0), (1, 0), (2, 1), (1, 1), (2, 2), (2, 3)],
    [(1, 0), (0, 0), (2, 0), (1, 1), (2, 1), (2, 2), (2, 3)],
    [(2, 0), (1, 0), (0, 0), (1, 1), (2, 1), (2, 2), (2, 3)],
]


def turn(mask, j):
    return ((mask << j) | (mask >> (N - j))) & (2**N - 1)


def piece(j):
    return pl.ds(STARTS[j], STARTS[j + 1] - STARTS[j])


def slot_messages(order, slot):
    out = []
    for d in range(N):
        k, r = order[d][slot]
        j = (d - k) % N
        out.append((d, j, turn(r, j), turn(r, j) | (1 << d)))
    return out


def onward(order, d, j, mask):
    out = []
    for dd in range(N):
        for slot in range(7):
            for link, jj, sent, _ in slot_messages(order, slot):
                if link == dd and jj == j and sent == mask:
                    out.append((slot, dd))
    return [dd for _, dd in sorted(out)]


def flip1(v):
    return v + 1 - 2 * (v % 2)


def cos_sin(position, inverse):
    angle = position * inverse
    lane = lax.broadcasted_iota(jnp.int32, angle.shape, 1)
    quarter = jnp.floor(angle * 0.6366197723675814 + 0.5)
    rest = ((angle - quarter * 1.5703125) - quarter * 4.837512969970703125e-4) - quarter * 7.54978995489188e-8
    turns = quarter.astype(jnp.int32) - jnp.where(lane >= 64, 1, 0)
    turns = jnp.bitwise_and(turns, 3)
    square = rest * rest
    sine = rest + rest * square * (-1.6666654611e-1 + square * (8.3321608736e-3 - square * 1.9515295891e-4))
    cosine = 1.0 - 0.5 * square + square * square * (
        4.166664568298827e-2 + square * (-1.388731625493765e-3 + square * 2.443315711809948e-5)
    )
    value = jnp.where(jnp.bitwise_and(turns, 1) == 1, sine, cosine)
    negative = jnp.logical_or(turns == 1, turns == 2)
    return jnp.where(negative, -value, value)


def kernel(
    decay, x_hbm, wk_hbm, wv_hbm, query, key_new, value_new, gain, inverse,
    state_out, read_out,
    xbuf, wk, wv, acc, cosine, sine, weight, mini_own, mini_got, send_state, send_read, got_state, got_read,
    mine_sem, sib_sem, w_sem, wl_sem, mini_sem,
    link_send, sib_send, x_send, w_send, wz_send, wzz_send, mini_send,
    tail_send, tail_send2, tail_recv, tail_recv2, chain,
):
    sp = lax.axis_index("sp")
    tp = lax.axis_index("tp")
    z, core = sp // 2, sp % 2
    y, x = tp // 4, tp % 4
    group = (x + 1) // 2 % 2
    block = z * 2 + group
    links = [
        (sp, y * 4 + 3 - x),
        (sp, flip1(y) * 4 + x),
        (sp, (3 - y) * 4 + x),
    ]
    sibling = (z * 2 + 1 - core, tp)
    partner_tp = y * 4 + flip1(x)
    partner = (z * 2 + 1 - core, partner_tp)

    def along_z(step):
        return ((z + step + Z) % Z * 2 + core, tp)

    def signal(semaphore, device):
        pl.semaphore_signal(semaphore, inc=1, device_id=device, device_id_type=MESH)

    def remote(src, dst, send, recv, device):
        return pltpu.make_async_remote_copy(
            src_ref=src, dst_ref=dst, send_sem=send, recv_sem=recv, device_id=device, device_id_type=MESH
        )

    def arrived(ref, semaphore):
        pltpu.make_async_copy(ref, ref, semaphore).wait()

    is_native = core == group
    is_foreign = core != group

    @pl.when(is_native)
    def _():
        for j in range(N):
            pltpu.make_async_copy(x_hbm.at[piece(j)], xbuf.at[0, 0, piece(j)], mine_sem.at[0, j]).start()
        pltpu.make_async_copy(wk_hbm, wk, wl_sem.at[0]).start()
        pltpu.make_async_copy(wv_hbm, wv, wl_sem.at[1]).start()

    for h in range(2):
        mini_own[h : h + 1, :] = jnp.full((1, 128), decay[h], jnp.float32)
        mini_own[2 + 2 * h : 4 + 2 * h, :] = query[:, h * 128 : h * 128 + 128].astype(jnp.float32)

    barrier = pltpu.get_barrier_semaphore()
    near = links + [sibling, partner, along_z(1), along_z(-1), along_z(2), along_z(-2)]
    for device in near:
        signal(barrier, device)
    pl.semaphore_wait(barrier, len(near))

    steps = [
        [sibling, partner, along_z(1), along_z(-1), along_z(2), along_z(-2)],
        [along_z(2), along_z(-2)],
        [sibling],
        [along_z(4), along_z(-4)],
    ]

    def chain_signal(n):
        for device in steps[n]:
            signal(chain.at[n], device)

    def chain_wait(n):
        pl.semaphore_wait(chain.at[n], len(steps[n]))

    def send_on(mask, j, over):
        for d in over:
            remote(
                xbuf.at[0, mask, piece(j)], xbuf.at[0, mask | (1 << d), piece(j)],
                link_send, mine_sem.at[mask | (1 << d), j], links[d],
            ).start()

    def to_sibling(mask, j):
        remote(
            xbuf.at[0, mask, piece(j)], xbuf.at[1, mask, piece(j)], sib_send, sib_sem.at[mask, j], sibling
        ).start()

    def column_of(mask, native_part):
        b = [mask // 2**i % 2 for i in range(N)]
        cx = x + b[0] * (3 - 2 * x)
        cy = y + b[1] * (1 - 2 * (y % 2))
        cy = cy + b[2] * (3 - 2 * cy)
        return cy * 4 + (cx if native_part else flip1(cx))

    def weight_rows(t):
        return pl.ds(pl.multiple_of(t * FEAT, FEAT), FEAT)

    def add_product(part, mask, j, native_part, first=False):
        wrows = weight_rows(column_of(mask, native_part))
        block_x = xbuf[part, mask, piece(j), :]
        for i, w in enumerate((wk, wv)):
            product = jnp.dot(block_x, w[wrows, :], preferred_element_type=jnp.float32)
            if first:
                acc[i, piece(j), :] = product
            else:
                acc[i, piece(j), :] += product

    def mine_arrived(mask, j):
        arrived(xbuf.at[0, mask, piece(j)], mine_sem.at[mask, j])

    def sib_arrived(mask, j):
        arrived(xbuf.at[1, mask, piece(j)], sib_sem.at[mask, j])

    def tables(mini):
        @pl.loop(0, 4)
        def _(c):
            rows = pl.ds(pl.multiple_of(c * 256, 256), 256)
            first = (block % 16) * TOK + c * 256
            position = (lax.broadcasted_iota(jnp.int32, (256, 128), 0) + first).astype(jnp.float32)
            table = cos_sin(position, inverse[...])
            swapped = pltpu.roll(table, 64, axis=1)
            low = lax.broadcasted_iota(jnp.int32, (256, 128), 1) < 64
            cosine[rows, :] = jnp.where(low, table, swapped)
            sine[rows, :] = jnp.where(low, -swapped, table)
            distance = 16384 - 1.0 - position
            for h in range(2):
                weight[h, rows, :] = jnp.exp(mini[h : h + 1, :] * distance)

    def receive_slot(order, slot):
        got = slot_messages(order, slot)
        for d, j, _, mask in got:
            mine_arrived(mask, j)
            send_on(mask, j, onward(order, d, j, mask))
            to_sibling(mask, j)
        return got

    @pl.when(is_native)
    def _():
        for j in range(N):
            mine_arrived(0, j)
        for slot in range(3):
            for d, j, mask, _ in slot_messages(NATIVE_ORDER, slot):
                send_on(mask, j, [d])
        for j in range(N):
            to_sibling(0, j)
        chain_signal(0)
        mini_got[...] = mini_own[...]
        tables(mini_own)
        arrived(wk, wl_sem.at[0])
        arrived(wv, wl_sem.at[1])
        for j in range(N):
            add_product(0, 0, j, True, first=True)
        for slot in range(7):
            got = receive_slot(NATIVE_ORDER, slot)
            if slot in (1, 3, 5):
                chain_wait(slot // 2)
                chain_signal(slot // 2 + 1)
            for _, j, _, mask in got:
                add_product(0, mask, j, True)
        for j in range(N):
            sib_arrived(0, j)
            add_product(1, 0, j, False)
        for slot in range(7):
            for _, j, _, mask in slot_messages(FOREIGN_ORDER, slot):
                sib_arrived(mask, j)
                add_product(1, mask, j, False)
        chain_wait(3)

    @pl.when(is_foreign)
    def _():
        quarter = z % 4
        opposite = (z + 2) % 4
        kv = ((wk_hbm, wk), (wv_hbm, wv))

        def direct(t):
            rows = weight_rows(t)
            for i, (src, dst) in enumerate(kv):
                remote(src.at[rows], dst.at[rows], w_send, w_sem.at[t, i], partner).start()

        def pass_weights(t, i, step, semaphore):
            ref = kv[i][1]
            rows = weight_rows(t)
            remote(ref.at[rows], ref.at[rows], semaphore, w_sem.at[t, i], along_z(step)).start()

        def exchange(j):
            remote(x_hbm.at[piece(j)], xbuf.at[0, 0, piece(j)], x_send, mine_sem.at[0, j], partner).start()

        def own_piece(j):
            mine_arrived(0, j)
            send_on(0, j, onward(FOREIGN_ORDER, 0, j, 0))
            to_sibling(0, j)

        def weights_arrived(t):
            for i, (_, ref) in enumerate(kv):
                arrived(ref.at[weight_rows(t)], w_sem.at[t, i])

        def own_weights(c):
            t = quarter * 4 + c
            weights_arrived(t)
            for i in range(2):
                pass_weights(t, i, 1, wz_send)
                pass_weights(t, i, -1, wz_send)
            if c == 0:
                pass_weights(t, 0, 2, wzz_send)
                pass_weights(t, 1, 2, wzz_send)
            if c == 1:
                pass_weights(t, 0, -2, wzz_send)
                pass_weights(t, 1, -2, wzz_send)
            if c == 3:
                pass_weights(t, 0, 2, wzz_send)
                pass_weights(t, 1, -2, wzz_send)

        def quarter_product(row, first=False):
            m1 = jnp.where(row == flip1(y), 2, 0)
            m2 = jnp.where(row == 3 - y, 4, 0)
            m3 = jnp.where(row == 3 - flip1(y), 6, 0)
            base = m1 + m2 + m3
            columns = (row * 4 + x, row * 4 + 3 - x)

            @pl.loop(0, 4)
            def _(c):
                rows = pl.ds(pl.multiple_of(c * 256, 256), 256)
                for i, w in enumerate((wk, wv)):
                    product = jnp.dot(
                        xbuf[1, base, rows, :], w[weight_rows(columns[0]), :], preferred_element_type=jnp.float32
                    ) + jnp.dot(
                        xbuf[1, base + 1, rows, :], w[weight_rows(columns[1]), :], preferred_element_type=jnp.float32
                    )
                    if first:
                        acc[i, rows, :] = product
                    else:
                        acc[i, rows, :] += product

        remote(mini_own, mini_got, mini_send, mini_sem, partner).start()
        exchange(0)
        direct(quarter * 4)
        exchange(1)
        exchange(2)
        for c in (1, 2, 3):
            direct(quarter * 4 + c)
        direct(opposite * 4 + 2)
        chain_signal(0)
        arrived(mini_got, mini_sem)
        tables(mini_got)
        own_piece(0)
        own_weights(0)
        chain_wait(0)
        chain_signal(1)
        own_piece(1)
        own_piece(2)
        receive_slot(FOREIGN_ORDER, 0)
        own_weights(1)
        chain_wait(1)
        chain_signal(2)
        own_weights(2)
        receive_slot(FOREIGN_ORDER, 1)
        own_weights(3)
        chain_wait(2)
        chain_signal(3)
        for mask in range(8):
            for j in range(N):
                sib_arrived(mask, j)
        quarter_product(quarter, first=True)
        receive_slot(FOREIGN_ORDER, 2)
        for step in (1, 3):
            row = (z + step) % 4
            for c in range(4):
                weights_arrived(row * 4 + c)
            quarter_product(row)
            receive_slot(FOREIGN_ORDER, 3 if step == 1 else 4)
        for c in range(4):
            weights_arrived(opposite * 4 + c)
        quarter_product(opposite)
        for j in range(N):
            add_product(0, 0, j, False)
        for slot in range(7):
            got = receive_slot(FOREIGN_ORDER, slot) if slot > 4 else slot_messages(FOREIGN_ORDER, slot)
            for _, j, _, mask in got:
                add_product(0, mask, j, False)
        chain_wait(3)

    scale = 128 ** (-0.5)
    states = []
    for h in range(2):
        cols = pl.ds(h * 128, 128)
        k = acc[0, :, cols]
        turned = k * cosine[...] + pltpu.roll(k, 64, axis=1) * sine[...]
        keys = (turned * scale).astype(jnp.bfloat16)
        weighted = (keys.astype(jnp.float32) * weight[h]).astype(jnp.bfloat16)
        values = acc[1, :, cols].astype(jnp.bfloat16)
        states.append(
            lax.dot_general(
                weighted, values, (((0,), (0,)), ((), ())), preferred_element_type=jnp.float32
            )
        )
    top = lax.broadcasted_iota(jnp.int32, (8, 128), 0) < 4
    for i in range(16):
        a = states[0][8 * i : 8 * i + 8]
        b = states[1][8 * i : 8 * i + 8]
        send_state[2 * i] = jnp.where(top, a, pltpu.roll(b, 4, axis=0)).astype(jnp.bfloat16)
        send_state[2 * i + 1] = jnp.where(top, pltpu.roll(a, 4, axis=0), b).astype(jnp.bfloat16)
    prompt = z // 8
    for h in range(2):
        rows = pl.ds(2 + 2 * h, 2)
        both = jnp.dot(mini_got[rows, :], states[h], precision=lax.Precision.HIGHEST, preferred_element_type=jnp.float32)
        send_read[h : h + 1, :] = jnp.where(prompt == 0, both[0:1], both[1:2])

    target_tp = jnp.where(is_native, tp, partner_tp)

    def tail(step, other):
        target = (z + step + Z) % Z * 2 + (1 - core if other else core)
        device = (target, target_tp)
        remote(send_state.at[target], got_state.at[block], tail_send, tail_recv, device).start()
        remote(send_read, got_read.at[block], tail_send2, tail_recv2, device).start()

    far = [8]
    for s in range(7, 0, -1):
        far += [s, -s]
    for step in far:
        for other in (False, True):
            tail(step, other)
    tail(0, True)

    @pl.when(is_native)
    def _():
        pltpu.make_async_copy(send_state.at[sp], got_state.at[block], tail_recv).start()
        pltpu.make_async_copy(send_read, got_read.at[block], tail_recv2).start()

    @pl.when(is_foreign)
    def _():
        tail(0, False)

    queries = query[...].astype(jnp.float32)
    dots = queries * key_new[...].astype(jnp.float32)
    news = value_new[...].astype(jnp.float32)
    own_terms = [
        jnp.sum(dots[:, h * 128 : h * 128 + 128], axis=1, keepdims=True) * news[:, h * 128 : h * 128 + 128]
        for h in range(2)
    ]

    arrived(got_read, tail_recv2)
    carried = [jnp.sum(got_read[16 * s : 16 * s + 16], axis=0) for s in range(2)]
    for h in range(2):
        scaled = jnp.exp(jnp.full((1, 128), decay[h], jnp.float32))
        rows = jnp.concatenate([carried[0][h : h + 1], carried[1][h : h + 1]], axis=0)
        mixed = scaled * rows + own_terms[h]
        normed = mixed * lax.rsqrt(jnp.mean(mixed * mixed, axis=1, keepdims=True) + 1e-06)
        read_out[:, h * 128 : h * 128 + 128] = normed * gain[:, h * 128 : h * 128 + 128]
    arrived(got_state, tail_recv)
    for s in range(2):
        total = jnp.zeros((8, 128), jnp.float32)
        for i in range(16):
            total = total + got_state[16 * s + i].astype(jnp.float32)
        state_out[s] = total

    arrived(xbuf.at[0, pl.ds(0, 7)], link_send)
    arrived(xbuf.at[0], sib_send)

    @pl.when(is_native)
    def _():
        arrived(got_state.at[pl.ds(0, 31)], tail_send)
        arrived(got_read.at[pl.ds(0, 31)], tail_send2)

    @pl.when(is_foreign)
    def _():
        arrived(got_state, tail_send)
        arrived(got_read, tail_send2)
        arrived(xbuf.at[0, 0], x_send)
        arrived(mini_own, mini_send)
        arrived(wk.at[pl.ds(0, 2560)], w_send)
        arrived(wk, wz_send)
        arrived(wk.at[pl.ds(0, 1536)], wzz_send)


def on_device(
    layer_input, key_weight, value_weight, decay_exponent, query_new, key_new, value_new, norm_gain
):
    inverse = (1.0 / 10000.0 ** (np.arange(64) / 63.0)).astype(np.float32)
    inverse = jnp.asarray(np.concatenate([inverse, inverse])[None, :])
    vmem = pl.BlockSpec(memory_space=pltpu.VMEM)
    anywhere = pl.BlockSpec(memory_space=pl.ANY)
    dma = pltpu.SemaphoreType.DMA
    state, read = pl.pallas_call(
        kernel,
        name="gather_project_reduce",
        out_shape=(
            jax.ShapeDtypeStruct((2, 8, 128), jnp.float32),
            jax.ShapeDtypeStruct((2, 256), jnp.float32),
        ),
        in_specs=[
            pl.BlockSpec(memory_space=pltpu.SMEM), anywhere, anywhere, anywhere,
            vmem, vmem, vmem, vmem, vmem,
        ],
        out_specs=(vmem, vmem),
        scratch_shapes=[
            pltpu.VMEM((2, 8, TOK, FEAT), jnp.bfloat16),
            pltpu.VMEM((4096, 256), jnp.bfloat16),
            pltpu.VMEM((4096, 256), jnp.bfloat16),
            pltpu.VMEM((2, TOK, 256), jnp.float32),
            pltpu.VMEM((TOK, 128), jnp.float32),
            pltpu.VMEM((TOK, 128), jnp.float32),
            pltpu.VMEM((2, TOK, 128), jnp.float32),
            pltpu.VMEM((8, 128), jnp.float32),
            pltpu.VMEM((8, 128), jnp.float32),
            pltpu.VMEM((SP, 8, 128), jnp.bfloat16),
            pltpu.VMEM((2, 128), jnp.float32),
            pltpu.VMEM((SP, 8, 128), jnp.bfloat16),
            pltpu.VMEM((SP, 2, 128), jnp.float32),
            dma((8, N)), dma((8, N)), dma((16, 2)), dma((2,)), dma,
            dma, dma, dma, dma, dma, dma, dma,
            dma, dma, dma, dma,
            pltpu.SemaphoreType.REGULAR((4,)),
        ],
        compiler_params=pltpu.CompilerParams(collective_id=0, has_side_effects=True),
    )(
        decay_exponent, layer_input, key_weight, value_weight,
        query_new, key_new, value_new, norm_gain[None, :], inverse,
    )
    return (
        state.reshape(2, 2, 4, 128).astype(jnp.bfloat16),
        read.astype(jnp.bfloat16),
    )


def solution(mesh):
    in_specs = (
        P("sp", "tp"), P(None, "tp"), P(None, "tp"), P("tp"),
        P(None, "tp"), P(None, "tp"), P(None, "tp"), P("tp"),
    )
    out_specs = (P(None, "tp", "sp", None), P(None, "tp"))
    return jax.shard_map(
        on_device, mesh=mesh, in_specs=in_specs, out_specs=out_specs, check_vma=False
    )
```

```python
import jax
import jax.numpy as jnp
import numpy as np
from jax import lax
from jax.experimental import pallas as pl
from jax.experimental.pallas import tpu as pltpu
from jax.sharding import PartitionSpec as P

MESH = pl.DeviceIdType.MESH
N = 3
TOK = 1024
FEAT = 256
STARTS = (0, 352, 688, 1024)
SP = 32
Z = 16

NATIVE_ORDER = [[(0, 0), (1, 0), (2, 0), (1, 1), (2, 1), (2, 2), (2, 3)]] * 3
FOREIGN_ORDER = [
    [(0, 0), (2, 0), (1, 0), (2, 1), (1, 1), (2, 2), (2, 3)],
    [(1, 0), (0, 0), (2, 0), (1, 1), (2, 1), (2, 2), (2, 3)],
    [(2, 0), (1, 0), (0, 0), (1, 1), (2, 1), (2, 2), (2, 3)],
]


def turn(mask, j):
    return ((mask << j) | (mask >> (N - j))) & (2**N - 1)


def piece(j):
    return pl.ds(STARTS[j], STARTS[j + 1] - STARTS[j])


def slot_messages(order, slot):
    out = []
    for d in range(N):
        k, r = order[d][slot]
        j = (d - k) % N
        out.append((d, j, turn(r, j), turn(r, j) | (1 << d)))
    return out


def onward(order, d, j, mask):
    out = []
    for dd in range(N):
        for slot in range(7):
            for link, jj, sent, _ in slot_messages(order, slot):
                if link == dd and jj == j and sent == mask:
                    out.append((slot, dd))
    return [dd for _, dd in sorted(out)]


def flip1(v):
    return v + 1 - 2 * (v % 2)


def cos_sin(position, inverse):
    angle = position * inverse
    lane = lax.broadcasted_iota(jnp.int32, angle.shape, 1)
    quarter = jnp.floor(angle * 0.6366197723675814 + 0.5)
    rest = ((angle - quarter * 1.5703125) - quarter * 4.837512969970703125e-4) - quarter * 7.54978995489188e-8
    turns = quarter.astype(jnp.int32) - jnp.where(lane >= 64, 1, 0)
    turns = jnp.bitwise_and(turns, 3)
    square = rest * rest
    sine = rest + rest * square * (-1.6666654611e-1 + square * (8.3321608736e-3 - square * 1.9515295891e-4))
    cosine = 1.0 - 0.5 * square + square * square * (
        4.166664568298827e-2 + square * (-1.388731625493765e-3 + square * 2.443315711809948e-5)
    )
    value = jnp.where(jnp.bitwise_and(turns, 1) == 1, sine, cosine)
    negative = jnp.logical_or(turns == 1, turns == 2)
    return jnp.where(negative, -value, value)


def kernel(
    decay_hbm, x_hbm, wk_hbm, wv_hbm, query_hbm, key_hbm, value_hbm, gain_hbm, inverse_hbm,
    state_out, read_out,
    decay, query, key_new, value_new, gain, inverse,
    xbuf, wk, wv, acc, cosine, sine, weight, mini_own, mini_got, send_state, send_read, got_state, got_read,
    small_sem, mine_sem, sib_sem, w_sem, wl_sem, mini_sem,
    link_send, sib_send, x_send, w_send, wz_send, wzz_send, mini_send,
    tail_send, tail_send2, tail_recv, tail_recv2, chain,
):
    sp = lax.axis_index("sp")
    tp = lax.axis_index("tp")
    z, core = sp // 2, sp % 2
    y, x = tp // 4, tp % 4
    group = (x + 1) // 2 % 2
    block = z * 2 + group
    links = [
        (sp, y * 4 + 3 - x),
        (sp, flip1(y) * 4 + x),
        (sp, (3 - y) * 4 + x),
    ]
    sibling = (z * 2 + 1 - core, tp)
    partner_tp = y * 4 + flip1(x)
    partner = (z * 2 + 1 - core, partner_tp)

    def along_z(step):
        return ((z + step + Z) % Z * 2 + core, tp)

    def signal(semaphore, device):
        pl.semaphore_signal(semaphore, inc=1, device_id=device, device_id_type=MESH)

    def remote(src, dst, send, recv, device):
        return pltpu.make_async_remote_copy(
            src_ref=src, dst_ref=dst, send_sem=send, recv_sem=recv, device_id=device, device_id_type=MESH
        )

    def arrived(ref, semaphore):
        pltpu.make_async_copy(ref, ref, semaphore).wait()

    is_native = core == group
    is_foreign = core != group

    barrier = pltpu.get_barrier_semaphore()
    near = links + [sibling, partner, along_z(1), along_z(-1), along_z(2), along_z(-2)]
    for device in near:
        signal(barrier, device)

    @pl.when(is_native)
    def _():
        for j in range(N):
            pltpu.make_async_copy(x_hbm.at[piece(j)], xbuf.at[0, 0, piece(j)], mine_sem.at[0, j]).start()

    smalls = [
        pltpu.make_async_copy(src, dst, small_sem.at[i])
        for i, (src, dst) in enumerate((
            (decay_hbm, decay), (query_hbm, query), (key_hbm, key_new), (value_hbm, value_new),
            (gain_hbm, gain), (inverse_hbm, inverse),
        ))
    ]
    for copy in smalls:
        copy.start()

    @pl.when(is_native)
    def _():
        pltpu.make_async_copy(wk_hbm, wk, wl_sem.at[0]).start()
        pltpu.make_async_copy(wv_hbm, wv, wl_sem.at[1]).start()

    for copy in smalls:
        copy.wait()
    for h in range(2):
        mini_own[h : h + 1, :] = jnp.broadcast_to(decay[:, h : h + 1], (1, 128))
        mini_own[2 + 2 * h : 4 + 2 * h, :] = query[:, h * 128 : h * 128 + 128].astype(jnp.float32)
    pl.semaphore_wait(barrier, len(near))

    steps = [
        [sibling, partner, along_z(1), along_z(-1), along_z(2), along_z(-2)],
        [along_z(2), along_z(-2)],
        [sibling],
        [along_z(4), along_z(-4)],
    ]

    def chain_signal(n):
        for device in steps[n]:
            signal(chain.at[n], device)

    def chain_wait(n):
        pl.semaphore_wait(chain.at[n], len(steps[n]))

    def send_on(mask, j, over):
        for d in over:
            remote(
                xbuf.at[0, mask, piece(j)], xbuf.at[0, mask | (1 << d), piece(j)],
                link_send, mine_sem.at[mask | (1 << d), j], links[d],
            ).start()

    def to_sibling(mask, j):
        remote(
            xbuf.at[0, mask, piece(j)], xbuf.at[1, mask, piece(j)], sib_send, sib_sem.at[mask, j], sibling
        ).start()

    def column_of(mask, native_part):
        b = [mask // 2**i % 2 for i in range(N)]
        cx = x + b[0] * (3 - 2 * x)
        cy = y + b[1] * (1 - 2 * (y % 2))
        cy = cy + b[2] * (3 - 2 * cy)
        return cy * 4 + (cx if native_part else flip1(cx))

    def weight_rows(t):
        return pl.ds(pl.multiple_of(t * FEAT, FEAT), FEAT)

    def add_product(part, mask, j, native_part, first=False):
        wrows = weight_rows(column_of(mask, native_part))
        block_x = xbuf[part, mask, piece(j), :]
        for i, w in enumerate((wk, wv)):
            product = jnp.dot(block_x, w[wrows, :], preferred_element_type=jnp.float32)
            if first:
                acc[i, piece(j), :] = product
            else:
                acc[i, piece(j), :] += product

    def mine_arrived(mask, j):
        arrived(xbuf.at[0, mask, piece(j)], mine_sem.at[mask, j])

    def sib_arrived(mask, j):
        arrived(xbuf.at[1, mask, piece(j)], sib_sem.at[mask, j])

    def tables(mini):
        @pl.loop(0, 4)
        def _(c):
            rows = pl.ds(pl.multiple_of(c * 256, 256), 256)
            first = (block % 16) * TOK + c * 256
            position = (lax.broadcasted_iota(jnp.int32, (256, 128), 0) + first).astype(jnp.float32)
            table = cos_sin(position, inverse[...])
            swapped = pltpu.roll(table, 64, axis=1)
            low = lax.broadcasted_iota(jnp.int32, (256, 128), 1) < 64
            cosine[rows, :] = jnp.where(low, table, swapped)
            sine[rows, :] = jnp.where(low, -swapped, table)
            distance = 16384 - 1.0 - position
            for h in range(2):
                weight[h, rows, :] = jnp.exp(mini[h : h + 1, :] * distance)

    def receive_slot(order, slot):
        got = slot_messages(order, slot)
        for d, j, _, mask in got:
            mine_arrived(mask, j)
            send_on(mask, j, onward(order, d, j, mask))
            to_sibling(mask, j)
        return got

    @pl.when(is_native)
    def _():
        for j in range(N):
            mine_arrived(0, j)
        for slot in range(3):
            for d, j, mask, _ in slot_messages(NATIVE_ORDER, slot):
                send_on(mask, j, [d])
        for j in range(N):
            to_sibling(0, j)
        chain_signal(0)
        mini_got[...] = mini_own[...]
        tables(mini_own)
        arrived(wk, wl_sem.at[0])
        arrived(wv, wl_sem.at[1])
        for j in range(N):
            add_product(0, 0, j, True, first=True)
        for slot in range(7):
            got = receive_slot(NATIVE_ORDER, slot)
            if slot in (1, 3, 5):
                chain_wait(slot // 2)
                chain_signal(slot // 2 + 1)
            for _, j, _, mask in got:
                add_product(0, mask, j, True)
        for j in range(N):
            sib_arrived(0, j)
            add_product(1, 0, j, False)
        for slot in range(7):
            for _, j, _, mask in slot_messages(FOREIGN_ORDER, slot):
                sib_arrived(mask, j)
                add_product(1, mask, j, False)
        chain_wait(3)

    @pl.when(is_foreign)
    def _():
        quarter = z % 4
        opposite = (z + 2) % 4
        kv = ((wk_hbm, wk), (wv_hbm, wv))

        def direct(t):
            rows = weight_rows(t)
            for i, (src, dst) in enumerate(kv):
                remote(src.at[rows], dst.at[rows], w_send, w_sem.at[t, i], partner).start()

        def pass_weights(t, i, step, semaphore):
            ref = kv[i][1]
            rows = weight_rows(t)
            remote(ref.at[rows], ref.at[rows], semaphore, w_sem.at[t, i], along_z(step)).start()

        def exchange(j):
            remote(x_hbm.at[piece(j)], xbuf.at[0, 0, piece(j)], x_send, mine_sem.at[0, j], partner).start()

        def own_piece(j):
            mine_arrived(0, j)
            send_on(0, j, onward(FOREIGN_ORDER, 0, j, 0))
            to_sibling(0, j)

        def weights_arrived(t):
            for i, (_, ref) in enumerate(kv):
                arrived(ref.at[weight_rows(t)], w_sem.at[t, i])

        def own_weights(c):
            t = quarter * 4 + c
            weights_arrived(t)
            for i in range(2):
                pass_weights(t, i, 1, wz_send)
                pass_weights(t, i, -1, wz_send)

        def quarter_product(row, first=False):
            m1 = jnp.where(row == flip1(y), 2, 0)
            m2 = jnp.where(row == 3 - y, 4, 0)
            m3 = jnp.where(row == 3 - flip1(y), 6, 0)
            base = m1 + m2 + m3
            columns = (row * 4 + x, row * 4 + 3 - x)

            @pl.loop(0, 4)
            def _(c):
                rows = pl.ds(pl.multiple_of(c * 256, 256), 256)
                for i, w in enumerate((wk, wv)):
                    product = jnp.dot(
                        xbuf[1, base, rows, :], w[weight_rows(columns[0]), :], preferred_element_type=jnp.float32
                    ) + jnp.dot(
                        xbuf[1, base + 1, rows, :], w[weight_rows(columns[1]), :], preferred_element_type=jnp.float32
                    )
                    if first:
                        acc[i, rows, :] = product
                    else:
                        acc[i, rows, :] += product

        def pass_on(step):
            t = (z + step) % 4 * 4 + (1 if step == 1 else 0)
            weights_arrived(t)
            pass_weights(t, 0, -step, wzz_send)
            pass_weights(t, 1, -step, wzz_send)

        remote(mini_own, mini_got, mini_send, mini_sem, partner).start()
        direct(quarter * 4)
        direct(quarter * 4 + 1)
        for j in range(N):
            exchange(j)
        for c in (2, 3):
            direct(quarter * 4 + c)
        direct(opposite * 4 + 2)
        direct(opposite * 4 + 3)
        chain_signal(0)
        own_weights(0)
        own_weights(1)
        chain_wait(0)
        chain_signal(1)
        own_piece(0)
        pass_on(-1)
        own_piece(1)
        pass_on(1)
        own_piece(2)
        chain_wait(1)
        chain_signal(2)
        arrived(mini_got, mini_sem)
        tables(mini_got)
        receive_slot(FOREIGN_ORDER, 0)
        own_weights(2)
        receive_slot(FOREIGN_ORDER, 1)
        own_weights(3)
        chain_wait(2)
        chain_signal(3)
        for mask in range(8):
            for j in range(N):
                sib_arrived(mask, j)
        quarter_product(quarter, first=True)
        receive_slot(FOREIGN_ORDER, 2)
        receive_slot(FOREIGN_ORDER, 3)
        for step in (1, 3):
            row = (z + step) % 4
            for c in range(4):
                if (step, c) not in ((1, 1), (3, 0)):
                    weights_arrived(row * 4 + c)
            quarter_product(row)
        receive_slot(FOREIGN_ORDER, 4)
        for c in range(4):
            weights_arrived(opposite * 4 + c)
        quarter_product(opposite)
        for j in range(N):
            add_product(0, 0, j, False)
        for slot in range(7):
            got = receive_slot(FOREIGN_ORDER, slot) if slot > 4 else slot_messages(FOREIGN_ORDER, slot)
            for _, j, _, mask in got:
                add_product(0, mask, j, False)
        chain_wait(3)

    scale = 128 ** (-0.5)
    states = []
    for h in range(2):
        cols = pl.ds(h * 128, 128)
        k = acc[0, :, cols]
        turned = k * cosine[...] + pltpu.roll(k, 64, axis=1) * sine[...]
        keys = (turned * scale).astype(jnp.bfloat16)
        weighted = (keys.astype(jnp.float32) * weight[h]).astype(jnp.bfloat16)
        values = acc[1, :, cols].astype(jnp.bfloat16)
        states.append(
            lax.dot_general(
                weighted, values, (((0,), (0,)), ((), ())), preferred_element_type=jnp.float32
            )
        )
    top = lax.broadcasted_iota(jnp.int32, (8, 128), 0) < 4
    for i in range(16):
        a = states[0][8 * i : 8 * i + 8]
        b = states[1][8 * i : 8 * i + 8]
        send_state[2 * i] = jnp.where(top, a, pltpu.roll(b, 4, axis=0)).astype(jnp.bfloat16)
        send_state[2 * i + 1] = jnp.where(top, pltpu.roll(a, 4, axis=0), b).astype(jnp.bfloat16)
    prompt = z // 8
    for h in range(2):
        rows = pl.ds(2 + 2 * h, 2)
        both = jnp.dot(mini_got[rows, :], states[h], precision=lax.Precision.HIGHEST, preferred_element_type=jnp.float32)
        send_read[h : h + 1, :] = jnp.where(prompt == 0, both[0:1], both[1:2])

    target_tp = jnp.where(is_native, tp, partner_tp)

    def tail(step, other):
        target = (z + step + Z) % Z * 2 + (1 - core if other else core)
        device = (target, target_tp)
        remote(send_state.at[target], got_state.at[block], tail_send, tail_recv, device).start()
        remote(send_read, got_read.at[block], tail_send2, tail_recv2, device).start()

    far = [8]
    for s in range(7, 0, -1):
        far += [s, -s]
    for step in far:
        for other in (False, True):
            tail(step, other)
    tail(0, True)

    @pl.when(is_native)
    def _():
        pltpu.make_async_copy(send_state.at[sp], got_state.at[block], tail_recv).start()
        pltpu.make_async_copy(send_read, got_read.at[block], tail_recv2).start()

    @pl.when(is_foreign)
    def _():
        tail(0, False)

    queries = query[...].astype(jnp.float32)
    dots = queries * key_new[...].astype(jnp.float32)
    news = value_new[...].astype(jnp.float32)
    own_terms = [
        jnp.sum(dots[:, h * 128 : h * 128 + 128], axis=1, keepdims=True) * news[:, h * 128 : h * 128 + 128]
        for h in range(2)
    ]

    arrived(got_read, tail_recv2)
    carried = [jnp.sum(got_read[16 * s : 16 * s + 16], axis=0) for s in range(2)]
    for h in range(2):
        scaled = jnp.exp(mini_own[h : h + 1, :])
        rows = jnp.concatenate([carried[0][h : h + 1], carried[1][h : h + 1]], axis=0)
        mixed = scaled * rows + own_terms[h]
        normed = mixed * lax.rsqrt(jnp.mean(mixed * mixed, axis=1, keepdims=True) + 1e-06)
        read_out[:, h * 128 : h * 128 + 128] = normed * gain[:, h * 128 : h * 128 + 128]
    arrived(got_state, tail_recv)
    for s in range(2):
        total = jnp.zeros((8, 128), jnp.float32)
        for i in range(16):
            total = total + got_state[16 * s + i].astype(jnp.float32)
        state_out[s] = total

    arrived(xbuf.at[0, pl.ds(0, 7)], link_send)
    arrived(xbuf.at[0], sib_send)

    @pl.when(is_native)
    def _():
        arrived(got_state.at[pl.ds(0, 31)], tail_send)
        arrived(got_read.at[pl.ds(0, 31)], tail_send2)

    @pl.when(is_foreign)
    def _():
        arrived(got_state, tail_send)
        arrived(got_read, tail_send2)
        arrived(xbuf.at[0, 0], x_send)
        arrived(mini_own, mini_send)
        arrived(wk.at[pl.ds(0, 3072)], w_send)
        arrived(wk, wz_send)
        arrived(wk.at[pl.ds(0, 1024)], wzz_send)


def on_device(
    layer_input, key_weight, value_weight, decay_exponent, query_new, key_new, value_new, norm_gain
):
    inverse = (1.0 / 10000.0 ** (np.arange(64) / 63.0)).astype(np.float32)
    inverse = jnp.asarray(np.concatenate([inverse, inverse])[None, :])
    vmem = pl.BlockSpec(memory_space=pltpu.VMEM)
    anywhere = pl.BlockSpec(memory_space=pl.ANY)
    dma = pltpu.SemaphoreType.DMA
    state, read = pl.pallas_call(
        kernel,
        name="gather_project_reduce",
        out_shape=(
            pltpu.VMEM((2, 8, 128), jnp.float32),
            pltpu.VMEM((2, 256), jnp.float32),
        ),
        in_specs=[
            anywhere, anywhere, anywhere, anywhere, anywhere, anywhere, anywhere, anywhere, anywhere,
        ],
        out_specs=(vmem, vmem),
        scratch_shapes=[
            pltpu.VMEM((1, 2), jnp.float32),
            pltpu.VMEM((2, 256), jnp.bfloat16),
            pltpu.VMEM((2, 256), jnp.bfloat16),
            pltpu.VMEM((2, 256), jnp.bfloat16),
            pltpu.VMEM((1, 256), jnp.float32),
            pltpu.VMEM((1, 128), jnp.float32),
            pltpu.VMEM((2, 8, TOK, FEAT), jnp.bfloat16),
            pltpu.VMEM((4096, 256), jnp.bfloat16),
            pltpu.VMEM((4096, 256), jnp.bfloat16),
            pltpu.VMEM((2, TOK, 256), jnp.float32),
            pltpu.VMEM((TOK, 128), jnp.float32),
            pltpu.VMEM((TOK, 128), jnp.float32),
            pltpu.VMEM((2, TOK, 128), jnp.float32),
            pltpu.VMEM((8, 128), jnp.float32),
            pltpu.VMEM((8, 128), jnp.float32),
            pltpu.VMEM((SP, 8, 128), jnp.bfloat16),
            pltpu.VMEM((2, 128), jnp.float32),
            pltpu.VMEM((SP, 8, 128), jnp.bfloat16),
            pltpu.VMEM((SP, 2, 128), jnp.float32),
            dma((6,)), dma((8, N)), dma((8, N)), dma((16, 2)), dma((2,)), dma,
            dma, dma, dma, dma, dma, dma, dma,
            dma, dma, dma, dma,
            pltpu.SemaphoreType.REGULAR((4,)),
        ],
        compiler_params=pltpu.CompilerParams(collective_id=0, has_side_effects=True),
    )(
        decay_exponent[None, :], layer_input, key_weight, value_weight,
        query_new, key_new, value_new, norm_gain[None, :], inverse,
    )
    return (
        state.reshape(2, 2, 4, 128).astype(jnp.bfloat16),
        read.astype(jnp.bfloat16),
    )


def solution(mesh):
    in_specs = (
        P("sp", "tp"), P(None, "tp"), P(None, "tp"), P("tp"),
        P(None, "tp"), P(None, "tp"), P(None, "tp"), P("tp"),
    )
    out_specs = (P(None, "tp", "sp", None), P(None, "tp"))
    return jax.shard_map(
        on_device, mesh=mesh, in_specs=in_specs, out_specs=out_specs, check_vma=False
    )
```

```python
import jax
import jax.numpy as jnp
import numpy as np
from jax import lax
from jax.experimental import pallas as pl
from jax.experimental.pallas import tpu as pltpu
from jax.sharding import PartitionSpec as P

MESH = pl.DeviceIdType.MESH
N = 3
TOK = 1024
FEAT = 256
STARTS = (0, 352, 688, 1024)
SP = 32
Z = 16

NATIVE_ORDER = [(0, 0), (1, 0), (2, 0), (1, 1), (2, 1), (2, 2), (2, 3)]
FOREIGN_OWN = [[(k, 0, j) for k in range(N)] for j in range(N)]
FOREIGN_NEXT = [(1, 1, 0), (2, 1, 0), (2, 1, 1)]
FOREIGN_THEN = [(1, 1, 1), (1, 1, 2), (2, 1, 2)]
FOREIGN_LATE = [(2, 2, j) for j in range(N)]
FOREIGN_LAST = [(2, 3, j) for j in range(N)]
FOREIGN_ALL = FOREIGN_OWN + [FOREIGN_NEXT, FOREIGN_THEN, FOREIGN_LATE, FOREIGN_LAST]


def turn(mask, j):
    return ((mask << j) | (mask >> (N - j))) & (2**N - 1)


def piece(j):
    return pl.ds(STARTS[j], STARTS[j + 1] - STARTS[j])


def landing(k, r, j):
    return turn(r, j) | (1 << (j + k) % N)


def native_slot(slot):
    k, r = NATIVE_ORDER[slot]
    out = []
    for d in range(N):
        j = (d - k) % N
        sent = r | (1 << k)
        onward = [(j + kk) % N for kk, rr in NATIVE_ORDER if rr == sent]
        out.append((j, turn(r, j), landing(k, r, j), onward))
    return out


def flip1(v):
    return v + 1 - 2 * (v % 2)


def cos_sin(position, inverse):
    angle = position * inverse
    lane = lax.broadcasted_iota(jnp.int32, angle.shape, 1)
    quarter = jnp.floor(angle * 0.6366197723675814 + 0.5)
    rest = ((angle - quarter * 1.5703125) - quarter * 4.837512969970703125e-4) - quarter * 7.54978995489188e-8
    turns = quarter.astype(jnp.int32) - jnp.where(lane >= 64, 1, 0)
    turns = jnp.bitwise_and(turns, 3)
    square = rest * rest
    sine = rest + rest * square * (-1.6666654611e-1 + square * (8.3321608736e-3 - square * 1.9515295891e-4))
    cosine = 1.0 - 0.5 * square + square * square * (
        4.166664568298827e-2 + square * (-1.388731625493765e-3 + square * 2.443315711809948e-5)
    )
    value = jnp.where(jnp.bitwise_and(turns, 1) == 1, sine, cosine)
    negative = jnp.logical_or(turns == 1, turns == 2)
    return jnp.where(negative, -value, value)


def kernel(
    decay_hbm, x_hbm, wk_hbm, wv_hbm, query_hbm, key_hbm, value_hbm, gain_hbm, inverse_hbm,
    state_out, read_out,
    decay, query, key_new, value_new, gain, inverse,
    xbuf, wk, wv, acc, cosine, sine, weight, mini_own, mini_got, send_state, send_read, got_state, got_read,
    small_sem, mine_sem, sib_sem, w_sem, wl_sem, mini_sem,
    link_send, sib_send, x_send, w_send, wz_send, wzz_send, mini_send,
    tail_send, tail_send2, tail_recv, tail_recv2, chain,
):
    sp = lax.axis_index("sp")
    tp = lax.axis_index("tp")
    z, core = sp // 2, sp % 2
    y, x = tp // 4, tp % 4
    group = 1 - (x + 1) // 2 % 2
    block = z * 2 + group
    links = [
        (sp, y * 4 + 3 - x),
        (sp, flip1(y) * 4 + x),
        (sp, (3 - y) * 4 + x),
    ]
    sibling = (z * 2 + 1 - core, tp)
    partner_tp = y * 4 + flip1(x)
    partner = (z * 2 + 1 - core, partner_tp)

    def along_z(step):
        return ((z + step + Z) % Z * 2 + core, tp)

    def signal(semaphore, device):
        pl.semaphore_signal(semaphore, inc=1, device_id=device, device_id_type=MESH)

    def remote(src, dst, send, recv, device):
        return pltpu.make_async_remote_copy(
            src_ref=src, dst_ref=dst, send_sem=send, recv_sem=recv, device_id=device, device_id_type=MESH
        )

    def arrived(ref, semaphore):
        pltpu.make_async_copy(ref, ref, semaphore).wait()

    is_native = core == group
    is_foreign = core != group

    barrier = pltpu.get_barrier_semaphore()
    near = links + [sibling, partner, along_z(1), along_z(-1), along_z(2), along_z(-2)]
    for device in near:
        signal(barrier, device)

    @pl.when(is_native)
    def _():
        for j in range(N):
            pltpu.make_async_copy(x_hbm.at[piece(j)], xbuf.at[0, 0, piece(j)], mine_sem.at[0, j]).start()

    smalls = [
        pltpu.make_async_copy(src, dst, small_sem.at[i])
        for i, (src, dst) in enumerate((
            (decay_hbm, decay), (query_hbm, query), (key_hbm, key_new), (value_hbm, value_new),
            (gain_hbm, gain), (inverse_hbm, inverse),
        ))
    ]
    for copy in smalls:
        copy.start()

    @pl.when(is_native)
    def _():
        pltpu.make_async_copy(wk_hbm, wk, wl_sem.at[0]).start()
        pltpu.make_async_copy(wv_hbm, wv, wl_sem.at[1]).start()

    pl.semaphore_wait(barrier, len(near))

    def fill_mini():
        for copy in smalls:
            copy.wait()
        for h in range(2):
            mini_own[h : h + 1, :] = jnp.broadcast_to(decay[:, h : h + 1], (1, 128))
            mini_own[2 + 2 * h : 4 + 2 * h, :] = query[:, h * 128 : h * 128 + 128].astype(jnp.float32)

    steps = [
        [sibling, partner, along_z(1), along_z(-1), along_z(2), along_z(-2)],
        [along_z(2), along_z(-2)],
        [sibling],
        [along_z(4), along_z(-4)],
    ]

    def chain_signal(n):
        for device in steps[n]:
            signal(chain.at[n], device)

    def chain_wait(n):
        pl.semaphore_wait(chain.at[n], len(steps[n]))

    def send_on(mask, j, over):
        for d in over:
            remote(
                xbuf.at[0, mask, piece(j)], xbuf.at[0, mask | (1 << d), piece(j)],
                link_send, mine_sem.at[mask | (1 << d), j], links[d],
            ).start()

    def to_sibling(mask, j):
        remote(
            xbuf.at[0, mask, piece(j)], xbuf.at[1, mask, piece(j)], sib_send, sib_sem.at[mask, j], sibling
        ).start()

    def column_of(mask, native_part):
        b = [mask // 2**i % 2 for i in range(N)]
        cx = x + b[0] * (3 - 2 * x)
        cy = y + b[1] * (1 - 2 * (y % 2))
        cy = cy + b[2] * (3 - 2 * cy)
        return cy * 4 + (cx if native_part else flip1(cx))

    def weight_rows(t):
        return pl.ds(pl.multiple_of(t * FEAT, FEAT), FEAT)

    def add_product(part, mask, j, native_part, first=False):
        wrows = weight_rows(column_of(mask, native_part))
        block_x = xbuf[part, mask, piece(j), :]
        for i, w in enumerate((wk, wv)):
            product = jnp.dot(block_x, w[wrows, :], preferred_element_type=jnp.float32)
            if first:
                acc[i, piece(j), :] = product
            else:
                acc[i, piece(j), :] += product

    def mine_arrived(mask, j):
        arrived(xbuf.at[0, mask, piece(j)], mine_sem.at[mask, j])

    def sib_arrived(mask, j):
        arrived(xbuf.at[1, mask, piece(j)], sib_sem.at[mask, j])

    def tables(mini):
        @pl.loop(0, 4)
        def _(c):
            rows = pl.ds(pl.multiple_of(c * 256, 256), 256)
            first = (block % 16) * TOK + c * 256
            position = (lax.broadcasted_iota(jnp.int32, (256, 128), 0) + first).astype(jnp.float32)
            table = cos_sin(position, inverse[...])
            swapped = pltpu.roll(table, 64, axis=1)
            low = lax.broadcasted_iota(jnp.int32, (256, 128), 1) < 64
            cosine[rows, :] = jnp.where(low, table, swapped)
            sine[rows, :] = jnp.where(low, -swapped, table)
            distance = 16384 - 1.0 - position
            for h in range(2):
                weight[h, rows, :] = jnp.exp(mini[h : h + 1, :] * distance)

    @pl.when(is_native)
    def _():
        for j in range(N):
            mine_arrived(0, j)
        for slot in range(3):
            for d in range(N):
                send_on(0, (d - slot) % N, [d])
        for j in range(N):
            to_sibling(0, j)
        chain_signal(0)
        fill_mini()
        mini_got[...] = mini_own[...]
        tables(mini_got)
        arrived(wk, wl_sem.at[0])
        arrived(wv, wl_sem.at[1])
        for j in range(N):
            add_product(0, 0, j, True, first=True)
        for slot in range(7):
            got = native_slot(slot)
            for j, _, mask, onward in got:
                mine_arrived(mask, j)
                send_on(mask, j, onward)
                to_sibling(mask, j)
            if slot in (1, 3, 5):
                chain_wait(slot // 2)
                chain_signal(slot // 2 + 1)
            for j, _, mask, _ in got:
                add_product(0, mask, j, True)
        for j in range(N):
            sib_arrived(0, j)
            add_product(1, 0, j, False)
        for slot in range(7):
            for k, r, j in FOREIGN_ALL[slot]:
                sib_arrived(landing(k, r, j), j)
                add_product(1, landing(k, r, j), j, False)
        chain_wait(3)

    @pl.when(is_foreign)
    def _():
        quarter = z % 4
        opposite = (z + 2) % 4
        kv = ((wk_hbm, wk), (wv_hbm, wv))

        def direct(t):
            rows = weight_rows(t)
            for i, (src, dst) in enumerate(kv):
                remote(src.at[rows], dst.at[rows], w_send, w_sem.at[t, i], partner).start()

        def pass_weights(t, i, step, semaphore):
            ref = kv[i][1]
            rows = weight_rows(t)
            remote(ref.at[rows], ref.at[rows], semaphore, w_sem.at[t, i], along_z(step)).start()

        def exchange(j):
            remote(x_hbm.at[piece(j)], xbuf.at[0, 0, piece(j)], x_send, mine_sem.at[0, j], partner).start()

        def own_piece(j):
            mine_arrived(0, j)
            send_on(0, j, [(j + k) % N for k in range(N)])
            to_sibling(0, j)

        def receive(k, r, j, *to):
            mask = landing(k, r, j)
            mine_arrived(mask, j)
            send_on(mask, j, [(j + kk) % N for kk in to])
            to_sibling(mask, j)

        def foreign_product(messages):
            for k, r, j in messages:
                add_product(0, landing(k, r, j), j, False)

        def weights_arrived(t):
            for i, (_, ref) in enumerate(kv):
                arrived(ref.at[weight_rows(t)], w_sem.at[t, i])

        def own_weights(c):
            t = quarter * 4 + c
            weights_arrived(t)
            for i in range(2):
                pass_weights(t, i, 1, wz_send)
                pass_weights(t, i, -1, wz_send)

        def quarter_product(row, first=False):
            m1 = jnp.where(row == flip1(y), 2, 0)
            m2 = jnp.where(row == 3 - y, 4, 0)
            m3 = jnp.where(row == 3 - flip1(y), 6, 0)
            base = m1 + m2 + m3
            columns = (row * 4 + x, row * 4 + 3 - x)

            @pl.loop(0, 4)
            def _(c):
                rows = pl.ds(pl.multiple_of(c * 256, 256), 256)
                for i, w in enumerate((wk, wv)):
                    product = jnp.dot(
                        xbuf[1, base, rows, :], w[weight_rows(columns[0]), :], preferred_element_type=jnp.float32
                    ) + jnp.dot(
                        xbuf[1, base + 1, rows, :], w[weight_rows(columns[1]), :], preferred_element_type=jnp.float32
                    )
                    if first:
                        acc[i, rows, :] = product
                    else:
                        acc[i, rows, :] += product

        def pass_on(step):
            t = (z + step) % 4 * 4 + (1 if step == 1 else 0)
            weights_arrived(t)
            pass_weights(t, 0, -step, wzz_send)
            pass_weights(t, 1, -step, wzz_send)

        direct(quarter * 4)
        direct(quarter * 4 + 1)
        fill_mini()
        for j in range(N):
            exchange(j)
        remote(mini_own, mini_got, mini_send, mini_sem, partner).start()
        for c in (2, 3):
            direct(quarter * 4 + c)
        direct(opposite * 4 + 2)
        direct(opposite * 4 + 3)
        chain_signal(0)
        own_weights(0)
        own_weights(1)
        chain_wait(0)
        chain_signal(1)
        own_piece(0)
        pass_on(-1)
        own_piece(1)
        pass_on(1)
        own_piece(2)
        chain_wait(1)
        chain_signal(2)
        arrived(mini_got, mini_sem)
        tables(mini_got)
        receive(0, 0, 0, 1, 2)
        receive(1, 0, 0)
        receive(2, 0, 0)
        own_weights(2)
        own_weights(3)
        receive(0, 0, 1, 1, 2)
        receive(1, 0, 1)
        send_on(landing(1, 0, 0), 0, [2])
        receive(2, 0, 1)
        chain_wait(2)
        chain_signal(3)
        receive(0, 0, 2, 1, 2)
        send_on(landing(1, 0, 1), 1, [0])
        receive(1, 0, 2, 2)
        receive(2, 0, 2)
        for mask in range(8):
            for j in range(N):
                sib_arrived(mask, j)
        quarter_product(quarter, first=True)
        receive(1, 1, 0, 2)
        receive(2, 1, 0)
        receive(2, 1, 1)
        row = (z + 1) % 4
        for c in (0, 2, 3):
            weights_arrived(row * 4 + c)
        quarter_product(row)
        for c in range(4):
            weights_arrived(opposite * 4 + c)
        row = (z + 3) % 4
        for c in (1, 2, 3):
            weights_arrived(row * 4 + c)
        for j in range(N):
            add_product(0, 0, j, False)
        receive(1, 1, 1, 2)
        receive(1, 1, 2, 2)
        receive(2, 1, 2)
        quarter_product(row)
        foreign_product(FOREIGN_OWN[0])
        foreign_product(FOREIGN_OWN[1])
        for message in FOREIGN_LATE:
            receive(*message)
        quarter_product(opposite)
        foreign_product(FOREIGN_OWN[2])
        for message in FOREIGN_LAST:
            receive(*message)
        for messages in FOREIGN_ALL[3:]:
            foreign_product(messages)
        chain_wait(3)

    scale = 128 ** (-0.5)
    states = []
    for h in range(2):
        cols = pl.ds(h * 128, 128)
        k = acc[0, :, cols]
        turned = k * cosine[...] + pltpu.roll(k, 64, axis=1) * sine[...]
        keys = (turned * scale).astype(jnp.bfloat16)
        weighted = (keys.astype(jnp.float32) * weight[h]).astype(jnp.bfloat16)
        values = acc[1, :, cols].astype(jnp.bfloat16)
        states.append(
            lax.dot_general(
                weighted, values, (((0,), (0,)), ((), ())), preferred_element_type=jnp.float32
            )
        )
    top = lax.broadcasted_iota(jnp.int32, (8, 128), 0) < 4
    for i in range(16):
        a = states[0][8 * i : 8 * i + 8]
        b = states[1][8 * i : 8 * i + 8]
        send_state[2 * i] = jnp.where(top, a, pltpu.roll(b, 4, axis=0)).astype(jnp.bfloat16)
        send_state[2 * i + 1] = jnp.where(top, pltpu.roll(a, 4, axis=0), b).astype(jnp.bfloat16)
    prompt = z // 8
    for h in range(2):
        rows = pl.ds(2 + 2 * h, 2)
        both = jnp.dot(mini_got[rows, :], states[h], precision=lax.Precision.HIGHEST, preferred_element_type=jnp.float32)
        send_read[h : h + 1, :] = jnp.where(prompt == 0, both[0:1], both[1:2])

    target_tp = jnp.where(is_native, tp, partner_tp)

    def tail(step, other):
        target = (z + step + Z) % Z * 2 + (1 - core if other else core)
        device = (target, target_tp)
        remote(send_state.at[target], got_state.at[block], tail_send, tail_recv, device).start()
        remote(send_read, got_read.at[block], tail_send2, tail_recv2, device).start()

    far = [8]
    for s in range(7, 0, -1):
        far += [s, -s]
    for step in far:
        for other in (False, True):
            tail(step, other)
    tail(0, True)

    @pl.when(is_native)
    def _():
        pltpu.make_async_copy(send_state.at[sp], got_state.at[block], tail_recv).start()
        pltpu.make_async_copy(send_read, got_read.at[block], tail_recv2).start()

    @pl.when(is_foreign)
    def _():
        tail(0, False)

    queries = query[...].astype(jnp.float32)
    dots = queries * key_new[...].astype(jnp.float32)
    news = value_new[...].astype(jnp.float32)
    own_terms = [
        jnp.sum(dots[:, h * 128 : h * 128 + 128], axis=1, keepdims=True) * news[:, h * 128 : h * 128 + 128]
        for h in range(2)
    ]

    arrived(got_read, tail_recv2)
    carried = [jnp.sum(got_read[16 * s : 16 * s + 16], axis=0) for s in range(2)]
    for h in range(2):
        scaled = jnp.exp(mini_own[h : h + 1, :])
        rows = jnp.concatenate([carried[0][h : h + 1], carried[1][h : h + 1]], axis=0)
        mixed = scaled * rows + own_terms[h]
        normed = mixed * lax.rsqrt(jnp.mean(mixed * mixed, axis=1, keepdims=True) + 1e-06)
        read_out[:, h * 128 : h * 128 + 128] = normed * gain[:, h * 128 : h * 128 + 128]
    arrived(got_state, tail_recv)
    for s in range(2):
        total = jnp.zeros((8, 128), jnp.float32)
        for i in range(16):
            total = total + got_state[16 * s + i].astype(jnp.float32)
        state_out[s] = total

    arrived(xbuf.at[0, pl.ds(0, 7)], link_send)
    arrived(xbuf.at[0], sib_send)

    @pl.when(is_native)
    def _():
        arrived(got_state.at[pl.ds(0, 31)], tail_send)
        arrived(got_read.at[pl.ds(0, 31)], tail_send2)

    @pl.when(is_foreign)
    def _():
        arrived(got_state, tail_send)
        arrived(got_read, tail_send2)
        arrived(xbuf.at[0, 0], x_send)
        arrived(mini_own, mini_send)
        arrived(wk.at[pl.ds(0, 3072)], w_send)
        arrived(wk, wz_send)
        arrived(wk.at[pl.ds(0, 1024)], wzz_send)


def on_device(
    layer_input, key_weight, value_weight, decay_exponent, query_new, key_new, value_new, norm_gain
):
    inverse = (1.0 / 10000.0 ** (np.arange(64) / 63.0)).astype(np.float32)
    inverse = jnp.asarray(np.concatenate([inverse, inverse])[None, :])
    vmem = pl.BlockSpec(memory_space=pltpu.VMEM)
    anywhere = pl.BlockSpec(memory_space=pl.ANY)
    dma = pltpu.SemaphoreType.DMA
    state, read = pl.pallas_call(
        kernel,
        name="gather_project_reduce",
        out_shape=(
            pltpu.VMEM((2, 8, 128), jnp.float32),
            pltpu.VMEM((2, 256), jnp.float32),
        ),
        in_specs=[
            anywhere, anywhere, anywhere, anywhere, anywhere, anywhere, anywhere, anywhere, anywhere,
        ],
        out_specs=(vmem, vmem),
        scratch_shapes=[
            pltpu.VMEM((1, 2), jnp.float32),
            pltpu.VMEM((2, 256), jnp.bfloat16),
            pltpu.VMEM((2, 256), jnp.bfloat16),
            pltpu.VMEM((2, 256), jnp.bfloat16),
            pltpu.VMEM((1, 256), jnp.float32),
            pltpu.VMEM((1, 128), jnp.float32),
            pltpu.VMEM((2, 8, TOK, FEAT), jnp.bfloat16),
            pltpu.VMEM((4096, 256), jnp.bfloat16),
            pltpu.VMEM((4096, 256), jnp.bfloat16),
            pltpu.VMEM((2, TOK, 256), jnp.float32),
            pltpu.VMEM((TOK, 128), jnp.float32),
            pltpu.VMEM((TOK, 128), jnp.float32),
            pltpu.VMEM((2, TOK, 128), jnp.float32),
            pltpu.VMEM((8, 128), jnp.float32),
            pltpu.VMEM((8, 128), jnp.float32),
            pltpu.VMEM((SP, 8, 128), jnp.bfloat16),
            pltpu.VMEM((2, 128), jnp.float32),
            pltpu.VMEM((SP, 8, 128), jnp.bfloat16),
            pltpu.VMEM((SP, 2, 128), jnp.float32),
            dma((6,)), dma((8, N)), dma((8, N)), dma((16, 2)), dma((2,)), dma,
            dma, dma, dma, dma, dma, dma, dma,
            dma, dma, dma, dma,
            pltpu.SemaphoreType.REGULAR((4,)),
        ],
        compiler_params=pltpu.CompilerParams(collective_id=0, has_side_effects=True),
    )(
        decay_exponent[None, :], layer_input, key_weight, value_weight,
        query_new, key_new, value_new, norm_gain[None, :], inverse,
    )
    return (
        state.reshape(2, 2, 4, 128).astype(jnp.bfloat16),
        read.astype(jnp.bfloat16),
    )


def solution(mesh):
    in_specs = (
        P("sp", "tp"), P(None, "tp"), P(None, "tp"), P("tp"),
        P(None, "tp"), P(None, "tp"), P(None, "tp"), P("tp"),
    )
    out_specs = (P(None, "tp", "sp", None), P(None, "tp"))
    return jax.shard_map(
        on_device, mesh=mesh, in_specs=in_specs, out_specs=out_specs, check_vma=False
    )
```

```python
import jax
import jax.numpy as jnp
import numpy as np
from jax import lax
from jax.experimental import pallas as pl
from jax.experimental.pallas import tpu as pltpu
from jax.sharding import PartitionSpec as P

MESH = pl.DeviceIdType.MESH
N = 3
TOK = 1024
FEAT = 256
STARTS = (0, 352, 688, 1024)
SP = 32
Z = 16

NATIVE_ORDER = [(0, 0), (1, 0), (2, 0), (1, 1), (2, 1), (2, 2), (2, 3)]
FOREIGN_ORDER = [(0, 0), (1, 0), (1, 1), (2, 0), (2, 1), (2, 2), (2, 3)]


def turn(mask, j):
    return ((mask << j) | (mask >> (N - j))) & (2**N - 1)


def piece(j):
    return pl.ds(STARTS[j], STARTS[j + 1] - STARTS[j])


def landing(k, r, j):
    return turn(r, j) | (1 << (j + k) % N)


def native_slot(slot):
    k, r = NATIVE_ORDER[slot]
    out = []
    for d in range(N):
        j = (d - k) % N
        sent = r | (1 << k)
        onward = [(j + kk) % N for kk, rr in NATIVE_ORDER if rr == sent]
        out.append((j, turn(r, j), landing(k, r, j), onward))
    return out


def flip1(v):
    return v + 1 - 2 * (v % 2)


def cos_sin(position, inverse):
    angle = position * inverse
    lane = lax.broadcasted_iota(jnp.int32, angle.shape, 1)
    quarter = jnp.floor(angle * 0.6366197723675814 + 0.5)
    rest = ((angle - quarter * 1.5703125) - quarter * 4.837512969970703125e-4) - quarter * 7.54978995489188e-8
    turns = quarter.astype(jnp.int32) - jnp.where(lane >= 64, 1, 0)
    turns = jnp.bitwise_and(turns, 3)
    square = rest * rest
    sine = rest + rest * square * (-1.6666654611e-1 + square * (8.3321608736e-3 - square * 1.9515295891e-4))
    cosine = 1.0 - 0.5 * square + square * square * (
        4.166664568298827e-2 + square * (-1.388731625493765e-3 + square * 2.443315711809948e-5)
    )
    value = jnp.where(jnp.bitwise_and(turns, 1) == 1, sine, cosine)
    negative = jnp.logical_or(turns == 1, turns == 2)
    return jnp.where(negative, -value, value)


def kernel(
    decay_hbm, x_hbm, wk_hbm, wv_hbm, query_hbm, key_hbm, value_hbm, gain_hbm, inverse_hbm,
    state_out, read_out,
    decay, query, key_new, value_new, gain, inverse,
    xbuf, wk, wv, acc, cosine, sine, weight, mini_own, mini_got, send_state, send_read, got_state, got_read,
    small_sem, mine_sem, sib_sem, w_sem, wl_sem, mini_sem,
    link_send, sib_send, x_send, w_send, wz_send, wzz_send, mini_send,
    tail_send, tail_send2, tail_recv, tail_recv2, chain,
):
    sp = lax.axis_index("sp")
    tp = lax.axis_index("tp")
    z, core = sp // 2, sp % 2
    y, x = tp // 4, tp % 4
    group = 1 - (x + 1) // 2 % 2
    block = z * 2 + group
    links = [
        (sp, y * 4 + 3 - x),
        (sp, flip1(y) * 4 + x),
        (sp, (3 - y) * 4 + x),
    ]
    sibling = (z * 2 + 1 - core, tp)
    partner_tp = y * 4 + flip1(x)
    partner = (z * 2 + 1 - core, partner_tp)

    def along_z(step):
        return ((z + step + Z) % Z * 2 + core, tp)

    def signal(semaphore, device):
        pl.semaphore_signal(semaphore, inc=1, device_id=device, device_id_type=MESH)

    def remote(src, dst, send, recv, device):
        return pltpu.make_async_remote_copy(
            src_ref=src, dst_ref=dst, send_sem=send, recv_sem=recv, device_id=device, device_id_type=MESH
        )

    def arrived(ref, semaphore):
        pltpu.make_async_copy(ref, ref, semaphore).wait()

    is_native = core == group
    is_foreign = core != group

    barrier = pltpu.get_barrier_semaphore()
    near = links + [sibling, partner, along_z(1), along_z(-1), along_z(2), along_z(-2)]
    for device in near:
        signal(barrier, device)

    @pl.when(is_native)
    def _():
        for j in range(N):
            pltpu.make_async_copy(x_hbm.at[piece(j)], xbuf.at[0, 0, piece(j)], mine_sem.at[0, j]).start()

    smalls = [
        pltpu.make_async_copy(src, dst, small_sem.at[i])
        for i, (src, dst) in enumerate((
            (decay_hbm, decay), (query_hbm, query), (key_hbm, key_new), (value_hbm, value_new),
            (gain_hbm, gain), (inverse_hbm, inverse),
        ))
    ]
    for copy in smalls:
        copy.start()

    @pl.when(is_native)
    def _():
        pltpu.make_async_copy(wk_hbm, wk, wl_sem.at[0]).start()
        pltpu.make_async_copy(wv_hbm, wv, wl_sem.at[1]).start()

    pl.semaphore_wait(barrier, len(near))

    def fill_mini():
        for copy in smalls:
            copy.wait()
        for h in range(2):
            mini_own[h : h + 1, :] = jnp.broadcast_to(decay[:, h : h + 1], (1, 128))
            mini_own[2 + 2 * h : 4 + 2 * h, :] = query[:, h * 128 : h * 128 + 128].astype(jnp.float32)

    steps = [
        [sibling, partner, along_z(1), along_z(-1), along_z(2), along_z(-2)],
        [along_z(2), along_z(-2)],
        [sibling],
        [along_z(4), along_z(-4)],
    ]

    def chain_signal(n):
        for device in steps[n]:
            signal(chain.at[n], device)

    def chain_wait(n):
        pl.semaphore_wait(chain.at[n], len(steps[n]))

    def send_on(mask, j, over):
        for d in over:
            remote(
                xbuf.at[0, mask, piece(j)], xbuf.at[0, mask | (1 << d), piece(j)],
                link_send, mine_sem.at[mask | (1 << d), j], links[d],
            ).start()

    def to_sibling(mask, j):
        remote(
            xbuf.at[0, mask, piece(j)], xbuf.at[1, mask, piece(j)], sib_send, sib_sem.at[mask, j], sibling
        ).start()

    def column_of(mask, native_part):
        b = [mask // 2**i % 2 for i in range(N)]
        cx = x + b[0] * (3 - 2 * x)
        cy = y + b[1] * (1 - 2 * (y % 2))
        cy = cy + b[2] * (3 - 2 * cy)
        return cy * 4 + (cx if native_part else flip1(cx))

    def weight_rows(t):
        return pl.ds(pl.multiple_of(t * FEAT, FEAT), FEAT)

    def add_product(part, mask, j, native_part, first=False):
        wrows = weight_rows(column_of(mask, native_part))
        block_x = xbuf[part, mask, piece(j), :]
        for i, w in enumerate((wk, wv)):
            product = jnp.dot(block_x, w[wrows, :], preferred_element_type=jnp.float32)
            if first:
                acc[i, piece(j), :] = product
            else:
                acc[i, piece(j), :] += product

    def mine_arrived(mask, j):
        arrived(xbuf.at[0, mask, piece(j)], mine_sem.at[mask, j])

    def sib_arrived(mask, j):
        arrived(xbuf.at[1, mask, piece(j)], sib_sem.at[mask, j])

    def tables(mini):
        @pl.loop(0, 4)
        def _(c):
            rows = pl.ds(pl.multiple_of(c * 256, 256), 256)
            first = (block % 16) * TOK + c * 256
            position = (lax.broadcasted_iota(jnp.int32, (256, 128), 0) + first).astype(jnp.float32)
            table = cos_sin(position, inverse[...])
            swapped = pltpu.roll(table, 64, axis=1)
            low = lax.broadcasted_iota(jnp.int32, (256, 128), 1) < 64
            cosine[rows, :] = jnp.where(low, table, swapped)
            sine[rows, :] = jnp.where(low, -swapped, table)
            distance = 16384 - 1.0 - position
            for h in range(2):
                weight[h, rows, :] = jnp.exp(mini[h : h + 1, :] * distance)

    @pl.when(is_native)
    def _():
        for j in range(N):
            mine_arrived(0, j)
        for slot in range(3):
            for d in range(N):
                send_on(0, (d - slot) % N, [d])
        for j in range(N):
            to_sibling(0, j)
        chain_signal(0)
        fill_mini()
        mini_got[...] = mini_own[...]
        tables(mini_got)
        arrived(wk, wl_sem.at[0])
        arrived(wv, wl_sem.at[1])
        for j in range(N):
            add_product(0, 0, j, True, first=True)
        for slot in range(7):
            got = native_slot(slot)
            for j, _, mask, onward in got:
                mine_arrived(mask, j)
                send_on(mask, j, onward)
                to_sibling(mask, j)
            if slot in (1, 3, 5):
                chain_wait(slot // 2)
                chain_signal(slot // 2 + 1)
            for j, _, mask, _ in got:
                add_product(0, mask, j, True)
        for j in range(N):
            sib_arrived(0, j)
            add_product(1, 0, j, False)
        for slot in range(7):
            k, r = FOREIGN_ORDER[slot]
            for j in range(N):
                sib_arrived(landing(k, r, j), j)
                add_product(1, landing(k, r, j), j, False)
        chain_wait(3)

    @pl.when(is_foreign)
    def _():
        quarter = z % 4
        opposite = (z + 2) % 4
        kv = ((wk_hbm, wk), (wv_hbm, wv))

        other = flip1(x)
        mine_first = (x, 3 - x, other, 3 - other)
        theirs_first = (other, 3 - other, x, 3 - x)

        def direct(row, i):
            t = row * 4 + theirs_first[i]
            rows = weight_rows(t)
            for n, (src, dst) in enumerate(kv):
                remote(src.at[rows], dst.at[rows], w_send, w_sem.at[t, n], partner).start()

        def pass_weights(t, i, step, semaphore):
            ref = kv[i][1]
            rows = weight_rows(t)
            remote(ref.at[rows], ref.at[rows], semaphore, w_sem.at[t, i], along_z(step)).start()

        def exchange(j):
            remote(x_hbm.at[piece(j)], xbuf.at[0, 0, piece(j)], x_send, mine_sem.at[0, j], partner).start()

        def own_piece(j):
            mine_arrived(0, j)
            send_on(0, j, [j])
            to_sibling(0, j)

        def receive(k, r, j, *to):
            mask = landing(k, r, j)
            mine_arrived(mask, j)
            send_on(mask, j, [(j + kk) % N for kk in to])
            to_sibling(mask, j)

        def native_product(slot):
            for j, _, mask, _ in native_slot(slot):
                sib_arrived(mask, j)
                add_product(1, mask, j, True)

        def foreign_product(k, r):
            for j in range(N):
                add_product(0, landing(k, r, j), j, False)

        def weights_arrived(t):
            for i, (_, ref) in enumerate(kv):
                arrived(ref.at[weight_rows(t)], w_sem.at[t, i])

        def own_weights(i):
            t = quarter * 4 + mine_first[i]
            weights_arrived(t)
            for n in range(2):
                pass_weights(t, n, 1, wz_send)
                pass_weights(t, n, -1, wz_send)

        def pass_on(step):
            t = (z + step) % 4 * 4 + mine_first[1 if step == 1 else 0]
            weights_arrived(t)
            pass_weights(t, 0, -step, wzz_send)
            pass_weights(t, 1, -step, wzz_send)

        def row_weights(step, *indices):
            for i in indices:
                weights_arrived((z + step) % 4 * 4 + mine_first[i])

        direct(quarter, 0)
        direct(quarter, 1)
        fill_mini()
        for j in range(N):
            exchange(j)
        remote(mini_own, mini_got, mini_send, mini_sem, partner).start()
        direct(quarter, 2)
        direct(quarter, 3)
        direct(opposite, 2)
        direct(opposite, 3)
        chain_signal(0)
        own_weights(0)
        own_weights(1)
        chain_wait(0)
        chain_signal(1)
        own_piece(0)
        pass_on(-1)
        own_piece(1)
        send_on(0, 0, [1])
        pass_on(1)
        own_piece(2)
        send_on(0, 1, [2])
        send_on(0, 2, [0])
        chain_wait(1)
        chain_signal(2)
        arrived(mini_got, mini_sem)
        tables(mini_got)
        receive(0, 0, 0, 1)
        row_weights(1, 0)
        row_weights(3, 1)
        row_weights(2, 0, 1)
        for j in range(N):
            sib_arrived(0, j)
            add_product(1, 0, j, True, first=True)
        own_weights(2)
        native_product(0)
        receive(0, 0, 1, 1)
        native_product(1)
        native_product(2)
        own_weights(3)
        receive(0, 0, 2, 1)
        for j in range(N):
            send_on(0, j, [(j + 2) % N])
            send_on(landing(0, 0, j), j, [(j + 2) % N])
        chain_wait(2)
        chain_signal(3)
        native_product(3)
        native_product(4)
        for j in (2, 0, 1):
            receive(1, 0, j, 2)
        native_product(5)
        native_product(6)
        for j in range(N):
            receive(1, 1, j, 2)
        for j in range(N):
            receive(2, 0, j)
        row_weights(1, 2, 3)
        row_weights(3, 2, 3)
        row_weights(2, 2, 3)
        for j in range(N):
            add_product(0, 0, j, False)
        foreign_product(0, 0)
        foreign_product(1, 0)
        for j in range(N):
            receive(2, 1, j)
        foreign_product(1, 1)
        foreign_product(2, 0)
        for j in range(N):
            receive(2, 2, j)
        foreign_product(2, 1)
        foreign_product(2, 2)
        for j in range(N):
            receive(2, 3, j)
        foreign_product(2, 3)
        chain_wait(3)

    scale = 128 ** (-0.5)
    states = []
    for h in range(2):
        cols = pl.ds(h * 128, 128)
        k = acc[0, :, cols]
        turned = k * cosine[...] + pltpu.roll(k, 64, axis=1) * sine[...]
        keys = (turned * scale).astype(jnp.bfloat16)
        weighted = (keys.astype(jnp.float32) * weight[h]).astype(jnp.bfloat16)
        values = acc[1, :, cols].astype(jnp.bfloat16)
        states.append(
            lax.dot_general(
                weighted, values, (((0,), (0,)), ((), ())), preferred_element_type=jnp.float32
            )
        )
    top = lax.broadcasted_iota(jnp.int32, (8, 128), 0) < 4
    for i in range(16):
        a = states[0][8 * i : 8 * i + 8]
        b = states[1][8 * i : 8 * i + 8]
        send_state[2 * i] = jnp.where(top, a, pltpu.roll(b, 4, axis=0)).astype(jnp.bfloat16)
        send_state[2 * i + 1] = jnp.where(top, pltpu.roll(a, 4, axis=0), b).astype(jnp.bfloat16)
    prompt = z // 8
    for h in range(2):
        rows = pl.ds(2 + 2 * h, 2)
        both = jnp.dot(mini_got[rows, :], states[h], precision=lax.Precision.HIGHEST, preferred_element_type=jnp.float32)
        send_read[h : h + 1, :] = jnp.where(prompt == 0, both[0:1], both[1:2])

    target_tp = jnp.where(is_native, tp, partner_tp)

    def tail(step, other):
        target = (z + step + Z) % Z * 2 + (1 - core if other else core)
        device = (target, target_tp)
        remote(send_state.at[target], got_state.at[block], tail_send, tail_recv, device).start()
        remote(send_read, got_read.at[block], tail_send2, tail_recv2, device).start()

    far = [8]
    for s in range(7, 0, -1):
        far += [s, -s]
    for step in far:
        for other in (False, True):
            tail(step, other)
    tail(0, True)

    @pl.when(is_native)
    def _():
        pltpu.make_async_copy(send_state.at[sp], got_state.at[block], tail_recv).start()
        pltpu.make_async_copy(send_read, got_read.at[block], tail_recv2).start()

    @pl.when(is_foreign)
    def _():
        tail(0, False)

    queries = query[...].astype(jnp.float32)
    dots = queries * key_new[...].astype(jnp.float32)
    news = value_new[...].astype(jnp.float32)
    own_terms = [
        jnp.sum(dots[:, h * 128 : h * 128 + 128], axis=1, keepdims=True) * news[:, h * 128 : h * 128 + 128]
        for h in range(2)
    ]

    arrived(got_read, tail_recv2)
    carried = [jnp.sum(got_read[16 * s : 16 * s + 16], axis=0) for s in range(2)]
    for h in range(2):
        scaled = jnp.exp(mini_own[h : h + 1, :])
        rows = jnp.concatenate([carried[0][h : h + 1], carried[1][h : h + 1]], axis=0)
        mixed = scaled * rows + own_terms[h]
        normed = mixed * lax.rsqrt(jnp.mean(mixed * mixed, axis=1, keepdims=True) + 1e-06)
        read_out[:, h * 128 : h * 128 + 128] = normed * gain[:, h * 128 : h * 128 + 128]
    arrived(got_state, tail_recv)
    for s in range(2):
        total = jnp.zeros((8, 128), jnp.float32)
        for i in range(16):
            total = total + got_state[16 * s + i].astype(jnp.float32)
        state_out[s] = total

    arrived(xbuf.at[0, pl.ds(0, 7)], link_send)
    arrived(xbuf.at[0], sib_send)

    @pl.when(is_native)
    def _():
        arrived(got_state.at[pl.ds(0, 31)], tail_send)
        arrived(got_read.at[pl.ds(0, 31)], tail_send2)

    @pl.when(is_foreign)
    def _():
        arrived(got_state, tail_send)
        arrived(got_read, tail_send2)
        arrived(xbuf.at[0, 0], x_send)
        arrived(mini_own, mini_send)
        arrived(wk.at[pl.ds(0, 3072)], w_send)
        arrived(wk, wz_send)
        arrived(wk.at[pl.ds(0, 1024)], wzz_send)


def on_device(
    layer_input, key_weight, value_weight, decay_exponent, query_new, key_new, value_new, norm_gain
):
    inverse = (1.0 / 10000.0 ** (np.arange(64) / 63.0)).astype(np.float32)
    inverse = jnp.asarray(np.concatenate([inverse, inverse])[None, :])
    vmem = pl.BlockSpec(memory_space=pltpu.VMEM)
    anywhere = pl.BlockSpec(memory_space=pl.ANY)
    dma = pltpu.SemaphoreType.DMA
    state, read = pl.pallas_call(
        kernel,
        name="gather_project_reduce",
        out_shape=(
            pltpu.VMEM((2, 8, 128), jnp.float32),
            pltpu.VMEM((2, 256), jnp.float32),
        ),
        in_specs=[
            anywhere, anywhere, anywhere, anywhere, anywhere, anywhere, anywhere, anywhere, anywhere,
        ],
        out_specs=(vmem, vmem),
        scratch_shapes=[
            pltpu.VMEM((1, 2), jnp.float32),
            pltpu.VMEM((2, 256), jnp.bfloat16),
            pltpu.VMEM((2, 256), jnp.bfloat16),
            pltpu.VMEM((2, 256), jnp.bfloat16),
            pltpu.VMEM((1, 256), jnp.float32),
            pltpu.VMEM((1, 128), jnp.float32),
            pltpu.VMEM((2, 8, TOK, FEAT), jnp.bfloat16),
            pltpu.VMEM((4096, 256), jnp.bfloat16),
            pltpu.VMEM((4096, 256), jnp.bfloat16),
            pltpu.VMEM((2, TOK, 256), jnp.float32),
            pltpu.VMEM((TOK, 128), jnp.float32),
            pltpu.VMEM((TOK, 128), jnp.float32),
            pltpu.VMEM((2, TOK, 128), jnp.float32),
            pltpu.VMEM((8, 128), jnp.float32),
            pltpu.VMEM((8, 128), jnp.float32),
            pltpu.VMEM((SP, 8, 128), jnp.bfloat16),
            pltpu.VMEM((2, 128), jnp.float32),
            pltpu.VMEM((SP, 8, 128), jnp.bfloat16),
            pltpu.VMEM((SP, 2, 128), jnp.float32),
            dma((6,)), dma((8, N)), dma((8, N)), dma((16, 2)), dma((2,)), dma,
            dma, dma, dma, dma, dma, dma, dma,
            dma, dma, dma, dma,
            pltpu.SemaphoreType.REGULAR((4,)),
        ],
        compiler_params=pltpu.CompilerParams(collective_id=0, has_side_effects=True),
    )(
        decay_exponent[None, :], layer_input, key_weight, value_weight,
        query_new, key_new, value_new, norm_gain[None, :], inverse,
    )
    return (
        state.reshape(2, 2, 4, 128).astype(jnp.bfloat16),
        read.astype(jnp.bfloat16),
    )


def solution(mesh):
    in_specs = (
        P("sp", "tp"), P(None, "tp"), P(None, "tp"), P("tp"),
        P(None, "tp"), P(None, "tp"), P(None, "tp"), P("tp"),
    )
    out_specs = (P(None, "tp", "sp", None), P(None, "tp"))
    return jax.shard_map(
        on_device, mesh=mesh, in_specs=in_specs, out_specs=out_specs, check_vma=False
    )
```

```python
import jax
import jax.numpy as jnp
import numpy as np
from jax import lax
from jax.experimental import pallas as pl
from jax.experimental.pallas import tpu as pltpu
from jax.sharding import PartitionSpec as P

MESH = pl.DeviceIdType.MESH
N = 3
TOK = 1024
FEAT = 256
STARTS = (0, 352, 688, 1024)
SP = 32
Z = 16

NATIVE_ORDER = [(0, 0), (1, 0), (2, 0), (1, 1), (2, 1), (2, 2), (2, 3)]
FOREIGN_ORDER = [
    (0, 0, 0), (0, 0, 1), (1, 0, 2), (0, 0, 2), (1, 0, 0), (2, 0, 1), (1, 0, 1), (1, 1, 0), (2, 1, 1), (2, 0, 0),
    (2, 0, 2), (1, 1, 2), (1, 1, 1), (2, 1, 2), (2, 2, 1), (2, 1, 0), (2, 2, 2), (2, 2, 0), (2, 3, 1), (2, 3, 2),
    (2, 3, 0),
]
OWN_SENDS = [
    [(0, 0, 0)],
    [(0, 0, 1), (1, 0, 0)],
    [(0, 0, 2), (1, 0, 1), (1, 0, 2), (2, 0, 1), (2, 0, 0)],
]
SENDS = {
    (0, 0, 0): [(1, 1, 0), (2, 0, 2)],
    (0, 0, 1): [(1, 1, 1), (2, 1, 1), (2, 1, 0)],
    (0, 0, 2): [(1, 1, 2), (2, 1, 2)],
}
for _j in range(N):
    SENDS[1, 0, _j] = [(2, 2, _j)]
    SENDS[1, 1, _j] = [(2, 3, _j)]


def turn(mask, j):
    return ((mask << j) | (mask >> (N - j))) & (2**N - 1)


def piece(j):
    return pl.ds(STARTS[j], STARTS[j + 1] - STARTS[j])


def landing(k, r, j):
    return turn(r, j) | (1 << (j + k) % N)


def native_slot(slot):
    k, r = NATIVE_ORDER[slot]
    out = []
    for d in range(N):
        j = (d - k) % N
        sent = r | (1 << k)
        onward = [(j + kk) % N for kk, rr in NATIVE_ORDER if rr == sent]
        out.append((j, turn(r, j), landing(k, r, j), onward))
    return out


def flip1(v):
    return v + 1 - 2 * (v % 2)


def cos_sin(position, inverse):
    angle = position * inverse
    lane = lax.broadcasted_iota(jnp.int32, angle.shape, 1)
    quarter = jnp.floor(angle * 0.6366197723675814 + 0.5)
    rest = ((angle - quarter * 1.5703125) - quarter * 4.837512969970703125e-4) - quarter * 7.54978995489188e-8
    turns = quarter.astype(jnp.int32) - jnp.where(lane >= 64, 1, 0)
    turns = jnp.bitwise_and(turns, 3)
    square = rest * rest
    sine = rest + rest * square * (-1.6666654611e-1 + square * (8.3321608736e-3 - square * 1.9515295891e-4))
    cosine = 1.0 - 0.5 * square + square * square * (
        4.166664568298827e-2 + square * (-1.388731625493765e-3 + square * 2.443315711809948e-5)
    )
    value = jnp.where(jnp.bitwise_and(turns, 1) == 1, sine, cosine)
    negative = jnp.logical_or(turns == 1, turns == 2)
    return jnp.where(negative, -value, value)


def kernel(
    decay_hbm, x_hbm, wk_hbm, wv_hbm, query_hbm, key_hbm, value_hbm, gain_hbm, inverse_hbm,
    state_out, read_out,
    decay, query, key_new, value_new, gain, inverse,
    xbuf, weights, acc, cosine, sine, weight, mini_own, mini_got, send_state, send_read, got_state, got_read,
    small_sem, mine_sem, sib_sem, w_sem, wl_sem, mini_sem,
    link_send, sib_send, x_send, w_send, wz_send, wzz_send, mini_send,
    tail_send, tail_send2, tail_recv, tail_recv2, chain,
):
    sp = lax.axis_index("sp")
    tp = lax.axis_index("tp")
    z, core = sp // 2, sp % 2
    y, x = tp // 4, tp % 4
    group = 1 - (x + 1) // 2 % 2
    block = z * 2 + group
    links = [
        (sp, y * 4 + 3 - x),
        (sp, flip1(y) * 4 + x),
        (sp, (3 - y) * 4 + x),
    ]
    sibling = (z * 2 + 1 - core, tp)
    partner_tp = y * 4 + flip1(x)
    partner = (z * 2 + 1 - core, partner_tp)

    def along_z(step):
        return ((z + step + Z) % Z * 2 + core, tp)

    def signal(semaphore, device):
        pl.semaphore_signal(semaphore, inc=1, device_id=device, device_id_type=MESH)

    def remote(src, dst, send, recv, device):
        return pltpu.make_async_remote_copy(
            src_ref=src, dst_ref=dst, send_sem=send, recv_sem=recv, device_id=device, device_id_type=MESH
        )

    def arrived(ref, semaphore):
        pltpu.make_async_copy(ref, ref, semaphore).wait()

    is_native = core == group
    is_foreign = core != group

    barrier = pltpu.get_barrier_semaphore()
    near = links + [sibling, partner, along_z(1), along_z(-1), along_z(2), along_z(-2)]
    for device in near:
        signal(barrier, device)

    @pl.when(is_native)
    def _():
        for j in range(N):
            pltpu.make_async_copy(x_hbm.at[piece(j)], xbuf.at[0, 0, piece(j)], mine_sem.at[0, j]).start()

    smalls = [
        pltpu.make_async_copy(src, dst, small_sem.at[i])
        for i, (src, dst) in enumerate((
            (decay_hbm, decay), (query_hbm, query), (key_hbm, key_new), (value_hbm, value_new),
            (gain_hbm, gain), (inverse_hbm, inverse),
        ))
    ]
    for copy in smalls:
        copy.start()

    @pl.when(is_native)
    def _():
        pltpu.make_async_copy(wk_hbm, weights.at[0], wl_sem.at[0]).start()
        pltpu.make_async_copy(wv_hbm, weights.at[1], wl_sem.at[1]).start()

    pl.semaphore_wait(barrier, len(near))

    def fill_mini():
        for copy in smalls:
            copy.wait()
        for h in range(2):
            mini_own[h : h + 1, :] = jnp.broadcast_to(decay[:, h : h + 1], (1, 128))
            mini_own[2 + 2 * h : 4 + 2 * h, :] = query[:, h * 128 : h * 128 + 128].astype(jnp.float32)

    steps = [
        [sibling, partner, along_z(1), along_z(-1), along_z(2), along_z(-2)],
        [along_z(2), along_z(-2)],
        [sibling],
        [along_z(4), along_z(-4)],
    ]

    def chain_signal(n):
        for device in steps[n]:
            signal(chain.at[n], device)

    def chain_wait(n):
        pl.semaphore_wait(chain.at[n], len(steps[n]))

    def send_on(mask, j, over):
        for d in over:
            remote(
                xbuf.at[0, mask, piece(j)], xbuf.at[0, mask | (1 << d), piece(j)],
                link_send, mine_sem.at[mask | (1 << d), j], links[d],
            ).start()

    def to_sibling(mask, j):
        remote(
            xbuf.at[0, mask, piece(j)], xbuf.at[1, mask, piece(j)], sib_send, sib_sem.at[mask, j], sibling
        ).start()

    def column_of(mask, native_part):
        b = [mask // 2**i % 2 for i in range(N)]
        cx = x + b[0] * (3 - 2 * x)
        cy = y + b[1] * (1 - 2 * (y % 2))
        cy = cy + b[2] * (3 - 2 * cy)
        return cy * 4 + (cx if native_part else flip1(cx))

    def weight_rows(t):
        return pl.ds(pl.multiple_of(t * FEAT, FEAT), FEAT)

    def add_product(part, mask, j, native_part, first=False):
        wrows = weight_rows(column_of(mask, native_part))
        block_x = xbuf[part, mask, piece(j), :]
        for i in range(2):
            product = jnp.dot(block_x, weights[i, wrows, :], preferred_element_type=jnp.float32)
            if first:
                acc[i, piece(j), :] = product
            else:
                acc[i, piece(j), :] += product

    def mine_arrived(mask, j):
        arrived(xbuf.at[0, mask, piece(j)], mine_sem.at[mask, j])

    def sib_arrived(mask, j):
        arrived(xbuf.at[1, mask, piece(j)], sib_sem.at[mask, j])

    def tables(mini):
        @pl.loop(0, 4)
        def _(c):
            rows = pl.ds(pl.multiple_of(c * 256, 256), 256)
            first = (block % 16) * TOK + c * 256
            position = (lax.broadcasted_iota(jnp.int32, (256, 128), 0) + first).astype(jnp.float32)
            table = cos_sin(position, inverse[...])
            swapped = pltpu.roll(table, 64, axis=1)
            low = lax.broadcasted_iota(jnp.int32, (256, 128), 1) < 64
            cosine[rows, :] = jnp.where(low, table, swapped)
            sine[rows, :] = jnp.where(low, -swapped, table)
            distance = 16384 - 1.0 - position
            for h in range(2):
                weight[h, rows, :] = jnp.exp(mini[h : h + 1, :] * distance)

    @pl.when(is_native)
    def _():
        for j in range(N):
            mine_arrived(0, j)
        for slot in range(3):
            for d in range(N):
                send_on(0, (d - slot) % N, [d])
        for j in range(N):
            to_sibling(0, j)
        chain_signal(0)
        fill_mini()
        mini_got[...] = mini_own[...]
        tables(mini_got)
        arrived(weights.at[0], wl_sem.at[0])
        arrived(weights.at[1], wl_sem.at[1])
        for j in range(N):
            add_product(0, 0, j, True, first=True)
        for slot in range(7):
            got = native_slot(slot)
            for j, _, mask, onward in got:
                mine_arrived(mask, j)
                send_on(mask, j, onward)
                to_sibling(mask, j)
            if slot in (1, 3, 5):
                chain_wait(slot // 2)
                chain_signal(slot // 2 + 1)
            for j, _, mask, _ in got:
                add_product(0, mask, j, True)
        for j in range(N):
            sib_arrived(0, j)
            add_product(1, 0, j, False)
        for k, r, j in FOREIGN_ORDER:
            sib_arrived(landing(k, r, j), j)
            add_product(1, landing(k, r, j), j, False)
        chain_wait(3)

    @pl.when(is_foreign)
    def _():
        quarter = z % 4
        opposite = (z + 2) % 4

        other = flip1(x)
        mine_first = (x, 3 - x, other, 3 - other)
        theirs_first = (other, 3 - other, x, 3 - x)

        def direct(row, i):
            t = row * 4 + theirs_first[i]
            rows = weight_rows(t)
            for n, src in enumerate((wk_hbm, wv_hbm)):
                remote(src.at[rows], weights.at[n, rows], w_send, w_sem.at[t], partner).start()

        def pass_weights(t, step, semaphore):
            ref = weights.at[:, weight_rows(t)]
            remote(ref, ref, semaphore, w_sem.at[t], along_z(step)).start()

        def exchange(j):
            remote(x_hbm.at[piece(j)], xbuf.at[0, 0, piece(j)], x_send, mine_sem.at[0, j], partner).start()

        def send_messages(messages):
            for k, r, j in messages:
                send_on(turn(r, j), j, [(j + k) % N])

        def own_piece(j):
            mine_arrived(0, j)
            send_messages(OWN_SENDS[j])
            to_sibling(0, j)

        waiting = list(FOREIGN_ORDER)
        ready = []

        def receive(*expected):
            k, r, j = waiting.pop(0)
            assert (k, r, j) == expected
            mask = landing(k, r, j)
            mine_arrived(mask, j)
            send_messages(SENDS.get((k, r, j), []))
            to_sibling(mask, j)
            ready.append((mask, j))

        def foreign_product(count):
            for _ in range(count):
                mask, j = ready.pop(0)
                add_product(0, mask, j, False)

        def native_product(slot):
            for j, _, mask, _ in native_slot(slot):
                sib_arrived(mask, j)
                add_product(1, mask, j, True)

        def weights_arrived(t):
            arrived(weights.at[:, weight_rows(t)], w_sem.at[t])

        def own_weights(i):
            t = quarter * 4 + mine_first[i]
            weights_arrived(t)
            pass_weights(t, 1, wz_send)
            pass_weights(t, -1, wz_send)

        def pass_on(step):
            t = (z + step) % 4 * 4 + mine_first[1 if step == 1 else 0]
            weights_arrived(t)
            pass_weights(t, -step, wzz_send)

        def row_weights(step, *indices):
            for i in indices:
                weights_arrived((z + step) % 4 * 4 + mine_first[i])

        direct(quarter, 0)
        direct(quarter, 1)
        fill_mini()
        for j in range(N):
            exchange(j)
        remote(mini_own, mini_got, mini_send, mini_sem, partner).start()
        direct(quarter, 2)
        direct(quarter, 3)
        direct(opposite, 2)
        direct(opposite, 3)
        chain_signal(0)
        own_weights(0)
        own_weights(1)
        chain_wait(0)
        chain_signal(1)
        own_piece(0)
        pass_on(-1)
        own_piece(1)
        pass_on(1)
        own_piece(2)
        chain_wait(1)
        chain_signal(2)
        arrived(mini_got, mini_sem)
        tables(mini_got)
        receive(0, 0, 0)
        own_weights(2)
        receive(0, 0, 1)
        row_weights(1, 0)
        row_weights(3, 1)
        row_weights(2, 0, 1)
        receive(1, 0, 2)
        receive(0, 0, 2)
        chain_wait(2)
        chain_signal(3)
        for j in range(N):
            sib_arrived(0, j)
            add_product(1, 0, j, True, first=True)
        native_product(0)
        native_product(1)
        own_weights(3)
        receive(1, 0, 0)
        receive(2, 0, 1)
        receive(1, 0, 1)
        native_product(2)
        native_product(3)
        native_product(4)
        receive(1, 1, 0)
        receive(2, 1, 1)
        receive(2, 0, 0)
        native_product(5)
        native_product(6)
        receive(2, 0, 2)
        receive(1, 1, 2)
        receive(1, 1, 1)
        receive(2, 1, 2)
        row_weights(1, 2, 3)
        row_weights(3, 2, 3)
        row_weights(2, 2, 3)
        for j in range(N):
            add_product(0, 0, j, False)
        foreign_product(4)
        receive(2, 2, 1)
        receive(2, 1, 0)
        foreign_product(6)
        receive(2, 2, 2)
        receive(2, 2, 0)
        foreign_product(5)
        receive(2, 3, 1)
        foreign_product(3)
        receive(2, 3, 2)
        receive(2, 3, 0)
        foreign_product(3)
        chain_wait(3)

    scale = 128 ** (-0.5)
    states = []
    for h in range(2):
        cols = pl.ds(h * 128, 128)
        k = acc[0, :, cols]
        turned = k * cosine[...] + pltpu.roll(k, 64, axis=1) * sine[...]
        keys = (turned * scale).astype(jnp.bfloat16)
        weighted = (keys.astype(jnp.float32) * weight[h]).astype(jnp.bfloat16)
        values = acc[1, :, cols].astype(jnp.bfloat16)
        states.append(
            lax.dot_general(
                weighted, values, (((0,), (0,)), ((), ())), preferred_element_type=jnp.float32
            )
        )
    top = lax.broadcasted_iota(jnp.int32, (8, 128), 0) < 4
    for i in range(16):
        a = states[0][8 * i : 8 * i + 8]
        b = states[1][8 * i : 8 * i + 8]
        send_state[2 * i] = jnp.where(top, a, pltpu.roll(b, 4, axis=0)).astype(jnp.bfloat16)
        send_state[2 * i + 1] = jnp.where(top, pltpu.roll(a, 4, axis=0), b).astype(jnp.bfloat16)
    prompt = z // 8
    for h in range(2):
        rows = pl.ds(2 + 2 * h, 2)
        both = jnp.dot(mini_got[rows, :], states[h], precision=lax.Precision.HIGHEST, preferred_element_type=jnp.float32)
        send_read[h : h + 1, :] = jnp.where(prompt == 0, both[0:1], both[1:2])

    target_tp = jnp.where(is_native, tp, partner_tp)

    def tail(step, other):
        target = (z + step + Z) % Z * 2 + (1 - core if other else core)
        device = (target, target_tp)
        remote(send_state.at[target], got_state.at[block], tail_send, tail_recv, device).start()
        remote(send_read, got_read.at[block], tail_send2, tail_recv2, device).start()

    far = [8]
    for s in range(7, 0, -1):
        far += [s, -s]
    for step in far:
        for other in (False, True):
            tail(step, other)
    tail(0, True)

    @pl.when(is_native)
    def _():
        pltpu.make_async_copy(send_state.at[sp], got_state.at[block], tail_recv).start()
        pltpu.make_async_copy(send_read, got_read.at[block], tail_recv2).start()

    @pl.when(is_foreign)
    def _():
        tail(0, False)

    queries = query[...].astype(jnp.float32)
    dots = queries * key_new[...].astype(jnp.float32)
    news = value_new[...].astype(jnp.float32)
    own_terms = [
        jnp.sum(dots[:, h * 128 : h * 128 + 128], axis=1, keepdims=True) * news[:, h * 128 : h * 128 + 128]
        for h in range(2)
    ]

    arrived(got_read, tail_recv2)
    carried = [jnp.sum(got_read[16 * s : 16 * s + 16], axis=0) for s in range(2)]
    for h in range(2):
        scaled = jnp.exp(mini_own[h : h + 1, :])
        rows = jnp.concatenate([carried[0][h : h + 1], carried[1][h : h + 1]], axis=0)
        mixed = scaled * rows + own_terms[h]
        normed = mixed * lax.rsqrt(jnp.mean(mixed * mixed, axis=1, keepdims=True) + 1e-06)
        read_out[:, h * 128 : h * 128 + 128] = normed * gain[:, h * 128 : h * 128 + 128]
    arrived(got_state, tail_recv)
    for s in range(2):
        total = jnp.zeros((8, 128), jnp.float32)
        for i in range(16):
            total = total + got_state[16 * s + i].astype(jnp.float32)
        state_out[s] = total

    arrived(xbuf.at[0, pl.ds(0, 7)], link_send)
    arrived(xbuf.at[0], sib_send)

    @pl.when(is_native)
    def _():
        arrived(got_state.at[pl.ds(0, 31)], tail_send)
        arrived(got_read.at[pl.ds(0, 31)], tail_send2)

    @pl.when(is_foreign)
    def _():
        arrived(got_state, tail_send)
        arrived(got_read, tail_send2)
        arrived(xbuf.at[0, 0], x_send)
        arrived(mini_own, mini_send)
        arrived(weights.at[:, pl.ds(0, 1536)], w_send)
        arrived(weights.at[0], wz_send)
        arrived(weights.at[0, pl.ds(0, 1024)], wzz_send)


def on_device(
    layer_input, key_weight, value_weight, decay_exponent, query_new, key_new, value_new, norm_gain
):
    inverse = (1.0 / 10000.0 ** (np.arange(64) / 63.0)).astype(np.float32)
    inverse = jnp.asarray(np.concatenate([inverse, inverse])[None, :])
    vmem = pl.BlockSpec(memory_space=pltpu.VMEM)
    anywhere = pl.BlockSpec(memory_space=pl.ANY)
    dma = pltpu.SemaphoreType.DMA
    state, read = pl.pallas_call(
        kernel,
        name="gather_project_reduce",
        out_shape=(
            pltpu.VMEM((2, 8, 128), jnp.float32),
            pltpu.VMEM((2, 256), jnp.float32),
        ),
        in_specs=[
            anywhere, anywhere, anywhere, anywhere, anywhere, anywhere, anywhere, anywhere, anywhere,
        ],
        out_specs=(vmem, vmem),
        scratch_shapes=[
            pltpu.VMEM((1, 2), jnp.float32),
            pltpu.VMEM((2, 256), jnp.bfloat16),
            pltpu.VMEM((2, 256), jnp.bfloat16),
            pltpu.VMEM((2, 256), jnp.bfloat16),
            pltpu.VMEM((1, 256), jnp.float32),
            pltpu.VMEM((1, 128), jnp.float32),
            pltpu.VMEM((2, 8, TOK, FEAT), jnp.bfloat16),
            pltpu.VMEM((2, 4096, 256), jnp.bfloat16),
            pltpu.VMEM((2, TOK, 256), jnp.float32),
            pltpu.VMEM((TOK, 128), jnp.float32),
            pltpu.VMEM((TOK, 128), jnp.float32),
            pltpu.VMEM((2, TOK, 128), jnp.float32),
            pltpu.VMEM((8, 128), jnp.float32),
            pltpu.VMEM((8, 128), jnp.float32),
            pltpu.VMEM((SP, 8, 128), jnp.bfloat16),
            pltpu.VMEM((2, 128), jnp.float32),
            pltpu.VMEM((SP, 8, 128), jnp.bfloat16),
            pltpu.VMEM((SP, 2, 128), jnp.float32),
            dma((6,)), dma((8, N)), dma((8, N)), dma((16,)), dma((2,)), dma,
            dma, dma, dma, dma, dma, dma, dma,
            dma, dma, dma, dma,
            pltpu.SemaphoreType.REGULAR((4,)),
        ],
        compiler_params=pltpu.CompilerParams(collective_id=0, has_side_effects=True),
    )(
        decay_exponent[None, :], layer_input, key_weight, value_weight,
        query_new, key_new, value_new, norm_gain[None, :], inverse,
    )
    return (
        state.reshape(2, 2, 4, 128).astype(jnp.bfloat16),
        read.astype(jnp.bfloat16),
    )


def solution(mesh):
    in_specs = (
        P("sp", "tp"), P(None, "tp"), P(None, "tp"), P("tp"),
        P(None, "tp"), P(None, "tp"), P(None, "tp"), P("tp"),
    )
    out_specs = (P(None, "tp", "sp", None), P(None, "tp"))
    return jax.shard_map(
        on_device, mesh=mesh, in_specs=in_specs, out_specs=out_specs, check_vma=False
    )
```

```python
import jax
import jax.numpy as jnp
import numpy as np
from jax import lax
from jax.experimental import pallas as pl
from jax.experimental.pallas import tpu as pltpu
from jax.sharding import PartitionSpec as P

MESH = pl.DeviceIdType.MESH
N = 3
TOK = 1024
FEAT = 256
STARTS = (0, 336, 672, 1024)
SP = 32
Z = 16

NATIVE_ORDER = [(0, 0), (1, 0), (2, 0), (1, 1), (2, 1), (2, 2), (2, 3)]
FOREIGN_ORDER = [
    (0, 0, 0), (0, 0, 1), (1, 0, 2), (0, 0, 2), (1, 0, 0), (2, 0, 1), (1, 0, 1), (1, 1, 0), (2, 1, 1), (1, 1, 1),
    (2, 0, 2), (1, 1, 2), (2, 0, 0), (2, 1, 2), (2, 2, 1), (2, 1, 0), (2, 2, 2), (2, 2, 0), (2, 3, 2), (2, 3, 1),
    (2, 3, 0),
]
OWN_SENDS = [
    [(0, 0, 0)],
    [(0, 0, 1), (1, 0, 0)],
    [(0, 0, 2), (1, 0, 1), (1, 0, 2), (2, 0, 1)],
]
SENDS = {
    (0, 0, 0): [(1, 1, 0), (2, 0, 2)],
    (0, 0, 1): [(1, 1, 1), (2, 0, 0), (2, 1, 1), (2, 1, 0)],
    (0, 0, 2): [(1, 1, 2), (2, 1, 2)],
}
for _j in range(N):
    SENDS[1, 0, _j] = [(2, 2, _j)]
    SENDS[1, 1, _j] = [(2, 3, _j)]


def turn(mask, j):
    return ((mask << j) | (mask >> (N - j))) & (2**N - 1)


def piece(j):
    return pl.ds(STARTS[j], STARTS[j + 1] - STARTS[j])


def landing(k, r, j):
    return turn(r, j) | (1 << (j + k) % N)


def native_slot(slot):
    k, r = NATIVE_ORDER[slot]
    out = []
    for d in range(N):
        j = (d - k) % N
        sent = r | (1 << k)
        onward = [(j + kk) % N for kk, rr in NATIVE_ORDER if rr == sent]
        out.append((j, turn(r, j), landing(k, r, j), onward))
    return out


def flip1(v):
    return v + 1 - 2 * (v % 2)


def cos_sin(position, inverse):
    angle = position * inverse
    lane = lax.broadcasted_iota(jnp.int32, angle.shape, 1)
    quarter = jnp.floor(angle * 0.6366197723675814 + 0.5)
    rest = ((angle - quarter * 1.5703125) - quarter * 4.837512969970703125e-4) - quarter * 7.54978995489188e-8
    turns = quarter.astype(jnp.int32) - jnp.where(lane >= 64, 1, 0)
    turns = jnp.bitwise_and(turns, 3)
    square = rest * rest
    sine = rest + rest * square * (-1.6666654611e-1 + square * (8.3321608736e-3 - square * 1.9515295891e-4))
    cosine = 1.0 - 0.5 * square + square * square * (
        4.166664568298827e-2 + square * (-1.388731625493765e-3 + square * 2.443315711809948e-5)
    )
    value = jnp.where(jnp.bitwise_and(turns, 1) == 1, sine, cosine)
    negative = jnp.logical_or(turns == 1, turns == 2)
    return jnp.where(negative, -value, value)


def kernel(
    decay_hbm, x_hbm, wk_hbm, wv_hbm, query_hbm, key_hbm, value_hbm, gain_hbm, inverse_hbm,
    state_out, read_out,
    decay, query, key_new, value_new, gain, inverse,
    xbuf, weights, acc, state, cosine, sine, weight, mini_own, mini_got, send_state, send_read, got_state, got_read,
    small_sem, mine_sem, sib_sem, w_sem, wl_sem, mini_sem,
    link_send, sib_send, x_send, w_send, wz_send, wzz_send, mini_send,
    tail_send, tail_send2, tail_recv, tail_recv2, chain,
):
    sp = lax.axis_index("sp")
    tp = lax.axis_index("tp")
    z, core = sp // 2, sp % 2
    y, x = tp // 4, tp % 4
    group = 1 - (x + 1) // 2 % 2
    block = z * 2 + group
    links = [
        (sp, y * 4 + 3 - x),
        (sp, flip1(y) * 4 + x),
        (sp, (3 - y) * 4 + x),
    ]
    sibling = (z * 2 + 1 - core, tp)
    partner_tp = y * 4 + flip1(x)
    partner = (z * 2 + 1 - core, partner_tp)

    def along_z(step):
        return ((z + step + Z) % Z * 2 + core, tp)

    def signal(semaphore, device):
        pl.semaphore_signal(semaphore, inc=1, device_id=device, device_id_type=MESH)

    def remote(src, dst, send, recv, device):
        return pltpu.make_async_remote_copy(
            src_ref=src, dst_ref=dst, send_sem=send, recv_sem=recv, device_id=device, device_id_type=MESH
        )

    def arrived(ref, semaphore):
        pltpu.make_async_copy(ref, ref, semaphore).wait()

    is_native = core == group
    is_foreign = core != group

    barrier = pltpu.get_barrier_semaphore()
    near = links + [sibling, partner, along_z(1), along_z(-1)]
    for device in near:
        signal(barrier, device)

    @pl.when(is_native)
    def _():
        for j in range(N):
            pltpu.make_async_copy(x_hbm.at[piece(j)], xbuf.at[0, 0, piece(j)], mine_sem.at[0, j]).start()

    smalls = [
        pltpu.make_async_copy(src, dst, small_sem.at[i])
        for i, (src, dst) in enumerate((
            (decay_hbm, decay), (query_hbm, query), (key_hbm, key_new), (value_hbm, value_new),
            (gain_hbm, gain), (inverse_hbm, inverse),
        ))
    ]
    for copy in smalls:
        copy.start()

    @pl.when(is_native)
    def _():
        pltpu.make_async_copy(wk_hbm, weights.at[0], wl_sem.at[0]).start()
        pltpu.make_async_copy(wv_hbm, weights.at[1], wl_sem.at[1]).start()

    pl.semaphore_wait(barrier, len(near))

    def fill_mini():
        for copy in smalls:
            copy.wait()
        for h in range(2):
            mini_own[h : h + 1, :] = jnp.broadcast_to(decay[:, h : h + 1], (1, 128))
            mini_own[2 + 2 * h : 4 + 2 * h, :] = query[:, h * 128 : h * 128 + 128].astype(jnp.float32)

    steps = [
        [sibling, partner, along_z(1), along_z(-1)],
        [along_z(2), along_z(-2)],
        [sibling],
        [along_z(3), along_z(-3)],
        [along_z(6), along_z(-6)],
    ]

    def chain_signal(n):
        for device in steps[n]:
            signal(chain.at[n], device)

    def chain_wait(n):
        pl.semaphore_wait(chain.at[n], len(steps[n]))

    def send_on(mask, j, over):
        for d in over:
            remote(
                xbuf.at[0, mask, piece(j)], xbuf.at[0, mask | (1 << d), piece(j)],
                link_send, mine_sem.at[mask | (1 << d), j], links[d],
            ).start()

    def to_sibling(mask, j):
        remote(
            xbuf.at[0, mask, piece(j)], xbuf.at[1, mask, piece(j)], sib_send, sib_sem.at[mask, j], sibling
        ).start()

    def column_of(mask, native_part):
        b = [mask // 2**i % 2 for i in range(N)]
        cx = x + b[0] * (3 - 2 * x)
        cy = y + b[1] * (1 - 2 * (y % 2))
        cy = cy + b[2] * (3 - 2 * cy)
        return cy * 4 + (cx if native_part else flip1(cx))

    def weight_rows(t):
        return pl.ds(pl.multiple_of(t * FEAT, FEAT), FEAT)

    def add_product(part, mask, j, native_part, first=False):
        wrows = weight_rows(column_of(mask, native_part))
        block_x = xbuf[part, mask, piece(j), :]
        for i in range(2):
            product = jnp.dot(block_x, weights[i, wrows, :], preferred_element_type=jnp.float32)
            if first:
                acc[i, piece(j), :] = product
            else:
                acc[i, piece(j), :] += product

    scale = 128 ** (-0.5)

    def add_state(j, first=False):
        rows = piece(j)
        for h in range(2):
            cols = pl.ds(h * 128, 128)
            k = acc[0, rows, cols]
            turned = k * cosine[rows, :] + pltpu.roll(k, 64, axis=1) * sine[rows, :]
            keys = (turned * scale).astype(jnp.bfloat16)
            weighted = (keys.astype(jnp.float32) * weight[h, rows, :]).astype(jnp.bfloat16)
            values = acc[1, rows, cols].astype(jnp.bfloat16)
            part = lax.dot_general(
                weighted, values, (((0,), (0,)), ((), ())), preferred_element_type=jnp.float32
            )
            if first:
                state[h] = part
            else:
                state[h] += part

    def mine_arrived(mask, j):
        arrived(xbuf.at[0, mask, piece(j)], mine_sem.at[mask, j])

    def sib_arrived(mask, j):
        arrived(xbuf.at[1, mask, piece(j)], sib_sem.at[mask, j])

    def tables(mini):
        @pl.loop(0, 4)
        def _(c):
            rows = pl.ds(pl.multiple_of(c * 256, 256), 256)
            first = (block % 16) * TOK + c * 256
            position = (lax.broadcasted_iota(jnp.int32, (256, 128), 0) + first).astype(jnp.float32)
            table = cos_sin(position, inverse[...])
            swapped = pltpu.roll(table, 64, axis=1)
            low = lax.broadcasted_iota(jnp.int32, (256, 128), 1) < 64
            cosine[rows, :] = jnp.where(low, table, swapped)
            sine[rows, :] = jnp.where(low, -swapped, table)
            distance = 16384 - 1.0 - position
            for h in range(2):
                weight[h, rows, :] = jnp.exp(mini[h : h + 1, :] * distance)

    @pl.when(is_native)
    def _():
        for j in range(N):
            mine_arrived(0, j)
        for slot in range(3):
            for d in range(N):
                send_on(0, (d - slot) % N, [d])
        for j in range(N):
            to_sibling(0, j)
        chain_signal(0)
        fill_mini()
        mini_got[...] = mini_own[...]
        tables(mini_got)
        arrived(weights.at[0], wl_sem.at[0])
        arrived(weights.at[1], wl_sem.at[1])
        for j in range(N):
            add_product(0, 0, j, True, first=True)
        for slot in range(7):
            got = native_slot(slot)
            for j, _, mask, onward in got:
                mine_arrived(mask, j)
                send_on(mask, j, onward)
                to_sibling(mask, j)
            if slot in (1, 3, 5):
                chain_wait(slot // 2)
                chain_signal(slot // 2 + 1)
            for j, _, mask, _ in got:
                add_product(0, mask, j, True)
        for j in range(N):
            sib_arrived(0, j)
            add_product(1, 0, j, False)
        for n, (k, r, j) in enumerate(FOREIGN_ORDER):
            if n == 10:
                chain_wait(3)
                chain_signal(4)
            sib_arrived(landing(k, r, j), j)
            add_product(1, landing(k, r, j), j, False)
            if (k, r) == (2, 3):
                add_state(j, first=j == 2)
        chain_wait(4)

    @pl.when(is_foreign)
    def _():
        quarter = z % 4
        opposite = (z + 2) % 4

        other = flip1(x)
        mine_first = (x, 3 - x, other, 3 - other)
        theirs_first = (other, 3 - other, x, 3 - x)

        def direct(row, i):
            t = row * 4 + theirs_first[i]
            rows = weight_rows(t)
            for n, src in enumerate((wk_hbm, wv_hbm)):
                remote(src.at[rows], weights.at[n, rows], w_send, w_sem.at[t], partner).start()

        def pass_weights(t, step, semaphore):
            ref = weights.at[:, weight_rows(t)]
            remote(ref, ref, semaphore, w_sem.at[t], along_z(step)).start()

        def exchange(j):
            remote(x_hbm.at[piece(j)], xbuf.at[0, 0, piece(j)], x_send, mine_sem.at[0, j], partner).start()

        def send_messages(messages):
            for k, r, j in messages:
                send_on(turn(r, j), j, [(j + k) % N])

        def own_piece(j):
            mine_arrived(0, j)
            send_messages(OWN_SENDS[j])
            to_sibling(0, j)

        waiting = list(FOREIGN_ORDER)
        ready = []

        def receive(*expected):
            k, r, j = waiting.pop(0)
            assert (k, r, j) == expected
            mask = landing(k, r, j)
            mine_arrived(mask, j)
            send_messages(SENDS.get((k, r, j), []))
            to_sibling(mask, j)
            ready.append((mask, j))

        def foreign_product(count):
            for _ in range(count):
                mask, j = ready.pop(0)
                add_product(0, mask, j, False)

        def native_product(slot):
            for j, _, mask, _ in native_slot(slot):
                sib_arrived(mask, j)
                add_product(1, mask, j, True)

        def weights_arrived(t):
            arrived(weights.at[:, weight_rows(t)], w_sem.at[t])

        def own_weights(i):
            t = quarter * 4 + mine_first[i]
            weights_arrived(t)
            pass_weights(t, 1, wz_send)
            pass_weights(t, -1, wz_send)

        def pass_on(step):
            t = (z + step) % 4 * 4 + mine_first[1 if step == 1 else 0]
            weights_arrived(t)
            pass_weights(t, -step, wzz_send)

        def row_weights(step, *indices):
            for i in indices:
                weights_arrived((z + step) % 4 * 4 + mine_first[i])

        direct(quarter, 0)
        direct(quarter, 1)
        fill_mini()
        for j in range(N):
            exchange(j)
        remote(mini_own, mini_got, mini_send, mini_sem, partner).start()
        direct(quarter, 2)
        direct(quarter, 3)
        direct(opposite, 2)
        direct(opposite, 3)
        chain_signal(0)
        own_weights(0)
        own_weights(1)
        chain_wait(0)
        chain_signal(1)
        own_piece(0)
        pass_on(-1)
        own_piece(1)
        pass_on(1)
        own_piece(2)
        chain_wait(1)
        chain_signal(2)
        arrived(mini_got, mini_sem)
        tables(mini_got)
        receive(0, 0, 0)
        own_weights(2)
        receive(0, 0, 1)
        row_weights(1, 0)
        row_weights(3, 1)
        row_weights(2, 0, 1)
        receive(1, 0, 2)
        receive(0, 0, 2)
        chain_wait(2)
        chain_signal(3)
        for j in range(N):
            sib_arrived(0, j)
            add_product(1, 0, j, True, first=True)
        native_product(0)
        native_product(1)
        own_weights(3)
        receive(1, 0, 0)
        receive(2, 0, 1)
        receive(1, 0, 1)
        native_product(2)
        native_product(3)
        native_product(4)
        receive(1, 1, 0)
        receive(2, 1, 1)
        receive(1, 1, 1)
        native_product(5)
        native_product(6)
        chain_wait(3)
        chain_signal(4)
        receive(2, 0, 2)
        receive(1, 1, 2)
        receive(2, 0, 0)
        receive(2, 1, 2)
        row_weights(1, 2, 3)
        row_weights(3, 2, 3)
        row_weights(2, 2, 3)
        for j in range(N):
            add_product(0, 0, j, False)
        foreign_product(4)
        receive(2, 2, 1)
        receive(2, 1, 0)
        foreign_product(6)
        receive(2, 2, 2)
        receive(2, 2, 0)
        foreign_product(8)
        receive(2, 3, 2)
        receive(2, 3, 1)
        receive(2, 3, 0)
        foreign_product(1)
        add_state(2, first=True)
        foreign_product(1)
        add_state(1)
        foreign_product(1)
        add_state(0)
        chain_wait(4)

    states = [state[0], state[1]]
    top = lax.broadcasted_iota(jnp.int32, (8, 128), 0) < 4
    for i in range(16):
        a = states[0][8 * i : 8 * i + 8]
        b = states[1][8 * i : 8 * i + 8]
        send_state[2 * i] = jnp.where(top, a, pltpu.roll(b, 4, axis=0)).astype(jnp.bfloat16)
        send_state[2 * i + 1] = jnp.where(top, pltpu.roll(a, 4, axis=0), b).astype(jnp.bfloat16)
    prompt = z // 8
    for h in range(2):
        rows = pl.ds(2 + 2 * h, 2)
        both = jnp.dot(mini_got[rows, :], states[h], precision=lax.Precision.HIGHEST, preferred_element_type=jnp.float32)
        send_read[h : h + 1, :] = jnp.where(prompt == 0, both[0:1], both[1:2])

    target_tp = jnp.where(is_native, tp, partner_tp)

    def tail(step, other):
        target = (z + step + Z) % Z * 2 + (1 - core if other else core)
        device = (target, target_tp)
        remote(send_state.at[target], got_state.at[block], tail_send, tail_recv, device).start()
        remote(send_read, got_read.at[block], tail_send2, tail_recv2, device).start()

    far = [8]
    for s in range(7, 0, -1):
        far += [s, -s]
    for step in far:
        for other in (False, True):
            tail(step, other)
    tail(0, True)

    @pl.when(is_native)
    def _():
        pltpu.make_async_copy(send_state.at[sp], got_state.at[block], tail_recv).start()
        pltpu.make_async_copy(send_read, got_read.at[block], tail_recv2).start()

    @pl.when(is_foreign)
    def _():
        tail(0, False)

    queries = query[...].astype(jnp.float32)
    dots = queries * key_new[...].astype(jnp.float32)
    news = value_new[...].astype(jnp.float32)
    own_terms = [
        jnp.sum(dots[:, h * 128 : h * 128 + 128], axis=1, keepdims=True) * news[:, h * 128 : h * 128 + 128]
        for h in range(2)
    ]

    arrived(got_read, tail_recv2)
    carried = [jnp.sum(got_read[16 * s : 16 * s + 16], axis=0) for s in range(2)]
    for h in range(2):
        scaled = jnp.exp(mini_own[h : h + 1, :])
        rows = jnp.concatenate([carried[0][h : h + 1], carried[1][h : h + 1]], axis=0)
        mixed = scaled * rows + own_terms[h]
        normed = mixed * lax.rsqrt(jnp.mean(mixed * mixed, axis=1, keepdims=True) + 1e-06)
        read_out[:, h * 128 : h * 128 + 128] = normed * gain[:, h * 128 : h * 128 + 128]
    arrived(got_state, tail_recv)
    for s in range(2):
        total = jnp.zeros((8, 128), jnp.float32)
        for i in range(16):
            total = total + got_state[16 * s + i].astype(jnp.float32)
        state_out[s] = total

    arrived(xbuf.at[0, pl.ds(0, 7)], link_send)
    arrived(xbuf.at[0], sib_send)

    @pl.when(is_native)
    def _():
        arrived(got_state.at[pl.ds(0, 31)], tail_send)
        arrived(got_read.at[pl.ds(0, 31)], tail_send2)

    @pl.when(is_foreign)
    def _():
        arrived(got_state, tail_send)
        arrived(got_read, tail_send2)
        arrived(xbuf.at[0, 0], x_send)
        arrived(mini_own, mini_send)
        arrived(weights.at[:, pl.ds(0, 1536)], w_send)
        arrived(weights.at[0], wz_send)
        arrived(weights.at[0, pl.ds(0, 1024)], wzz_send)


def on_device(
    layer_input, key_weight, value_weight, decay_exponent, query_new, key_new, value_new, norm_gain
):
    inverse = (1.0 / 10000.0 ** (np.arange(64) / 63.0)).astype(np.float32)
    inverse = jnp.asarray(np.concatenate([inverse, inverse])[None, :])
    vmem = pl.BlockSpec(memory_space=pltpu.VMEM)
    anywhere = pl.BlockSpec(memory_space=pl.ANY)
    dma = pltpu.SemaphoreType.DMA
    state, read = pl.pallas_call(
        kernel,
        name="gather_project_reduce",
        out_shape=(
            pltpu.VMEM((2, 8, 128), jnp.float32),
            pltpu.VMEM((2, 256), jnp.float32),
        ),
        in_specs=[
            anywhere, anywhere, anywhere, anywhere, anywhere, anywhere, anywhere, anywhere, anywhere,
        ],
        out_specs=(vmem, vmem),
        scratch_shapes=[
            pltpu.VMEM((1, 2), jnp.float32),
            pltpu.VMEM((2, 256), jnp.bfloat16),
            pltpu.VMEM((2, 256), jnp.bfloat16),
            pltpu.VMEM((2, 256), jnp.bfloat16),
            pltpu.VMEM((1, 256), jnp.float32),
            pltpu.VMEM((1, 128), jnp.float32),
            pltpu.VMEM((2, 8, TOK, FEAT), jnp.bfloat16),
            pltpu.VMEM((2, 4096, 256), jnp.bfloat16),
            pltpu.VMEM((2, TOK, 256), jnp.float32),
            pltpu.VMEM((2, 128, 128), jnp.float32),
            pltpu.VMEM((TOK, 128), jnp.float32),
            pltpu.VMEM((TOK, 128), jnp.float32),
            pltpu.VMEM((2, TOK, 128), jnp.float32),
            pltpu.VMEM((8, 128), jnp.float32),
            pltpu.VMEM((8, 128), jnp.float32),
            pltpu.VMEM((SP, 8, 128), jnp.bfloat16),
            pltpu.VMEM((2, 128), jnp.float32),
            pltpu.VMEM((SP, 8, 128), jnp.bfloat16),
            pltpu.VMEM((SP, 2, 128), jnp.float32),
            dma((6,)), dma((8, N)), dma((8, N)), dma((16,)), dma((2,)), dma,
            dma, dma, dma, dma, dma, dma, dma,
            dma, dma, dma, dma,
            pltpu.SemaphoreType.REGULAR((5,)),
        ],
        compiler_params=pltpu.CompilerParams(collective_id=0, has_side_effects=True),
    )(
        decay_exponent[None, :], layer_input, key_weight, value_weight,
        query_new, key_new, value_new, norm_gain[None, :], inverse,
    )
    return (
        state.reshape(2, 2, 4, 128).astype(jnp.bfloat16),
        read.astype(jnp.bfloat16),
    )


def solution(mesh):
    in_specs = (
        P("sp", "tp"), P(None, "tp"), P(None, "tp"), P("tp"),
        P(None, "tp"), P(None, "tp"), P(None, "tp"), P("tp"),
    )
    out_specs = (P(None, "tp", "sp", None), P(None, "tp"))
    return jax.shard_map(
        on_device, mesh=mesh, in_specs=in_specs, out_specs=out_specs, check_vma=False
    )
```

```python
import jax
import jax.numpy as jnp
import numpy as np
from jax import lax
from jax.experimental import pallas as pl
from jax.experimental.pallas import tpu as pltpu
from jax.sharding import PartitionSpec as P

MESH = pl.DeviceIdType.MESH
N = 3
TOK = 1024
FEAT = 256
STARTS = (0, 336, 672, 1024)
SP = 32
Z = 16

NATIVE_ORDER = [(0, 0), (1, 0), (2, 0), (1, 1), (2, 1), (2, 2), (2, 3)]
FOREIGN_ORDER = [
    (0, 0, 0), (0, 0, 1), (1, 0, 2), (0, 0, 2), (1, 0, 0), (2, 0, 1), (1, 0, 1), (1, 1, 0), (2, 1, 1), (1, 1, 1),
    (2, 0, 2), (1, 1, 2), (2, 0, 0), (2, 1, 2), (2, 2, 1), (2, 1, 0), (2, 2, 2), (2, 2, 0), (2, 3, 2), (2, 3, 1),
    (2, 3, 0),
]
BATCHES = []
for _size in (2, 2, 3, 3, 2, 2, 2, 2, 3):
    _first = sum(len(batch) for batch in BATCHES)
    BATCHES.append(FOREIGN_ORDER[_first : _first + _size])
OWN_SENDS = [
    [(0, 0, 0)],
    [(0, 0, 1), (1, 0, 0)],
    [(0, 0, 2), (1, 0, 1), (1, 0, 2), (2, 0, 1)],
]
SENDS = {
    (0, 0, 0): [(1, 1, 0), (2, 0, 2)],
    (0, 0, 1): [(1, 1, 1), (2, 0, 0), (2, 1, 1), (2, 1, 0)],
    (0, 0, 2): [(1, 1, 2), (2, 1, 2)],
}
for _j in range(N):
    SENDS[1, 0, _j] = [(2, 2, _j)]
    SENDS[1, 1, _j] = [(2, 3, _j)]


def turn(mask, j):
    return ((mask << j) | (mask >> (N - j))) & (2**N - 1)


def piece(j):
    return pl.ds(STARTS[j], STARTS[j + 1] - STARTS[j])


HALF = 176


def half(j, second):
    size = STARTS[j + 1] - STARTS[j]
    return pl.ds(STARTS[j] + HALF, size - HALF) if second else pl.ds(STARTS[j], HALF)


def landing(k, r, j):
    return turn(r, j) | (1 << (j + k) % N)


def native_slot(slot):
    k, r = NATIVE_ORDER[slot]
    out = []
    for d in range(N):
        j = (d - k) % N
        sent = r | (1 << k)
        onward = [(j + kk) % N for kk, rr in NATIVE_ORDER if rr == sent]
        out.append((j, turn(r, j), landing(k, r, j), onward))
    return out


def flip1(v):
    return v + 1 - 2 * (v % 2)


def cos_sin(position, inverse):
    angle = position * inverse
    lane = lax.broadcasted_iota(jnp.int32, angle.shape, 1)
    quarter = jnp.floor(angle * 0.6366197723675814 + 0.5)
    rest = ((angle - quarter * 1.5703125) - quarter * 4.837512969970703125e-4) - quarter * 7.54978995489188e-8
    turns = quarter.astype(jnp.int32) - jnp.where(lane >= 64, 1, 0)
    turns = jnp.bitwise_and(turns, 3)
    square = rest * rest
    sine = rest + rest * square * (-1.6666654611e-1 + square * (8.3321608736e-3 - square * 1.9515295891e-4))
    cosine = 1.0 - 0.5 * square + square * square * (
        4.166664568298827e-2 + square * (-1.388731625493765e-3 + square * 2.443315711809948e-5)
    )
    value = jnp.where(jnp.bitwise_and(turns, 1) == 1, sine, cosine)
    negative = jnp.logical_or(turns == 1, turns == 2)
    return jnp.where(negative, -value, value)


def kernel(
    decay_hbm, x_hbm, wk_hbm, wv_hbm, query_hbm, key_hbm, value_hbm, gain_hbm, inverse_hbm,
    state_out, read_out,
    decay, query, key_new, value_new, gain, inverse,
    xbuf, weights, acc, cosine, sine, weight, mini_own, mini_got, send_state, send_read, got_state, got_read,
    small_sem, mine_sem, last_sem, sib_sem, w_sem, wl_sem, mini_sem,
    link_send, sib_send, x_send, w_send, wz_send, wzz_send, mini_send,
    tail_send, tail_send2, tail_recv, tail_recv2, chain,
):
    sp = lax.axis_index("sp")
    tp = lax.axis_index("tp")
    z, core = sp // 2, sp % 2
    y, x = tp // 4, tp % 4
    group = 1 - (x + 1) // 2 % 2
    block = z * 2 + group
    links = [
        (sp, y * 4 + 3 - x),
        (sp, flip1(y) * 4 + x),
        (sp, (3 - y) * 4 + x),
    ]
    sibling = (z * 2 + 1 - core, tp)
    partner_tp = y * 4 + flip1(x)
    partner = (z * 2 + 1 - core, partner_tp)

    def along_z(step):
        return ((z + step + Z) % Z * 2 + core, tp)

    def signal(semaphore, device):
        pl.semaphore_signal(semaphore, inc=1, device_id=device, device_id_type=MESH)

    def remote(src, dst, send, recv, device):
        return pltpu.make_async_remote_copy(
            src_ref=src, dst_ref=dst, send_sem=send, recv_sem=recv, device_id=device, device_id_type=MESH
        )

    def arrived(ref, semaphore):
        pltpu.make_async_copy(ref, ref, semaphore).wait()

    is_native = core == group
    is_foreign = core != group

    barrier = pltpu.get_barrier_semaphore()
    near = links + [sibling, partner, along_z(1), along_z(-1)]
    for device in near:
        signal(barrier, device)

    @pl.when(is_native)
    def _():
        for j in range(N):
            pltpu.make_async_copy(x_hbm.at[piece(j)], xbuf.at[0, 0, piece(j)], mine_sem.at[0, j]).start()

    smalls = [
        pltpu.make_async_copy(src, dst, small_sem.at[i])
        for i, (src, dst) in enumerate((
            (decay_hbm, decay), (query_hbm, query), (key_hbm, key_new), (value_hbm, value_new),
            (gain_hbm, gain), (inverse_hbm, inverse),
        ))
    ]
    pl.semaphore_wait(barrier, len(near))

    def start_smalls():
        for copy in smalls:
            copy.start()

    def fill_mini():
        for copy in smalls:
            copy.wait()
        for h in range(2):
            mini_own[h : h + 1, :] = jnp.broadcast_to(decay[:, h : h + 1], (1, 128))
            mini_own[2 + 2 * h : 4 + 2 * h, :] = query[:, h * 128 : h * 128 + 128].astype(jnp.float32)

    steps = [
        [sibling, partner, along_z(1), along_z(-1)],
        [along_z(2), along_z(-2)],
        [sibling],
        [along_z(3), along_z(-3)],
        [along_z(6), along_z(-6)],
    ]

    def chain_signal(n):
        for device in steps[n]:
            signal(chain.at[n], device)

    def chain_wait(n):
        pl.semaphore_wait(chain.at[n], len(steps[n]))

    def send_on(mask, j, over):
        for d in over:
            remote(
                xbuf.at[0, mask, piece(j)], xbuf.at[0, mask | (1 << d), piece(j)],
                link_send, mine_sem.at[mask | (1 << d), j], links[d],
            ).start()

    def to_sibling(mask, j, group):
        remote(
            xbuf.at[0, mask, piece(j)], xbuf.at[1, mask, piece(j)], sib_send, sib_sem.at[group], sibling
        ).start()

    def column_of(mask, native_part):
        b = [mask // 2**i % 2 for i in range(N)]
        cx = x + b[0] * (3 - 2 * x)
        cy = y + b[1] * (1 - 2 * (y % 2))
        cy = cy + b[2] * (3 - 2 * cy)
        return cy * 4 + (cx if native_part else flip1(cx))

    def weight_rows(t):
        return pl.ds(pl.multiple_of(t * FEAT, FEAT), FEAT)

    def add_product(part, mask, j, native_part, first=False):
        wrows = weight_rows(column_of(mask, native_part))
        block_x = xbuf[part, mask, piece(j), :]
        for i in range(2):
            product = jnp.dot(block_x, weights[i, wrows, :], preferred_element_type=jnp.float32)
            if first:
                acc[i, piece(j), :] = product
            else:
                acc[i, piece(j), :] += product

    def mine_arrived(mask, j):
        arrived(xbuf.at[0, mask, piece(j)], mine_sem.at[mask, j])

    def sib_arrived(group, pieces):
        rows = sum(STARTS[j + 1] - STARTS[j] for j in pieces)
        arrived(xbuf.at[1, 0, pl.ds(0, rows)], sib_sem.at[group])

    def tables(mini):
        @pl.loop(0, 4)
        def _(c):
            rows = pl.ds(pl.multiple_of(c * 256, 256), 256)
            first = (block % 16) * TOK + c * 256
            position = (lax.broadcasted_iota(jnp.int32, (256, 128), 0) + first).astype(jnp.float32)
            table = cos_sin(position, inverse[...]) * 128 ** (-0.5)
            swapped = pltpu.roll(table, 64, axis=1)
            low = lax.broadcasted_iota(jnp.int32, (256, 128), 1) < 64
            cosine[rows, :] = jnp.where(low, table, swapped)
            sine[rows, :] = jnp.where(low, -swapped, table)
            distance = 16384 - 1.0 - position
            for h in range(2):
                weight[h, rows, :] = jnp.exp(mini[h : h + 1, :] * distance)

    @pl.when(is_native)
    def _():
        for j in range(N):
            mine_arrived(0, j)
        for slot in range(3):
            for d in range(N):
                send_on(0, (d - slot) % N, [d])
        start_smalls()
        pltpu.make_async_copy(wk_hbm, weights.at[0], wl_sem.at[0]).start()
        pltpu.make_async_copy(wv_hbm, weights.at[1], wl_sem.at[1]).start()
        for j in range(N):
            to_sibling(0, j, 0)
        chain_signal(0)
        fill_mini()
        mini_got[...] = mini_own[...]
        tables(mini_got)
        arrived(weights.at[0], wl_sem.at[0])
        arrived(weights.at[1], wl_sem.at[1])
        for j in range(N):
            add_product(0, 0, j, True, first=True)
        for slot in range(7):
            got = native_slot(slot)
            for j, _, mask, onward in got:
                mine_arrived(mask, j)
                send_on(mask, j, onward)
                to_sibling(mask, j, 1 + slot)
            if slot in (1, 3, 5):
                chain_wait(slot // 2)
                chain_signal(slot // 2 + 1)
            for j, _, mask, _ in got:
                add_product(0, mask, j, True)
        sib_arrived(0, range(N))
        for j in range(N):
            add_product(1, 0, j, False)
        for n, batch in enumerate(BATCHES):
            if n == 4:
                chain_wait(3)
                chain_signal(4)
            sib_arrived(1 + n, [j for _, _, j in batch])
            for k, r, j in batch:
                add_product(1, landing(k, r, j), j, False)
        chain_wait(4)

    @pl.when(is_foreign)
    def _():
        quarter = z % 4
        opposite = (z + 2) % 4

        other = flip1(x)
        mine_first = (x, 3 - x, other, 3 - other)
        theirs_first = (other, 3 - other, x, 3 - x)

        from_below, from_above, early, late = 4, 5, 6, 7

        def direct(row, i, role):
            t = row * 4 + theirs_first[i]
            rows = weight_rows(t)
            for n, src in enumerate((wk_hbm, wv_hbm)):
                remote(src.at[rows], weights.at[n, rows], w_send, w_sem.at[role], partner).start()

        def pass_weights(t, step, semaphore, role):
            ref = weights.at[:, weight_rows(t)]
            remote(ref, ref, semaphore, w_sem.at[role], along_z(step)).start()

        def exchange(j):
            remote(x_hbm.at[piece(j)], xbuf.at[0, 0, piece(j)], x_send, mine_sem.at[0, j], partner).start()

        def send_messages(messages):
            for k, r, j in messages:
                if (k, r) != (2, 3):
                    send_on(turn(r, j), j, [(j + k) % N])
                    continue
                for second in (False, True):
                    remote(
                        xbuf.at[0, turn(r, j), half(j, second)], xbuf.at[0, landing(k, r, j), half(j, second)],
                        link_send, last_sem.at[j] if second else mine_sem.at[landing(k, r, j), j],
                        links[(j + k) % N],
                    ).start()

        def own_piece(j):
            mine_arrived(0, j)
            send_messages(OWN_SENDS[j])
            to_sibling(0, j, 0)

        waiting = list(FOREIGN_ORDER)
        ready = []

        def receive(*expected):
            k, r, j = waiting.pop(0)
            assert (k, r, j) == expected
            mask = landing(k, r, j)
            ready.append((mask, j))
            if (k, r) == (2, 3):
                return
            mine_arrived(mask, j)
            send_messages(SENDS.get((k, r, j), []))
            to_sibling(mask, j, 1 + [(k, r, j) in batch for batch in BATCHES].index(True))

        def receive_half(j, second):
            ref = xbuf.at[0, landing(2, 3, j), half(j, second)]
            arrived(ref, last_sem.at[j] if second else mine_sem.at[landing(2, 3, j), j])
            remote(ref, xbuf.at[1, landing(2, 3, j), half(j, second)], sib_send, sib_sem.at[9], sibling).start()

        def foreign_product(count):
            for _ in range(count):
                mask, j = ready.pop(0)
                add_product(0, mask, j, False)

        def native_product(slot):
            got = native_slot(slot)
            sib_arrived(1 + slot, [j for j, _, _, _ in got])
            for j, _, mask, _ in got:
                add_product(1, mask, j, True)

        def weights_arrived(role, columns):
            arrived(weights.at[:, pl.ds(0, columns * FEAT)], w_sem.at[role])

        def own_weights(i):
            t = quarter * 4 + mine_first[i]
            weights_arrived(i, 1)
            pass_weights(t, 1, wz_send, (from_below, early, late, late)[i])
            pass_weights(t, -1, wz_send, (early, from_above, late, late)[i])

        def pass_on(step):
            t = (z + step) % 4 * 4 + mine_first[1 if step == 1 else 0]
            weights_arrived(from_above if step == 1 else from_below, 1)
            pass_weights(t, -step, wzz_send, early)

        direct(quarter, 0, 0)
        direct(quarter, 1, 1)
        start_smalls()
        fill_mini()
        for j in range(N):
            exchange(j)
        remote(mini_own, mini_got, mini_send, mini_sem, partner).start()
        direct(quarter, 2, 2)
        direct(quarter, 3, 3)
        direct(opposite, 2, late)
        direct(opposite, 3, late)
        chain_signal(0)
        own_weights(0)
        own_weights(1)
        chain_wait(0)
        chain_signal(1)
        own_piece(0)
        pass_on(-1)
        own_piece(1)
        pass_on(1)
        own_piece(2)
        chain_wait(1)
        chain_signal(2)
        arrived(mini_got, mini_sem)
        tables(mini_got)
        receive(0, 0, 0)
        own_weights(2)
        receive(0, 0, 1)
        weights_arrived(early, 4)
        receive(1, 0, 2)
        receive(0, 0, 2)
        chain_wait(2)
        chain_signal(3)
        sib_arrived(0, range(N))
        for j in range(N):
            add_product(1, 0, j, True, first=True)
        native_product(0)
        native_product(1)
        own_weights(3)
        receive(1, 0, 0)
        receive(2, 0, 1)
        receive(1, 0, 1)
        native_product(2)
        native_product(3)
        native_product(4)
        receive(1, 1, 0)
        receive(2, 1, 1)
        receive(1, 1, 1)
        native_product(5)
        native_product(6)
        chain_wait(3)
        chain_signal(4)
        receive(2, 0, 2)
        receive(1, 1, 2)
        receive(2, 0, 0)
        receive(2, 1, 2)
        weights_arrived(late, 6)
        for j in range(N):
            add_product(0, 0, j, False)
        foreign_product(4)
        receive(2, 2, 1)
        receive(2, 1, 0)
        foreign_product(6)
        receive(2, 2, 2)
        receive(2, 2, 0)
        foreign_product(8)
        receive(2, 3, 2)
        receive(2, 3, 1)
        receive(2, 3, 0)
        for second in (False, True):
            for j in (2, 1, 0):
                receive_half(j, second)
        foreign_product(3)
        chain_wait(4)

    states = []
    for h in range(2):
        cols = pl.ds(h * 128, 128)
        k = acc[0, :, cols]
        keys = (k * cosine[...] + pltpu.roll(k, 64, axis=1) * sine[...]).astype(jnp.bfloat16)
        weighted = (keys.astype(jnp.float32) * weight[h]).astype(jnp.bfloat16)
        values = acc[1, :, cols].astype(jnp.bfloat16)
        states.append(
            lax.dot_general(
                weighted, values, (((0,), (0,)), ((), ())), preferred_element_type=jnp.float32
            )
        )
    top = lax.broadcasted_iota(jnp.int32, (8, 128), 0) < 4
    for i in range(16):
        a = states[0][8 * i : 8 * i + 8]
        b = states[1][8 * i : 8 * i + 8]
        send_state[2 * i] = jnp.where(top, a, pltpu.roll(b, 4, axis=0)).astype(jnp.bfloat16)
        send_state[2 * i + 1] = jnp.where(top, pltpu.roll(a, 4, axis=0), b).astype(jnp.bfloat16)
    prompt = z // 8
    for h in range(2):
        rows = pl.ds(2 + 2 * h, 2)
        both = jnp.dot(mini_got[rows, :], states[h], precision=lax.Precision.HIGHEST, preferred_element_type=jnp.float32)
        send_read[h : h + 1, :] = jnp.where(prompt == 0, both[0:1], both[1:2])

    target_tp = jnp.where(is_native, tp, partner_tp)

    def tail(step, other):
        target = (z + step + Z) % Z * 2 + (1 - core if other else core)
        device = (target, target_tp)
        remote(send_state.at[target], got_state.at[block], tail_send, tail_recv, device).start()
        remote(send_read, got_read.at[block], tail_send2, tail_recv2, device).start()

    far = [8]
    for s in range(7, 0, -1):
        far += [s, -s]
    for step in far:
        for other in (False, True):
            tail(step, other)
    tail(0, True)

    @pl.when(is_native)
    def _():
        pltpu.make_async_copy(send_state.at[sp], got_state.at[block], tail_recv).start()
        pltpu.make_async_copy(send_read, got_read.at[block], tail_recv2).start()

    @pl.when(is_foreign)
    def _():
        tail(0, False)

    queries = query[...].astype(jnp.float32)
    dots = queries * key_new[...].astype(jnp.float32)
    news = value_new[...].astype(jnp.float32)
    own_terms = [
        jnp.sum(dots[:, h * 128 : h * 128 + 128], axis=1, keepdims=True) * news[:, h * 128 : h * 128 + 128]
        for h in range(2)
    ]

    arrived(got_read, tail_recv2)
    carried = [jnp.sum(got_read[16 * s : 16 * s + 16], axis=0) for s in range(2)]
    for h in range(2):
        scaled = jnp.exp(mini_own[h : h + 1, :])
        rows = jnp.concatenate([carried[0][h : h + 1], carried[1][h : h + 1]], axis=0)
        mixed = scaled * rows + own_terms[h]
        normed = mixed * lax.rsqrt(jnp.mean(mixed * mixed, axis=1, keepdims=True) + 1e-06)
        read_out[:, h * 128 : h * 128 + 128] = normed * gain[:, h * 128 : h * 128 + 128]
    arrived(got_state, tail_recv)
    for s in range(2):
        total = jnp.zeros((8, 128), jnp.float32)
        for i in range(16):
            total = total + got_state[16 * s + i].astype(jnp.float32)
        state_out[s] = total

    arrived(xbuf.at[0, pl.ds(0, 7)], link_send)
    arrived(xbuf.at[0], sib_send)

    @pl.when(is_native)
    def _():
        arrived(got_state.at[pl.ds(0, 31)], tail_send)
        arrived(got_read.at[pl.ds(0, 31)], tail_send2)

    @pl.when(is_foreign)
    def _():
        arrived(got_state, tail_send)
        arrived(got_read, tail_send2)
        arrived(xbuf.at[0, 0], x_send)
        arrived(mini_own, mini_send)
        arrived(weights.at[:, pl.ds(0, 1536)], w_send)
        arrived(weights.at[0], wz_send)
        arrived(weights.at[0, pl.ds(0, 1024)], wzz_send)


def round_results(state, read, state_out, read_out):
    state_out[...] = state[...].astype(jnp.bfloat16)
    read_out[...] = read[...].astype(jnp.bfloat16)


def on_device(
    layer_input, key_weight, value_weight, decay_exponent, query_new, key_new, value_new, norm_gain
):
    inverse = (1.0 / 10000.0 ** (np.arange(64) / 63.0)).astype(np.float32)
    inverse = jnp.asarray(np.concatenate([inverse, inverse])[None, :])
    vmem = pl.BlockSpec(memory_space=pltpu.VMEM)
    anywhere = pl.BlockSpec(memory_space=pl.ANY)
    dma = pltpu.SemaphoreType.DMA
    state, read = pl.pallas_call(
        kernel,
        name="gather_project_reduce",
        out_shape=(
            pltpu.VMEM((2, 8, 128), jnp.float32),
            pltpu.VMEM((2, 256), jnp.float32),
        ),
        in_specs=[
            anywhere, anywhere, anywhere, anywhere, anywhere, anywhere, anywhere, anywhere, anywhere,
        ],
        out_specs=(vmem, vmem),
        scratch_shapes=[
            pltpu.VMEM((1, 2), jnp.float32),
            pltpu.VMEM((2, 256), jnp.bfloat16),
            pltpu.VMEM((2, 256), jnp.bfloat16),
            pltpu.VMEM((2, 256), jnp.bfloat16),
            pltpu.VMEM((1, 256), jnp.float32),
            pltpu.VMEM((1, 128), jnp.float32),
            pltpu.VMEM((2, 8, TOK, FEAT), jnp.bfloat16),
            pltpu.VMEM((2, 4096, 256), jnp.bfloat16),
            pltpu.VMEM((2, TOK, 256), jnp.float32),
            pltpu.VMEM((TOK, 128), jnp.float32),
            pltpu.VMEM((TOK, 128), jnp.float32),
            pltpu.VMEM((2, TOK, 128), jnp.float32),
            pltpu.VMEM((8, 128), jnp.float32),
            pltpu.VMEM((8, 128), jnp.float32),
            pltpu.VMEM((SP, 8, 128), jnp.bfloat16),
            pltpu.VMEM((2, 128), jnp.float32),
            pltpu.VMEM((SP, 8, 128), jnp.bfloat16),
            pltpu.VMEM((SP, 2, 128), jnp.float32),
            dma((6,)), dma((8, N)), dma((N,)), dma((10,)), dma((8,)), dma((2,)), dma,
            dma, dma, dma, dma, dma, dma, dma,
            dma, dma, dma, dma,
            pltpu.SemaphoreType.REGULAR((5,)),
        ],
        compiler_params=pltpu.CompilerParams(collective_id=0, has_side_effects=True),
    )(
        decay_exponent[None, :], layer_input, key_weight, value_weight,
        query_new, key_new, value_new, norm_gain[None, :], inverse,
    )
    in_vmem = [pltpu.with_memory_space_constraint(result, pltpu.VMEM) for result in (state, read)]
    state, read = pl.pallas_call(
        round_results,
        name="round_results",
        out_shape=(
            jax.ShapeDtypeStruct((2, 8, 128), jnp.bfloat16),
            jax.ShapeDtypeStruct((2, 256), jnp.bfloat16),
        ),
        in_specs=[vmem, vmem],
        out_specs=(vmem, vmem),
    )(*in_vmem)
    return (state.reshape(2, 2, 4, 128), read)


def solution(mesh):
    in_specs = (
        P("sp", "tp"), P(None, "tp"), P(None, "tp"), P("tp"),
        P(None, "tp"), P(None, "tp"), P(None, "tp"), P("tp"),
    )
    out_specs = (P(None, "tp", "sp", None), P(None, "tp"))
    return jax.shard_map(
        on_device, mesh=mesh, in_specs=in_specs, out_specs=out_specs, check_vma=False
    )
```

```python
import jax
import jax.numpy as jnp
import numpy as np
from jax import lax
from jax.experimental import pallas as pl
from jax.experimental.pallas import tpu as pltpu
from jax.sharding import PartitionSpec as P

MESH = pl.DeviceIdType.MESH
N = 3
TOK = 1024
FEAT = 256
STARTS = (0, 336, 672, 1024)
SP = 32
Z = 16

NATIVE_ORDER = [(0, 0), (1, 0), (2, 0), (1, 1), (2, 1), (2, 2), (2, 3)]
FOREIGN_ORDER = [
    (0, 0, 0), (0, 0, 1), (1, 0, 2), (0, 0, 2), (1, 0, 0), (2, 0, 1), (1, 0, 1), (1, 1, 0), (2, 1, 1), (1, 1, 1),
    (2, 0, 2), (1, 1, 2), (2, 0, 0), (2, 1, 2), (2, 2, 1), (2, 1, 0), (2, 2, 2), (2, 2, 0), (2, 3, 2), (2, 3, 1),
    (2, 3, 0),
]
BATCHES = []
for _size in (2, 2, 3, 3, 2, 2, 2, 2, 3):
    _first = sum(len(batch) for batch in BATCHES)
    BATCHES.append(FOREIGN_ORDER[_first : _first + _size])
OWN_SENDS = [
    [(0, 0, 0)],
    [(0, 0, 1), (1, 0, 0)],
    [(0, 0, 2), (1, 0, 1), (1, 0, 2), (2, 0, 1)],
]
SENDS = {
    (0, 0, 0): [(1, 1, 0), (2, 0, 2)],
    (0, 0, 1): [(1, 1, 1), (2, 0, 0), (2, 1, 1), (2, 1, 0)],
    (0, 0, 2): [(1, 1, 2), (2, 1, 2)],
}
for _j in range(N):
    SENDS[1, 0, _j] = [(2, 2, _j)]
    SENDS[1, 1, _j] = [(2, 3, _j)]


def turn(mask, j):
    return ((mask << j) | (mask >> (N - j))) & (2**N - 1)


def piece(j):
    return pl.ds(STARTS[j], STARTS[j + 1] - STARTS[j])


HALF = 176


def half(j, second):
    size = STARTS[j + 1] - STARTS[j]
    return pl.ds(STARTS[j] + HALF, size - HALF) if second else pl.ds(STARTS[j], HALF)


def landing(k, r, j):
    return turn(r, j) | (1 << (j + k) % N)


def native_slot(slot):
    k, r = NATIVE_ORDER[slot]
    out = []
    for d in range(N):
        j = (d - k) % N
        sent = r | (1 << k)
        onward = [(j + kk) % N for kk, rr in NATIVE_ORDER if rr == sent]
        out.append((j, turn(r, j), landing(k, r, j), onward))
    return out


def flip1(v):
    return v + 1 - 2 * (v % 2)


def cos_sin(position, inverse):
    angle = position * inverse
    lane = lax.broadcasted_iota(jnp.int32, angle.shape, 1)
    quarter = jnp.floor(angle * 0.6366197723675814 + 0.5)
    rest = ((angle - quarter * 1.5703125) - quarter * 4.837512969970703125e-4) - quarter * 7.54978995489188e-8
    turns = quarter.astype(jnp.int32) - jnp.where(lane >= 64, 1, 0)
    turns = jnp.bitwise_and(turns, 3)
    square = rest * rest
    sine = rest + rest * square * (-1.6666654611e-1 + square * (8.3321608736e-3 - square * 1.9515295891e-4))
    cosine = 1.0 - 0.5 * square + square * square * (
        4.166664568298827e-2 + square * (-1.388731625493765e-3 + square * 2.443315711809948e-5)
    )
    value = jnp.where(jnp.bitwise_and(turns, 1) == 1, sine, cosine)
    negative = jnp.logical_or(turns == 1, turns == 2)
    return jnp.where(negative, -value, value)


def kernel(
    decay_hbm, x_hbm, wk_hbm, wv_hbm, query_hbm, key_hbm, value_hbm, gain_hbm, inverse_hbm,
    state_out, read_out,
    decay, query, key_new, value_new, gain, inverse,
    xbuf, weights, acc, state, cosine, sine, weight, mini_own, mini_got, send_state, send_read, got_state, got_read,
    small_sem, mine_sem, last_sem, sib_sem, w_sem, wl_sem, mini_sem,
    link_send, sib_send, x_send, w_send, wz_send, wzz_send, mini_send,
    tail_send, tail_send2, tail_recv, tail_recv2, chain,
):
    sp = lax.axis_index("sp")
    tp = lax.axis_index("tp")
    z, core = sp // 2, sp % 2
    y, x = tp // 4, tp % 4
    group = 1 - (x + 1) // 2 % 2
    block = z * 2 + group
    links = [
        (sp, y * 4 + 3 - x),
        (sp, flip1(y) * 4 + x),
        (sp, (3 - y) * 4 + x),
    ]
    sibling = (z * 2 + 1 - core, tp)
    partner_tp = y * 4 + flip1(x)
    partner = (z * 2 + 1 - core, partner_tp)

    def along_z(step):
        return ((z + step + Z) % Z * 2 + core, tp)

    def signal(semaphore, device):
        pl.semaphore_signal(semaphore, inc=1, device_id=device, device_id_type=MESH)

    def remote(src, dst, send, recv, device):
        return pltpu.make_async_remote_copy(
            src_ref=src, dst_ref=dst, send_sem=send, recv_sem=recv, device_id=device, device_id_type=MESH
        )

    def arrived(ref, semaphore):
        pltpu.make_async_copy(ref, ref, semaphore).wait()

    is_native = core == group
    is_foreign = core != group

    barrier = pltpu.get_barrier_semaphore()
    near = links + [sibling, partner, along_z(1), along_z(-1)]
    for device in near:
        signal(barrier, device)

    @pl.when(is_native)
    def _():
        for j in range(N):
            pltpu.make_async_copy(x_hbm.at[piece(j)], xbuf.at[0, 0, piece(j)], mine_sem.at[0, j]).start()

    smalls = [
        pltpu.make_async_copy(src, dst, small_sem.at[i])
        for i, (src, dst) in enumerate((
            (decay_hbm, decay), (query_hbm, query), (key_hbm, key_new), (value_hbm, value_new),
            (gain_hbm, gain), (inverse_hbm, inverse),
        ))
    ]
    pl.semaphore_wait(barrier, len(near))

    def start_smalls():
        for copy in smalls:
            copy.start()

    def fill_mini():
        for copy in smalls:
            copy.wait()
        for h in range(2):
            mini_own[h : h + 1, :] = jnp.broadcast_to(decay[:, h : h + 1], (1, 128))
            mini_own[2 + 2 * h : 4 + 2 * h, :] = query[:, h * 128 : h * 128 + 128].astype(jnp.float32)

    steps = [
        [sibling, partner, along_z(1), along_z(-1)],
        [along_z(2), along_z(-2)],
        [sibling],
        [along_z(3), along_z(-3)],
        [along_z(6), along_z(-6)],
    ]

    def chain_signal(n):
        for device in steps[n]:
            signal(chain.at[n], device)

    def chain_wait(n):
        pl.semaphore_wait(chain.at[n], len(steps[n]))

    def send_on(mask, j, over):
        for d in over:
            remote(
                xbuf.at[0, mask, piece(j)], xbuf.at[0, mask | (1 << d), piece(j)],
                link_send, mine_sem.at[mask | (1 << d), j], links[d],
            ).start()

    def to_sibling(mask, j, group):
        remote(
            xbuf.at[0, mask, piece(j)], xbuf.at[1, mask, piece(j)], sib_send, sib_sem.at[group], sibling
        ).start()

    def column_of(mask, native_part):
        b = [mask // 2**i % 2 for i in range(N)]
        cx = x + b[0] * (3 - 2 * x)
        cy = y + b[1] * (1 - 2 * (y % 2))
        cy = cy + b[2] * (3 - 2 * cy)
        return cy * 4 + (cx if native_part else flip1(cx))

    def weight_rows(t):
        return pl.ds(pl.multiple_of(t * FEAT, FEAT), FEAT)

    def add_product(part, mask, j, native_part, first=False, second=None):
        wrows = weight_rows(column_of(mask, native_part))
        rows = piece(j) if second is None else half(j, second)
        block_x = xbuf[part, mask, rows, :]
        for i in range(2):
            product = jnp.dot(block_x, weights[i, wrows, :], preferred_element_type=jnp.float32)
            if first:
                acc[i, rows, :] = product
            else:
                acc[i, rows, :] += product

    def add_state(ranges, first=False):
        for h in range(2):
            cols = pl.ds(h * 128, 128)
            total = None if first else state[h]
            for rows in ranges:
                k = acc[0, rows, cols]
                keys = (k * cosine[rows, :] + pltpu.roll(k, 64, axis=1) * sine[rows, :]).astype(jnp.bfloat16)
                weighted = (keys.astype(jnp.float32) * weight[h, rows, :]).astype(jnp.bfloat16)
                values = acc[1, rows, cols].astype(jnp.bfloat16)
                product = lax.dot_general(
                    weighted, values, (((0,), (0,)), ((), ())), preferred_element_type=jnp.float32
                )
                total = product if total is None else total + product
            state[h] = total

    def mine_arrived(mask, j):
        arrived(xbuf.at[0, mask, piece(j)], mine_sem.at[mask, j])

    def sib_arrived(group, pieces):
        rows = sum(STARTS[j + 1] - STARTS[j] for j in pieces)
        arrived(xbuf.at[1, 0, pl.ds(0, rows)], sib_sem.at[group])

    def tables(mini):
        @pl.loop(0, 4)
        def _(c):
            rows = pl.ds(pl.multiple_of(c * 256, 256), 256)
            first = (block % 16) * TOK + c * 256
            position = (lax.broadcasted_iota(jnp.int32, (256, 128), 0) + first).astype(jnp.float32)
            table = cos_sin(position, inverse[...]) * 128 ** (-0.5)
            swapped = pltpu.roll(table, 64, axis=1)
            low = lax.broadcasted_iota(jnp.int32, (256, 128), 1) < 64
            cosine[rows, :] = jnp.where(low, table, swapped)
            sine[rows, :] = jnp.where(low, -swapped, table)
            distance = 16384 - 1.0 - position
            for h in range(2):
                weight[h, rows, :] = jnp.exp(mini[h : h + 1, :] * distance)

    @pl.when(is_native)
    def _():
        for j in range(N):
            mine_arrived(0, j)
        for slot in range(3):
            for d in range(N):
                send_on(0, (d - slot) % N, [d])
        start_smalls()
        pltpu.make_async_copy(wk_hbm, weights.at[0], wl_sem.at[0]).start()
        pltpu.make_async_copy(wv_hbm, weights.at[1], wl_sem.at[1]).start()
        for j in range(N):
            to_sibling(0, j, 0)
        chain_signal(0)
        fill_mini()
        mini_got[...] = mini_own[...]
        tables(mini_got)
        arrived(weights.at[0], wl_sem.at[0])
        arrived(weights.at[1], wl_sem.at[1])
        for j in range(N):
            add_product(0, 0, j, True, first=True)
        for slot in range(7):
            got = native_slot(slot)
            for j, _, mask, onward in got:
                mine_arrived(mask, j)
                send_on(mask, j, onward)
                to_sibling(mask, j, 1 + slot)
            if slot in (1, 3, 5):
                chain_wait(slot // 2)
                chain_signal(slot // 2 + 1)
            for j, _, mask, _ in got:
                add_product(0, mask, j, True)
        sib_arrived(0, range(N))
        for j in range(N):
            add_product(1, 0, j, False)
        for n, batch in enumerate(BATCHES):
            if n == 4:
                chain_wait(3)
                chain_signal(4)
            if n == 8:
                continue
            sib_arrived(1 + n, [j for _, _, j in batch])
            for k, r, j in batch:
                add_product(1, landing(k, r, j), j, False)
        for second in (False, True):
            ranges = [half(j, second) for j in (2, 1, 0)]
            rows = sum(span.size for span in ranges)
            arrived(xbuf.at[1, 0, pl.ds(0, rows)], sib_sem.at[10 if second else 9])
            for j in (2, 1, 0):
                add_product(1, landing(2, 3, j), j, False, second=second)
            add_state(ranges, first=not second)
        chain_wait(4)

    @pl.when(is_foreign)
    def _():
        quarter = z % 4
        opposite = (z + 2) % 4

        other = flip1(x)
        mine_first = (x, 3 - x, other, 3 - other)
        theirs_first = (other, 3 - other, x, 3 - x)

        from_below, from_above, early, late = 4, 5, 6, 7

        def direct(row, i, role):
            t = row * 4 + theirs_first[i]
            rows = weight_rows(t)
            for n, src in enumerate((wk_hbm, wv_hbm)):
                remote(src.at[rows], weights.at[n, rows], w_send, w_sem.at[role], partner).start()

        def pass_weights(t, step, semaphore, role):
            ref = weights.at[:, weight_rows(t)]
            remote(ref, ref, semaphore, w_sem.at[role], along_z(step)).start()

        def exchange(j):
            remote(x_hbm.at[piece(j)], xbuf.at[0, 0, piece(j)], x_send, mine_sem.at[0, j], partner).start()

        def send_messages(messages):
            for k, r, j in messages:
                if (k, r) != (2, 3):
                    send_on(turn(r, j), j, [(j + k) % N])
                    continue
                for second in (False, True):
                    remote(
                        xbuf.at[0, turn(r, j), half(j, second)], xbuf.at[0, landing(k, r, j), half(j, second)],
                        link_send, last_sem.at[j] if second else mine_sem.at[landing(k, r, j), j],
                        links[(j + k) % N],
                    ).start()

        def own_piece(j):
            mine_arrived(0, j)
            send_messages(OWN_SENDS[j])
            to_sibling(0, j, 0)

        waiting = list(FOREIGN_ORDER)
        ready = []

        def receive(*expected):
            k, r, j = waiting.pop(0)
            assert (k, r, j) == expected
            mask = landing(k, r, j)
            ready.append((mask, j))
            if (k, r) == (2, 3):
                return
            mine_arrived(mask, j)
            send_messages(SENDS.get((k, r, j), []))
            to_sibling(mask, j, 1 + [(k, r, j) in batch for batch in BATCHES].index(True))

        def receive_half(j, second):
            ref = xbuf.at[0, landing(2, 3, j), half(j, second)]
            arrived(ref, last_sem.at[j] if second else mine_sem.at[landing(2, 3, j), j])
            remote(ref, xbuf.at[1, landing(2, 3, j), half(j, second)], sib_send, sib_sem.at[10 if second else 9], sibling).start()

        def foreign_product(count):
            for _ in range(count):
                mask, j = ready.pop(0)
                add_product(0, mask, j, False)

        def native_product(slot):
            got = native_slot(slot)
            sib_arrived(1 + slot, [j for j, _, _, _ in got])
            for j, _, mask, _ in got:
                add_product(1, mask, j, True)

        def weights_arrived(role, columns):
            arrived(weights.at[:, pl.ds(0, columns * FEAT)], w_sem.at[role])

        def own_weights(i):
            t = quarter * 4 + mine_first[i]
            weights_arrived(i, 1)
            pass_weights(t, 1, wz_send, (from_below, early, late, late)[i])
            pass_weights(t, -1, wz_send, (early, from_above, late, late)[i])

        def pass_on(step):
            t = (z + step) % 4 * 4 + mine_first[1 if step == 1 else 0]
            weights_arrived(from_above if step == 1 else from_below, 1)
            pass_weights(t, -step, wzz_send, early)

        direct(quarter, 0, 0)
        direct(quarter, 1, 1)
        start_smalls()
        fill_mini()
        for j in range(N):
            exchange(j)
        remote(mini_own, mini_got, mini_send, mini_sem, partner).start()
        direct(quarter, 2, 2)
        direct(quarter, 3, 3)
        direct(opposite, 2, late)
        direct(opposite, 3, late)
        chain_signal(0)
        own_weights(0)
        own_weights(1)
        chain_wait(0)
        chain_signal(1)
        own_piece(0)
        pass_on(-1)
        own_piece(1)
        pass_on(1)
        own_piece(2)
        chain_wait(1)
        chain_signal(2)
        arrived(mini_got, mini_sem)
        tables(mini_got)
        receive(0, 0, 0)
        own_weights(2)
        receive(0, 0, 1)
        weights_arrived(early, 4)
        receive(1, 0, 2)
        receive(0, 0, 2)
        chain_wait(2)
        chain_signal(3)
        sib_arrived(0, range(N))
        for j in range(N):
            add_product(1, 0, j, True, first=True)
        native_product(0)
        native_product(1)
        own_weights(3)
        receive(1, 0, 0)
        receive(2, 0, 1)
        receive(1, 0, 1)
        native_product(2)
        native_product(3)
        native_product(4)
        receive(1, 1, 0)
        receive(2, 1, 1)
        receive(1, 1, 1)
        native_product(5)
        native_product(6)
        chain_wait(3)
        chain_signal(4)
        receive(2, 0, 2)
        receive(1, 1, 2)
        receive(2, 0, 0)
        receive(2, 1, 2)
        weights_arrived(late, 6)
        for j in range(N):
            add_product(0, 0, j, False)
        foreign_product(4)
        receive(2, 2, 1)
        receive(2, 1, 0)
        foreign_product(6)
        receive(2, 2, 2)
        receive(2, 2, 0)
        foreign_product(4)
        receive(2, 3, 2)
        receive(2, 3, 1)
        receive(2, 3, 0)
        for j in (2, 1, 0):
            receive_half(j, False)
        foreign_product(4)
        for j in (2, 1, 0):
            receive_half(j, True)
        foreign_product(3)
        add_state([pl.ds(0, TOK)], first=True)
        chain_wait(4)

    states = [state[0], state[1]]
    top = lax.broadcasted_iota(jnp.int32, (8, 128), 0) < 4
    for i in range(16):
        a = states[0][8 * i : 8 * i + 8]
        b = states[1][8 * i : 8 * i + 8]
        send_state[2 * i] = jnp.where(top, a, pltpu.roll(b, 4, axis=0)).astype(jnp.bfloat16)
        send_state[2 * i + 1] = jnp.where(top, pltpu.roll(a, 4, axis=0), b).astype(jnp.bfloat16)
    prompt = z // 8
    reads = []
    for h in range(2):
        rows = pl.ds(2 + 2 * h, 2)
        both = jnp.dot(
            mini_got[rows, :], states[h], precision=lax.Precision.HIGHEST, preferred_element_type=jnp.float32
        )
        reads.append(jnp.where(prompt == 0, both[0:1], both[1:2]))
    send_read[...] = jnp.concatenate(reads, axis=0).astype(jnp.bfloat16)

    target_tp = jnp.where(is_native, tp, partner_tp)

    def tail(step, other):
        target = (z + step + Z) % Z * 2 + (1 - core if other else core)
        device = (target, target_tp)
        remote(send_state.at[target], got_state.at[block], tail_send, tail_recv, device).start()
        remote(send_read, got_read.at[block], tail_send2, tail_recv2, device).start()

    far = [8]
    for s in range(7, 0, -1):
        far += [s, -s]
    for step in far:
        for other in (False, True):
            tail(step, other)
    tail(0, True)

    @pl.when(is_native)
    def _():
        pltpu.make_async_copy(send_state.at[sp], got_state.at[block], tail_recv).start()
        pltpu.make_async_copy(send_read, got_read.at[block], tail_recv2).start()

    @pl.when(is_foreign)
    def _():
        tail(0, False)

    queries = query[...].astype(jnp.float32)
    dots = queries * key_new[...].astype(jnp.float32)
    news = value_new[...].astype(jnp.float32)
    own_terms = [
        jnp.sum(dots[:, h * 128 : h * 128 + 128], axis=1, keepdims=True) * news[:, h * 128 : h * 128 + 128]
        for h in range(2)
    ]

    arrived(got_read, tail_recv2)
    carried = [jnp.sum(got_read[16 * s : 16 * s + 16].astype(jnp.float32), axis=0) for s in range(2)]
    for h in range(2):
        scaled = jnp.exp(mini_own[h : h + 1, :])
        rows = jnp.concatenate([carried[0][h : h + 1], carried[1][h : h + 1]], axis=0)
        mixed = scaled * rows + own_terms[h]
        normed = mixed * lax.rsqrt(jnp.mean(mixed * mixed, axis=1, keepdims=True) + 1e-06)
        read_out[:, h * 128 : h * 128 + 128] = normed * gain[:, h * 128 : h * 128 + 128]
    arrived(got_state, tail_recv)
    for s in range(2):
        total = jnp.zeros((8, 128), jnp.float32)
        for i in range(16):
            total = total + got_state[16 * s + i].astype(jnp.float32)
        state_out[s] = total

    arrived(xbuf.at[0, pl.ds(0, 7)], link_send)
    arrived(xbuf.at[0], sib_send)

    @pl.when(is_native)
    def _():
        arrived(got_state.at[pl.ds(0, 31)], tail_send)
        arrived(got_read.at[pl.ds(0, 31)], tail_send2)

    @pl.when(is_foreign)
    def _():
        arrived(got_state, tail_send)
        arrived(got_read, tail_send2)
        arrived(xbuf.at[0, 0], x_send)
        arrived(mini_own, mini_send)
        arrived(weights.at[:, pl.ds(0, 1536)], w_send)
        arrived(weights.at[0], wz_send)
        arrived(weights.at[0, pl.ds(0, 1024)], wzz_send)


def round_results(state, read, state_out, read_out):
    state_out[...] = state[...].astype(jnp.bfloat16)
    read_out[...] = read[...].astype(jnp.bfloat16)


def on_device(
    layer_input, key_weight, value_weight, decay_exponent, query_new, key_new, value_new, norm_gain
):
    inverse = (1.0 / 10000.0 ** (np.arange(64) / 63.0)).astype(np.float32)
    inverse = jnp.asarray(np.concatenate([inverse, inverse])[None, :])
    vmem = pl.BlockSpec(memory_space=pltpu.VMEM)
    anywhere = pl.BlockSpec(memory_space=pl.ANY)
    dma = pltpu.SemaphoreType.DMA
    state, read = pl.pallas_call(
        kernel,
        name="gather_project_reduce",
        out_shape=(
            pltpu.VMEM((2, 8, 128), jnp.float32),
            pltpu.VMEM((2, 256), jnp.float32),
        ),
        in_specs=[
            anywhere, anywhere, anywhere, anywhere, anywhere, anywhere, anywhere, anywhere, anywhere,
        ],
        out_specs=(vmem, vmem),
        scratch_shapes=[
            pltpu.VMEM((1, 2), jnp.float32),
            pltpu.VMEM((2, 256), jnp.bfloat16),
            pltpu.VMEM((2, 256), jnp.bfloat16),
            pltpu.VMEM((2, 256), jnp.bfloat16),
            pltpu.VMEM((1, 256), jnp.float32),
            pltpu.VMEM((1, 128), jnp.float32),
            pltpu.VMEM((2, 8, TOK, FEAT), jnp.bfloat16),
            pltpu.VMEM((2, 4096, 256), jnp.bfloat16),
            pltpu.VMEM((2, TOK, 256), jnp.float32),
            pltpu.VMEM((2, 128, 128), jnp.float32),
            pltpu.VMEM((TOK, 128), jnp.float32),
            pltpu.VMEM((TOK, 128), jnp.float32),
            pltpu.VMEM((2, TOK, 128), jnp.float32),
            pltpu.VMEM((8, 128), jnp.float32),
            pltpu.VMEM((8, 128), jnp.float32),
            pltpu.VMEM((SP, 8, 128), jnp.bfloat16),
            pltpu.VMEM((2, 128), jnp.bfloat16),
            pltpu.VMEM((SP, 8, 128), jnp.bfloat16),
            pltpu.VMEM((SP, 2, 128), jnp.bfloat16),
            dma((6,)), dma((8, N)), dma((N,)), dma((11,)), dma((8,)), dma((2,)), dma,
            dma, dma, dma, dma, dma, dma, dma,
            dma, dma, dma, dma,
            pltpu.SemaphoreType.REGULAR((5,)),
        ],
        compiler_params=pltpu.CompilerParams(collective_id=0, has_side_effects=True),
    )(
        decay_exponent[None, :], layer_input, key_weight, value_weight,
        query_new, key_new, value_new, norm_gain[None, :], inverse,
    )
    in_vmem = [pltpu.with_memory_space_constraint(result, pltpu.VMEM) for result in (state, read)]
    state, read = pl.pallas_call(
        round_results,
        name="round_results",
        out_shape=(
            jax.ShapeDtypeStruct((2, 8, 128), jnp.bfloat16),
            jax.ShapeDtypeStruct((2, 256), jnp.bfloat16),
        ),
        in_specs=[vmem, vmem],
        out_specs=(vmem, vmem),
    )(*in_vmem)
    return (state.reshape(2, 2, 4, 128), read)


def solution(mesh):
    in_specs = (
        P("sp", "tp"), P(None, "tp"), P(None, "tp"), P("tp"),
        P(None, "tp"), P(None, "tp"), P(None, "tp"), P("tp"),
    )
    out_specs = (P(None, "tp", "sp", None), P(None, "tp"))
    return jax.shard_map(
        on_device, mesh=mesh, in_specs=in_specs, out_specs=out_specs, check_vma=False
    )
```

```python
import jax
import jax.numpy as jnp
import numpy as np
from jax import lax
from jax.experimental import pallas as pl
from jax.experimental.pallas import tpu as pltpu
from jax.sharding import PartitionSpec as P

MESH = pl.DeviceIdType.MESH
N = 3
TOK = 1024
FEAT = 256
STARTS = (0, 336, 672, 1024)
SP = 32
Z = 16

NATIVE_ORDER = [(0, 0), (1, 0), (2, 0), (1, 1), (2, 1), (2, 2), (2, 3)]
FOREIGN_ORDER = [
    (0, 0, 0), (0, 0, 1), (1, 0, 2), (0, 0, 2), (1, 0, 0), (2, 0, 1), (1, 0, 1), (1, 1, 0), (2, 1, 1), (1, 1, 1),
    (2, 0, 2), (1, 1, 2), (2, 0, 0), (2, 1, 2), (2, 2, 1), (2, 1, 0), (2, 2, 2), (2, 2, 0), (2, 3, 2), (2, 3, 1),
    (2, 3, 0),
]
BATCHES = []
for _size in (2, 2, 3, 3, 2, 2, 2, 2, 3):
    _first = sum(len(batch) for batch in BATCHES)
    BATCHES.append(FOREIGN_ORDER[_first : _first + _size])
OWN_SENDS = [
    [(0, 0, 0)],
    [(0, 0, 1), (1, 0, 0)],
    [(0, 0, 2), (1, 0, 1), (1, 0, 2), (2, 0, 1)],
]
SENDS = {
    (0, 0, 0): [(1, 1, 0), (2, 0, 2)],
    (0, 0, 1): [(1, 1, 1), (2, 0, 0), (2, 1, 1), (2, 1, 0)],
    (0, 0, 2): [(1, 1, 2), (2, 1, 2)],
}
for _j in range(N):
    SENDS[1, 0, _j] = [(2, 2, _j)]
    SENDS[1, 1, _j] = [(2, 3, _j)]


def turn(mask, j):
    return ((mask << j) | (mask >> (N - j))) & (2**N - 1)


def piece(j):
    return pl.ds(STARTS[j], STARTS[j + 1] - STARTS[j])


HALF = 176
ROWS = 10


def half(j, second):
    size = STARTS[j + 1] - STARTS[j]
    return pl.ds(STARTS[j] + HALF, size - HALF) if second else pl.ds(STARTS[j], HALF)


def landing(k, r, j):
    return turn(r, j) | (1 << (j + k) % N)


def native_slot(slot):
    k, r = NATIVE_ORDER[slot]
    out = []
    for d in range(N):
        j = (d - k) % N
        sent = r | (1 << k)
        onward = [(j + kk) % N for kk, rr in NATIVE_ORDER if rr == sent]
        out.append((j, turn(r, j), landing(k, r, j), onward))
    return out


def flip1(v):
    return v + 1 - 2 * (v % 2)


def cos_sin(position, inverse):
    angle = position * inverse
    lane = lax.broadcasted_iota(jnp.int32, angle.shape, 1)
    quarter = jnp.floor(angle * 0.6366197723675814 + 0.5)
    rest = ((angle - quarter * 1.5703125) - quarter * 4.837512969970703125e-4) - quarter * 7.54978995489188e-8
    turns = quarter.astype(jnp.int32) - jnp.where(lane >= 64, 1, 0)
    turns = jnp.bitwise_and(turns, 3)
    square = rest * rest
    sine = rest + rest * square * (-1.6666654611e-1 + square * (8.3321608736e-3 - square * 1.9515295891e-4))
    cosine = 1.0 - 0.5 * square + square * square * (
        4.166664568298827e-2 + square * (-1.388731625493765e-3 + square * 2.443315711809948e-5)
    )
    value = jnp.where(jnp.bitwise_and(turns, 1) == 1, sine, cosine)
    negative = jnp.logical_or(turns == 1, turns == 2)
    return jnp.where(negative, -value, value)


def kernel(
    decay_hbm, x_hbm, wk_hbm, wv_hbm, query_hbm, key_hbm, value_hbm, gain_hbm, inverse_hbm,
    state_out, read_out,
    decay, query, key_new, value_new, gain, inverse,
    xbuf, weights, acc, state, cosine, sine, weight, mini_own, mini_got, send_share, got_share,
    small_sem, mine_sem, last_sem, sib_sem, w_sem, wl_sem, mini_sem,
    link_send, sib_send, x_send, w_send, wz_send, wzz_send, mini_send,
    tail_send, tail_recv, chain,
):
    sp = lax.axis_index("sp")
    tp = lax.axis_index("tp")
    z, core = sp // 2, sp % 2
    y, x = tp // 4, tp % 4
    group = 1 - (x + 1) // 2 % 2
    block = z * 2 + group
    links = [
        (sp, y * 4 + 3 - x),
        (sp, flip1(y) * 4 + x),
        (sp, (3 - y) * 4 + x),
    ]
    sibling = (z * 2 + 1 - core, tp)
    partner_tp = y * 4 + flip1(x)
    partner = (z * 2 + 1 - core, partner_tp)

    def along_z(step):
        return ((z + step + Z) % Z * 2 + core, tp)

    def signal(semaphore, device):
        pl.semaphore_signal(semaphore, inc=1, device_id=device, device_id_type=MESH)

    def remote(src, dst, send, recv, device):
        return pltpu.make_async_remote_copy(
            src_ref=src, dst_ref=dst, send_sem=send, recv_sem=recv, device_id=device, device_id_type=MESH
        )

    def arrived(ref, semaphore):
        pltpu.make_async_copy(ref, ref, semaphore).wait()

    is_native = core == group
    is_foreign = core != group

    barrier = pltpu.get_barrier_semaphore()
    near = links + [sibling, partner, along_z(1), along_z(-1)]
    for device in near:
        signal(barrier, device)

    @pl.when(is_native)
    def _():
        for j in range(N):
            pltpu.make_async_copy(x_hbm.at[piece(j)], xbuf.at[0, 0, piece(j)], mine_sem.at[0, j]).start()

    smalls = [
        pltpu.make_async_copy(src, dst, small_sem.at[i])
        for i, (src, dst) in enumerate((
            (decay_hbm, decay), (query_hbm, query), (key_hbm, key_new), (value_hbm, value_new),
            (gain_hbm, gain), (inverse_hbm, inverse),
        ))
    ]
    pl.semaphore_wait(barrier, len(near))

    def start_smalls():
        for copy in smalls:
            copy.start()

    def fill_mini():
        for copy in smalls:
            copy.wait()
        for h in range(2):
            mini_own[h : h + 1, :] = jnp.broadcast_to(decay[:, h : h + 1], (1, 128))
            mini_own[2 + 2 * h : 4 + 2 * h, :] = query[:, h * 128 : h * 128 + 128].astype(jnp.float32)

    steps = [
        [sibling, partner, along_z(1), along_z(-1)],
        [along_z(2), along_z(-2)],
        [sibling],
        [along_z(3), along_z(-3)],
        [along_z(6), along_z(-6)],
    ]

    def chain_signal(n):
        for device in steps[n]:
            signal(chain.at[n], device)

    def chain_wait(n):
        pl.semaphore_wait(chain.at[n], len(steps[n]))

    def send_on(mask, j, over):
        for d in over:
            remote(
                xbuf.at[0, mask, piece(j)], xbuf.at[0, mask | (1 << d), piece(j)],
                link_send, mine_sem.at[mask | (1 << d), j], links[d],
            ).start()

    def to_sibling(mask, j, group):
        remote(
            xbuf.at[0, mask, piece(j)], xbuf.at[1, mask, piece(j)], sib_send, sib_sem.at[group], sibling
        ).start()

    def column_of(mask, native_part):
        b = [mask // 2**i % 2 for i in range(N)]
        cx = x + b[0] * (3 - 2 * x)
        cy = y + b[1] * (1 - 2 * (y % 2))
        cy = cy + b[2] * (3 - 2 * cy)
        return cy * 4 + (cx if native_part else flip1(cx))

    def weight_rows(t):
        return pl.ds(pl.multiple_of(t * FEAT, FEAT), FEAT)

    def add_product(part, mask, j, native_part, first=False, second=None):
        wrows = weight_rows(column_of(mask, native_part))
        rows = piece(j) if second is None else half(j, second)
        block_x = xbuf[part, mask, rows, :]
        for i in range(2):
            product = jnp.dot(block_x, weights[i, wrows, :], preferred_element_type=jnp.float32)
            if first:
                acc[i, rows, :] = product
            else:
                acc[i, rows, :] += product

    def add_state(ranges, first=False):
        for h in range(2):
            cols = pl.ds(h * 128, 128)
            total = None if first else state[h]
            for rows in ranges:
                k = acc[0, rows, cols]
                keys = (k * cosine[rows, :] + pltpu.roll(k, 64, axis=1) * sine[rows, :]).astype(jnp.bfloat16)
                weighted = (keys.astype(jnp.float32) * weight[h, rows, :]).astype(jnp.bfloat16)
                values = acc[1, rows, cols].astype(jnp.bfloat16)
                product = lax.dot_general(
                    weighted, values, (((0,), (0,)), ((), ())), preferred_element_type=jnp.float32
                )
                total = product if total is None else total + product
            state[h] = total

    def mine_arrived(mask, j):
        arrived(xbuf.at[0, mask, piece(j)], mine_sem.at[mask, j])

    def sib_arrived(group, pieces):
        rows = sum(STARTS[j + 1] - STARTS[j] for j in pieces)
        arrived(xbuf.at[1, 0, pl.ds(0, rows)], sib_sem.at[group])

    def tables(mini):
        @pl.loop(0, 4)
        def _(c):
            rows = pl.ds(pl.multiple_of(c * 256, 256), 256)
            first = (block % 16) * TOK + c * 256
            position = (lax.broadcasted_iota(jnp.int32, (256, 128), 0) + first).astype(jnp.float32)
            table = cos_sin(position, inverse[...]) * 128 ** (-0.5)
            swapped = pltpu.roll(table, 64, axis=1)
            low = lax.broadcasted_iota(jnp.int32, (256, 128), 1) < 64
            cosine[rows, :] = jnp.where(low, table, swapped)
            sine[rows, :] = jnp.where(low, -swapped, table)
            distance = 16384 - 1.0 - position
            for h in range(2):
                weight[h, rows, :] = jnp.exp(mini[h : h + 1, :] * distance)

    @pl.when(is_native)
    def _():
        for j in range(N):
            mine_arrived(0, j)
        for slot in range(3):
            for d in range(N):
                send_on(0, (d - slot) % N, [d])
        start_smalls()
        pltpu.make_async_copy(wk_hbm, weights.at[0], wl_sem.at[0]).start()
        pltpu.make_async_copy(wv_hbm, weights.at[1], wl_sem.at[1]).start()
        for j in range(N):
            to_sibling(0, j, 0)
        chain_signal(0)
        fill_mini()
        mini_got[...] = mini_own[...]
        tables(mini_got)
        arrived(weights.at[0], wl_sem.at[0])
        arrived(weights.at[1], wl_sem.at[1])
        for j in range(N):
            add_product(0, 0, j, True, first=True)
        for slot in range(7):
            got = native_slot(slot)
            for j, _, mask, onward in got:
                mine_arrived(mask, j)
                send_on(mask, j, onward)
                to_sibling(mask, j, 1 + slot)
            if slot in (1, 3, 5):
                chain_wait(slot // 2)
                chain_signal(slot // 2 + 1)
            for j, _, mask, _ in got:
                add_product(0, mask, j, True)
        sib_arrived(0, range(N))
        for j in range(N):
            add_product(1, 0, j, False)
        for n, batch in enumerate(BATCHES):
            if n == 4:
                chain_wait(3)
                chain_signal(4)
            if n == 8:
                continue
            sib_arrived(1 + n, [j for _, _, j in batch])
            for k, r, j in batch:
                add_product(1, landing(k, r, j), j, False)
        for second in (False, True):
            ranges = [half(j, second) for j in (2, 1, 0)]
            rows = sum(span.size for span in ranges)
            arrived(xbuf.at[1, 0, pl.ds(0, rows)], sib_sem.at[10 if second else 9])
            for j in (2, 1, 0):
                add_product(1, landing(2, 3, j), j, False, second=second)
            add_state(ranges, first=not second)
        chain_wait(4)

    @pl.when(is_foreign)
    def _():
        quarter = z % 4
        opposite = (z + 2) % 4

        other = flip1(x)
        mine_first = (x, 3 - x, other, 3 - other)
        theirs_first = (other, 3 - other, x, 3 - x)

        from_below, from_above, early, late = 4, 5, 6, 7

        def direct(row, i, role):
            t = row * 4 + theirs_first[i]
            rows = weight_rows(t)
            for n, src in enumerate((wk_hbm, wv_hbm)):
                remote(src.at[rows], weights.at[n, rows], w_send, w_sem.at[role], partner).start()

        def pass_weights(t, step, semaphore, role):
            ref = weights.at[:, weight_rows(t)]
            remote(ref, ref, semaphore, w_sem.at[role], along_z(step)).start()

        def exchange(j):
            remote(x_hbm.at[piece(j)], xbuf.at[0, 0, piece(j)], x_send, mine_sem.at[0, j], partner).start()

        def send_messages(messages):
            for k, r, j in messages:
                if (k, r) != (2, 3):
                    send_on(turn(r, j), j, [(j + k) % N])
                    continue
                for second in (False, True):
                    remote(
                        xbuf.at[0, turn(r, j), half(j, second)], xbuf.at[0, landing(k, r, j), half(j, second)],
                        link_send, last_sem.at[j] if second else mine_sem.at[landing(k, r, j), j],
                        links[(j + k) % N],
                    ).start()

        def own_piece(j):
            mine_arrived(0, j)
            send_messages(OWN_SENDS[j])
            to_sibling(0, j, 0)

        waiting = list(FOREIGN_ORDER)
        ready = []

        def receive(*expected):
            k, r, j = waiting.pop(0)
            assert (k, r, j) == expected
            mask = landing(k, r, j)
            ready.append((mask, j))
            if (k, r) == (2, 3):
                return
            mine_arrived(mask, j)
            send_messages(SENDS.get((k, r, j), []))
            to_sibling(mask, j, 1 + [(k, r, j) in batch for batch in BATCHES].index(True))

        def receive_half(j, second):
            ref = xbuf.at[0, landing(2, 3, j), half(j, second)]
            arrived(ref, last_sem.at[j] if second else mine_sem.at[landing(2, 3, j), j])
            remote(ref, xbuf.at[1, landing(2, 3, j), half(j, second)], sib_send, sib_sem.at[10 if second else 9], sibling).start()

        def foreign_product(count):
            for _ in range(count):
                mask, j = ready.pop(0)
                add_product(0, mask, j, False)

        def native_product(slot):
            got = native_slot(slot)
            sib_arrived(1 + slot, [j for j, _, _, _ in got])
            for j, _, mask, _ in got:
                add_product(1, mask, j, True)

        def weights_arrived(role, columns):
            arrived(weights.at[:, pl.ds(0, columns * FEAT)], w_sem.at[role])

        def own_weights(i):
            t = quarter * 4 + mine_first[i]
            weights_arrived(i, 1)
            pass_weights(t, 1, wz_send, (from_below, early, late, late)[i])
            pass_weights(t, -1, wz_send, (early, from_above, late, late)[i])

        def pass_on(step):
            t = (z + step) % 4 * 4 + mine_first[1 if step == 1 else 0]
            weights_arrived(from_above if step == 1 else from_below, 1)
            pass_weights(t, -step, wzz_send, early)

        direct(quarter, 0, 0)
        direct(quarter, 1, 1)
        start_smalls()
        fill_mini()
        for j in range(N):
            exchange(j)
        remote(mini_own, mini_got, mini_send, mini_sem, partner).start()
        direct(quarter, 2, 2)
        direct(quarter, 3, 3)
        direct(opposite, 2, late)
        direct(opposite, 3, late)
        chain_signal(0)
        own_weights(0)
        own_weights(1)
        chain_wait(0)
        chain_signal(1)
        own_piece(0)
        pass_on(-1)
        own_piece(1)
        pass_on(1)
        own_piece(2)
        chain_wait(1)
        chain_signal(2)
        arrived(mini_got, mini_sem)
        tables(mini_got)
        receive(0, 0, 0)
        own_weights(2)
        receive(0, 0, 1)
        weights_arrived(early, 4)
        receive(1, 0, 2)
        receive(0, 0, 2)
        chain_wait(2)
        chain_signal(3)
        sib_arrived(0, range(N))
        for j in range(N):
            add_product(1, 0, j, True, first=True)
        native_product(0)
        native_product(1)
        own_weights(3)
        receive(1, 0, 0)
        receive(2, 0, 1)
        receive(1, 0, 1)
        native_product(2)
        native_product(3)
        native_product(4)
        receive(1, 1, 0)
        receive(2, 1, 1)
        receive(1, 1, 1)
        native_product(5)
        native_product(6)
        chain_wait(3)
        chain_signal(4)
        receive(2, 0, 2)
        receive(1, 1, 2)
        receive(2, 0, 0)
        receive(2, 1, 2)
        weights_arrived(late, 6)
        for j in range(N):
            add_product(0, 0, j, False)
        foreign_product(4)
        receive(2, 2, 1)
        receive(2, 1, 0)
        foreign_product(6)
        receive(2, 2, 2)
        receive(2, 2, 0)
        foreign_product(4)
        receive(2, 3, 2)
        receive(2, 3, 1)
        receive(2, 3, 0)
        for j in (2, 1, 0):
            receive_half(j, False)
        foreign_product(4)
        for j in (2, 1, 0):
            receive_half(j, True)
        foreign_product(3)
        add_state([pl.ds(0, TOK)], first=True)
        chain_wait(4)

    states = [state[0], state[1]]
    prompt = z // 8
    reads = []
    for h in range(2):
        rows = pl.ds(2 + 2 * h, 2)
        both = jnp.dot(
            mini_got[rows, :], states[h], precision=lax.Precision.HIGHEST, preferred_element_type=jnp.float32
        )
        reads.append(jnp.where(prompt == 0, both[0:1], both[1:2]))
    reads = jnp.concatenate(reads + [jnp.zeros((6, 128), jnp.float32)], axis=0)
    top = lax.broadcasted_iota(jnp.int32, (8, 128), 0) < 4
    for i in range(16):
        a = states[0][8 * i : 8 * i + 8]
        b = states[1][8 * i : 8 * i + 8]
        for n, share in enumerate((
            jnp.where(top, a, pltpu.roll(b, 4, axis=0)), jnp.where(top, pltpu.roll(a, 4, axis=0), b)
        )):
            send_share[2 * i + n] = jnp.concatenate([share, reads], axis=0).astype(jnp.bfloat16)

    target_tp = jnp.where(is_native, tp, partner_tp)

    sent = pl.ds(0, ROWS)

    def tail(step, other):
        target = (z + step + Z) % Z * 2 + (1 - core if other else core)
        device = (target, target_tp)
        remote(
            send_share.at[target, sent], got_share.at[block, sent], tail_send, tail_recv, device
        ).start()

    far = [8]
    for s in range(7, 0, -1):
        far += [s, -s]
    for step in far:
        for other in (False, True):
            tail(step, other)
    tail(0, True)

    @pl.when(is_native)
    def _():
        pltpu.make_async_copy(send_share.at[sp, sent], got_share.at[block, sent], tail_recv).start()

    @pl.when(is_foreign)
    def _():
        tail(0, False)

    queries = query[...].astype(jnp.float32)
    dots = queries * key_new[...].astype(jnp.float32)
    news = value_new[...].astype(jnp.float32)
    own_terms = [
        jnp.sum(dots[:, h * 128 : h * 128 + 128], axis=1, keepdims=True) * news[:, h * 128 : h * 128 + 128]
        for h in range(2)
    ]

    arrived(got_share.at[:, sent], tail_recv)
    carried = [jnp.sum(got_share[16 * s : 16 * s + 16, 8:10, :].astype(jnp.float32), axis=0) for s in range(2)]
    for h in range(2):
        scaled = jnp.exp(mini_own[h : h + 1, :])
        rows = jnp.concatenate([carried[0][h : h + 1], carried[1][h : h + 1]], axis=0)
        mixed = scaled * rows + own_terms[h]
        normed = mixed * lax.rsqrt(jnp.mean(mixed * mixed, axis=1, keepdims=True) + 1e-06)
        read_out[:, h * 128 : h * 128 + 128] = normed * gain[:, h * 128 : h * 128 + 128]
    for s in range(2):
        total = jnp.zeros((8, 128), jnp.float32)
        for i in range(16):
            total = total + got_share[16 * s + i, 0:8, :].astype(jnp.float32)
        state_out[s] = total

    arrived(xbuf.at[0, pl.ds(0, 7)], link_send)
    arrived(xbuf.at[0], sib_send)

    @pl.when(is_native)
    def _():
        arrived(got_share.at[pl.ds(0, 31), sent], tail_send)

    @pl.when(is_foreign)
    def _():
        arrived(got_share.at[:, sent], tail_send)
        arrived(xbuf.at[0, 0], x_send)
        arrived(mini_own, mini_send)
        arrived(weights.at[:, pl.ds(0, 1536)], w_send)
        arrived(weights.at[0], wz_send)
        arrived(weights.at[0, pl.ds(0, 1024)], wzz_send)


def round_results(state, read, state_out, read_out):
    state_out[...] = state[...].astype(jnp.bfloat16)
    read_out[...] = read[...].astype(jnp.bfloat16)


def on_device(
    layer_input, key_weight, value_weight, decay_exponent, query_new, key_new, value_new, norm_gain
):
    inverse = (1.0 / 10000.0 ** (np.arange(64) / 63.0)).astype(np.float32)
    inverse = jnp.asarray(np.concatenate([inverse, inverse])[None, :])
    vmem = pl.BlockSpec(memory_space=pltpu.VMEM)
    anywhere = pl.BlockSpec(memory_space=pl.ANY)
    dma = pltpu.SemaphoreType.DMA
    state, read = pl.pallas_call(
        kernel,
        name="gather_project_reduce",
        out_shape=(
            pltpu.VMEM((2, 8, 128), jnp.float32),
            pltpu.VMEM((2, 256), jnp.float32),
        ),
        in_specs=[
            anywhere, anywhere, anywhere, anywhere, anywhere, anywhere, anywhere, anywhere, anywhere,
        ],
        out_specs=(vmem, vmem),
        scratch_shapes=[
            pltpu.VMEM((1, 2), jnp.float32),
            pltpu.VMEM((2, 256), jnp.bfloat16),
            pltpu.VMEM((2, 256), jnp.bfloat16),
            pltpu.VMEM((2, 256), jnp.bfloat16),
            pltpu.VMEM((1, 256), jnp.float32),
            pltpu.VMEM((1, 128), jnp.float32),
            pltpu.VMEM((2, 8, TOK, FEAT), jnp.bfloat16),
            pltpu.VMEM((2, 4096, 256), jnp.bfloat16),
            pltpu.VMEM((2, TOK, 256), jnp.float32),
            pltpu.VMEM((2, 128, 128), jnp.float32),
            pltpu.VMEM((TOK, 128), jnp.float32),
            pltpu.VMEM((TOK, 128), jnp.float32),
            pltpu.VMEM((2, TOK, 128), jnp.float32),
            pltpu.VMEM((8, 128), jnp.float32),
            pltpu.VMEM((8, 128), jnp.float32),
            pltpu.VMEM((SP, 16, 128), jnp.bfloat16),
            pltpu.VMEM((SP, 16, 128), jnp.bfloat16),
            dma((6,)), dma((8, N)), dma((N,)), dma((11,)), dma((8,)), dma((2,)), dma,
            dma, dma, dma, dma, dma, dma, dma,
            dma, dma,
            pltpu.SemaphoreType.REGULAR((5,)),
        ],
        compiler_params=pltpu.CompilerParams(collective_id=0, has_side_effects=True),
    )(
        decay_exponent[None, :], layer_input, key_weight, value_weight,
        query_new, key_new, value_new, norm_gain[None, :], inverse,
    )
    in_vmem = [pltpu.with_memory_space_constraint(result, pltpu.VMEM) for result in (state, read)]
    state, read = pl.pallas_call(
        round_results,
        name="round_results",
        out_shape=(
            jax.ShapeDtypeStruct((2, 8, 128), jnp.bfloat16),
            jax.ShapeDtypeStruct((2, 256), jnp.bfloat16),
        ),
        in_specs=[vmem, vmem],
        out_specs=(vmem, vmem),
    )(*in_vmem)
    return (state.reshape(2, 2, 4, 128), read)


def solution(mesh):
    in_specs = (
        P("sp", "tp"), P(None, "tp"), P(None, "tp"), P("tp"),
        P(None, "tp"), P(None, "tp"), P(None, "tp"), P("tp"),
    )
    out_specs = (P(None, "tp", "sp", None), P(None, "tp"))
    return jax.shard_map(
        on_device, mesh=mesh, in_specs=in_specs, out_specs=out_specs, check_vma=False
    )
```

```python
import jax
import jax.numpy as jnp
import numpy as np
from jax import lax
from jax.experimental import pallas as pl
from jax.experimental.pallas import tpu as pltpu
from jax.sharding import PartitionSpec as P

MESH = pl.DeviceIdType.MESH
N = 3
TOK = 1024
FEAT = 256
STARTS = (0, 336, 672, 1024)
SP = 32
Z = 16

NATIVE_ORDER = [(0, 0), (1, 0), (2, 0), (1, 1), (2, 1), (2, 2), (2, 3)]
FOREIGN_ORDER = [
    (0, 0, 0), (0, 0, 1), (1, 0, 2), (0, 0, 2), (1, 0, 0), (2, 0, 1), (1, 0, 1), (1, 1, 0), (2, 1, 1), (1, 1, 1),
    (2, 0, 2), (1, 1, 2), (2, 0, 0), (2, 1, 2), (2, 2, 1), (2, 1, 0), (2, 2, 2), (2, 2, 0), (2, 3, 2), (2, 3, 1),
    (2, 3, 0),
]
BATCHES = []
for _size in (2, 2, 3, 3, 2, 2, 2, 2, 3):
    _first = sum(len(batch) for batch in BATCHES)
    BATCHES.append(FOREIGN_ORDER[_first : _first + _size])
OWN_SENDS = [
    [(0, 0, 0)],
    [(0, 0, 1), (1, 0, 0)],
    [(0, 0, 2), (1, 0, 1), (1, 0, 2), (2, 0, 1)],
]
SENDS = {
    (0, 0, 0): [(1, 1, 0), (2, 0, 2)],
    (0, 0, 1): [(1, 1, 1), (2, 0, 0), (2, 1, 1), (2, 1, 0)],
    (0, 0, 2): [(1, 1, 2), (2, 1, 2)],
}
for _j in range(N):
    SENDS[1, 0, _j] = [(2, 2, _j)]
    SENDS[1, 1, _j] = [(2, 3, _j)]


def turn(mask, j):
    return ((mask << j) | (mask >> (N - j))) & (2**N - 1)


def piece(j):
    return pl.ds(STARTS[j], STARTS[j + 1] - STARTS[j])


HALF = 176
ROWS = 10


def half(j, second):
    size = STARTS[j + 1] - STARTS[j]
    return pl.ds(STARTS[j] + HALF, size - HALF) if second else pl.ds(STARTS[j], HALF)


def landing(k, r, j):
    return turn(r, j) | (1 << (j + k) % N)


def native_slot(slot):
    k, r = NATIVE_ORDER[slot]
    out = []
    for d in range(N):
        j = (d - k) % N
        sent = r | (1 << k)
        onward = [(j + kk) % N for kk, rr in NATIVE_ORDER if rr == sent]
        out.append((j, turn(r, j), landing(k, r, j), onward))
    return out


def flip1(v):
    return v + 1 - 2 * (v % 2)


def cos_sin(position, inverse):
    angle = position * inverse
    lane = lax.broadcasted_iota(jnp.int32, angle.shape, 1)
    quarter = jnp.floor(angle * 0.6366197723675814 + 0.5)
    rest = ((angle - quarter * 1.5703125) - quarter * 4.837512969970703125e-4) - quarter * 7.54978995489188e-8
    turns = quarter.astype(jnp.int32) - jnp.where(lane >= 64, 1, 0)
    turns = jnp.bitwise_and(turns, 3)
    square = rest * rest
    sine = rest + rest * square * (-1.6666654611e-1 + square * (8.3321608736e-3 - square * 1.9515295891e-4))
    cosine = 1.0 - 0.5 * square + square * square * (
        4.166664568298827e-2 + square * (-1.388731625493765e-3 + square * 2.443315711809948e-5)
    )
    value = jnp.where(jnp.bitwise_and(turns, 1) == 1, sine, cosine)
    negative = jnp.logical_or(turns == 1, turns == 2)
    return jnp.where(negative, -value, value)


def kernel(
    decay_hbm, x_hbm, wk_hbm, wv_hbm, query_hbm, key_hbm, value_hbm, gain_hbm, inverse_hbm,
    state_out, read_out,
    decay, query, key_new, value_new, gain, inverse,
    xbuf, weights, acc, state, cosine, sine, weight, mini_own, mini_got, send_share, got_share,
    small_sem, mine_sem, last_sem, sib_sem, w_sem, wl_sem, mini_sem,
    link_send, sib_send, x_send, w_send, wz_send, wzz_send, mini_send,
    tail_send, tail_recv, chain,
):
    sp = lax.axis_index("sp")
    tp = lax.axis_index("tp")
    z, core = sp // 2, sp % 2
    y, x = tp // 4, tp % 4
    group = 1 - (x + 1) // 2 % 2
    block = z * 2 + group
    links = [
        (sp, y * 4 + 3 - x),
        (sp, flip1(y) * 4 + x),
        (sp, (3 - y) * 4 + x),
    ]
    sibling = (z * 2 + 1 - core, tp)
    partner_tp = y * 4 + flip1(x)
    partner = (z * 2 + 1 - core, partner_tp)

    def along_z(step):
        return ((z + step + Z) % Z * 2 + core, tp)

    def signal(semaphore, device):
        pl.semaphore_signal(semaphore, inc=1, device_id=device, device_id_type=MESH)

    def remote(src, dst, send, recv, device):
        return pltpu.make_async_remote_copy(
            src_ref=src, dst_ref=dst, send_sem=send, recv_sem=recv, device_id=device, device_id_type=MESH
        )

    def arrived(ref, semaphore):
        pltpu.make_async_copy(ref, ref, semaphore).wait()

    is_native = core == group
    is_foreign = core != group

    barrier = pltpu.get_barrier_semaphore()
    near = links + [sibling, partner, along_z(1), along_z(-1)]
    for device in near:
        signal(barrier, device)

    @pl.when(is_native)
    def _():
        for j in range(N):
            pltpu.make_async_copy(x_hbm.at[piece(j)], xbuf.at[0, 0, piece(j)], mine_sem.at[0, j]).start()

    smalls = [
        pltpu.make_async_copy(src, dst, small_sem.at[i])
        for i, (src, dst) in enumerate((
            (decay_hbm, decay), (query_hbm, query), (key_hbm, key_new), (value_hbm, value_new),
            (gain_hbm, gain), (inverse_hbm, inverse),
        ))
    ]
    pl.semaphore_wait(barrier, len(near))

    def start_smalls():
        for copy in smalls:
            copy.start()

    def fill_mini():
        for copy in smalls:
            copy.wait()
        for h in range(2):
            mini_own[h : h + 1, :] = jnp.broadcast_to(decay[:, h : h + 1], (1, 128))
            mini_own[2 + 2 * h : 4 + 2 * h, :] = query[:, h * 128 : h * 128 + 128].astype(jnp.float32)

    steps = [
        [sibling, partner, along_z(1), along_z(-1)],
        [along_z(2), along_z(-2)],
        [sibling],
        [along_z(3), along_z(-3)],
        [along_z(6), along_z(-6)],
    ]

    def chain_signal(n):
        for device in steps[n]:
            signal(chain.at[n], device)

    def chain_wait(n):
        pl.semaphore_wait(chain.at[n], len(steps[n]))

    def send_on(mask, j, over):
        for d in over:
            remote(
                xbuf.at[0, mask, piece(j)], xbuf.at[0, mask | (1 << d), piece(j)],
                link_send, mine_sem.at[mask | (1 << d), j], links[d],
            ).start()

    def to_sibling(mask, j, group):
        remote(
            xbuf.at[0, mask, piece(j)], xbuf.at[1, mask, piece(j)], sib_send, sib_sem.at[group], sibling
        ).start()

    def column_of(mask, native_part):
        b = [mask // 2**i % 2 for i in range(N)]
        cx = x + b[0] * (3 - 2 * x)
        cy = y + b[1] * (1 - 2 * (y % 2))
        cy = cy + b[2] * (3 - 2 * cy)
        return cy * 4 + (cx if native_part else flip1(cx))

    def weight_rows(t):
        return pl.ds(pl.multiple_of(t * FEAT, FEAT), FEAT)

    def add_product(part, mask, j, native_part, first=False, second=None):
        wrows = weight_rows(column_of(mask, native_part))
        rows = piece(j) if second is None else half(j, second)
        block_x = xbuf[part, mask, rows, :]
        for i in range(2):
            product = jnp.dot(block_x, weights[i, wrows, :], preferred_element_type=jnp.float32)
            if first:
                acc[i, rows, :] = product
            else:
                acc[i, rows, :] += product

    def add_state(ranges, first=False):
        for h in range(2):
            cols = pl.ds(h * 128, 128)
            total = None if first else state[h]
            for rows in ranges:
                k = acc[0, rows, cols]
                keys = (k * cosine[rows, :] + pltpu.roll(k, 64, axis=1) * sine[rows, :]).astype(jnp.bfloat16)
                weighted = (keys.astype(jnp.float32) * weight[h, rows, :]).astype(jnp.bfloat16)
                values = acc[1, rows, cols].astype(jnp.bfloat16)
                product = lax.dot_general(
                    weighted, values, (((0,), (0,)), ((), ())), preferred_element_type=jnp.float32
                )
                total = product if total is None else total + product
            state[h] = total

    def mine_arrived(mask, j):
        arrived(xbuf.at[0, mask, piece(j)], mine_sem.at[mask, j])

    def sib_arrived(group, pieces):
        rows = sum(STARTS[j + 1] - STARTS[j] for j in pieces)
        arrived(xbuf.at[1, 0, pl.ds(0, rows)], sib_sem.at[group])

    def tables(mini):
        @pl.loop(0, 4)
        def _(c):
            rows = pl.ds(pl.multiple_of(c * 256, 256), 256)
            first = (block % 16) * TOK + c * 256
            position = (lax.broadcasted_iota(jnp.int32, (256, 128), 0) + first).astype(jnp.float32)
            table = cos_sin(position, inverse[...]) * 128 ** (-0.5)
            swapped = pltpu.roll(table, 64, axis=1)
            low = lax.broadcasted_iota(jnp.int32, (256, 128), 1) < 64
            cosine[rows, :] = jnp.where(low, table, swapped)
            sine[rows, :] = jnp.where(low, -swapped, table)
            distance = 16384 - 1.0 - position
            for h in range(2):
                weight[h, rows, :] = jnp.exp(mini[h : h + 1, :] * distance)

    @pl.when(is_native)
    def _():
        for j in range(N):
            mine_arrived(0, j)
        for slot in range(3):
            for d in range(N):
                send_on(0, (d - slot) % N, [d])
        start_smalls()
        pltpu.make_async_copy(wk_hbm, weights.at[0], wl_sem.at[0]).start()
        pltpu.make_async_copy(wv_hbm, weights.at[1], wl_sem.at[1]).start()
        for j in range(N):
            to_sibling(0, j, 0)
        chain_signal(0)
        fill_mini()
        mini_got[...] = mini_own[...]
        tables(mini_got)
        arrived(weights.at[0], wl_sem.at[0])
        arrived(weights.at[1], wl_sem.at[1])
        for j in range(N):
            add_product(0, 0, j, True, first=True)
        for slot in range(7):
            got = native_slot(slot)
            for j, _, mask, onward in got:
                mine_arrived(mask, j)
                send_on(mask, j, onward)
                to_sibling(mask, j, 1 + slot)
            if slot in (1, 3, 5):
                chain_wait(slot // 2)
                chain_signal(slot // 2 + 1)
            for j, _, mask, _ in got:
                add_product(0, mask, j, True)
        sib_arrived(0, range(N))
        for j in range(N):
            add_product(1, 0, j, False)
        for n, batch in enumerate(BATCHES):
            if n == 4:
                chain_wait(3)
                chain_signal(4)
            if n == 8:
                continue
            sib_arrived(1 + n, [j for _, _, j in batch])
            for k, r, j in batch:
                add_product(1, landing(k, r, j), j, False)
        for second in (False, True):
            ranges = [half(j, second) for j in (2, 1, 0)]
            rows = sum(span.size for span in ranges)
            arrived(xbuf.at[1, 0, pl.ds(0, rows)], sib_sem.at[10 if second else 9])
            for j in (2, 1, 0):
                add_product(1, landing(2, 3, j), j, False, second=second)
            add_state(ranges, first=not second)
        chain_wait(4)

    @pl.when(is_foreign)
    def _():
        quarter = z % 4
        opposite = (z + 2) % 4

        other = flip1(x)
        mine_first = (x, 3 - x, other, 3 - other)
        theirs_first = (other, 3 - other, x, 3 - x)

        from_below, from_above, early, late = 4, 5, 6, 7

        def direct(row, i, role):
            t = row * 4 + theirs_first[i]
            rows = weight_rows(t)
            for n, src in enumerate((wk_hbm, wv_hbm)):
                remote(src.at[rows], weights.at[n, rows], w_send, w_sem.at[role], partner).start()

        def pass_weights(t, step, semaphore, role):
            ref = weights.at[:, weight_rows(t)]
            remote(ref, ref, semaphore, w_sem.at[role], along_z(step)).start()

        def exchange(j):
            remote(x_hbm.at[piece(j)], xbuf.at[0, 0, piece(j)], x_send, mine_sem.at[0, j], partner).start()

        def send_messages(messages):
            for k, r, j in messages:
                if (k, r) != (2, 3):
                    send_on(turn(r, j), j, [(j + k) % N])
                    continue
                for second in (False, True):
                    remote(
                        xbuf.at[0, turn(r, j), half(j, second)], xbuf.at[0, landing(k, r, j), half(j, second)],
                        link_send, last_sem.at[j] if second else mine_sem.at[landing(k, r, j), j],
                        links[(j + k) % N],
                    ).start()

        def own_piece(j):
            mine_arrived(0, j)
            send_messages(OWN_SENDS[j])
            to_sibling(0, j, 0)

        waiting = list(FOREIGN_ORDER)
        ready = []

        def receive(*expected):
            k, r, j = waiting.pop(0)
            assert (k, r, j) == expected
            mask = landing(k, r, j)
            ready.append((mask, j))
            if (k, r) == (2, 3):
                return
            mine_arrived(mask, j)
            send_messages(SENDS.get((k, r, j), []))
            to_sibling(mask, j, 1 + [(k, r, j) in batch for batch in BATCHES].index(True))

        def receive_half(j, second):
            ref = xbuf.at[0, landing(2, 3, j), half(j, second)]
            arrived(ref, last_sem.at[j] if second else mine_sem.at[landing(2, 3, j), j])
            remote(ref, xbuf.at[1, landing(2, 3, j), half(j, second)], sib_send, sib_sem.at[10 if second else 9], sibling).start()

        def foreign_product(count):
            for _ in range(count):
                mask, j = ready.pop(0)
                add_product(0, mask, j, False)

        def native_product(slot):
            got = native_slot(slot)
            sib_arrived(1 + slot, [j for j, _, _, _ in got])
            for j, _, mask, _ in got:
                add_product(1, mask, j, True)

        def weights_arrived(role, columns):
            arrived(weights.at[:, pl.ds(0, columns * FEAT)], w_sem.at[role])

        def own_weights(i):
            t = quarter * 4 + mine_first[i]
            weights_arrived(i, 1)
            pass_weights(t, 1, wz_send, (from_below, early, late, late)[i])
            pass_weights(t, -1, wz_send, (early, from_above, late, late)[i])

        def pass_on(step):
            t = (z + step) % 4 * 4 + mine_first[1 if step == 1 else 0]
            weights_arrived(from_above if step == 1 else from_below, 1)
            pass_weights(t, -step, wzz_send, early)

        direct(quarter, 0, 0)
        direct(quarter, 1, 1)
        start_smalls()
        fill_mini()
        for j in range(N):
            exchange(j)
        remote(mini_own, mini_got, mini_send, mini_sem, partner).start()
        direct(quarter, 2, 2)
        direct(quarter, 3, 3)
        direct(opposite, 2, late)
        direct(opposite, 3, late)
        chain_signal(0)
        own_weights(0)
        own_weights(1)
        chain_wait(0)
        chain_signal(1)
        own_piece(0)
        pass_on(-1)
        own_piece(1)
        pass_on(1)
        own_piece(2)
        chain_wait(1)
        chain_signal(2)
        arrived(mini_got, mini_sem)
        tables(mini_got)
        receive(0, 0, 0)
        own_weights(2)
        receive(0, 0, 1)
        weights_arrived(early, 4)
        receive(1, 0, 2)
        receive(0, 0, 2)
        chain_wait(2)
        chain_signal(3)
        sib_arrived(0, range(N))
        for j in range(N):
            add_product(1, 0, j, True, first=True)
        native_product(0)
        native_product(1)
        own_weights(3)
        receive(1, 0, 0)
        receive(2, 0, 1)
        receive(1, 0, 1)
        native_product(2)
        native_product(3)
        native_product(4)
        receive(1, 1, 0)
        receive(2, 1, 1)
        receive(1, 1, 1)
        native_product(5)
        native_product(6)
        chain_wait(3)
        chain_signal(4)
        receive(2, 0, 2)
        receive(1, 1, 2)
        receive(2, 0, 0)
        receive(2, 1, 2)
        weights_arrived(late, 6)
        for j in range(N):
            add_product(0, 0, j, False)
        foreign_product(4)
        receive(2, 2, 1)
        receive(2, 1, 0)
        foreign_product(6)
        receive(2, 2, 2)
        receive(2, 2, 0)
        foreign_product(4)
        receive(2, 3, 2)
        receive(2, 3, 1)
        receive(2, 3, 0)
        for j in (2, 1, 0):
            receive_half(j, False)
        foreign_product(4)
        for j in (2, 1, 0):
            receive_half(j, True)
        foreign_product(3)
        add_state([pl.ds(0, TOK)], first=True)
        chain_wait(4)

    states = [state[0], state[1]]
    prompt = z // 8
    reads = []
    for h in range(2):
        rows = pl.ds(2 + 2 * h, 2)
        q = mini_got[rows, :].astype(jnp.bfloat16)
        high = states[h].astype(jnp.bfloat16)
        rest = states[h] - high.astype(jnp.float32)
        middle = rest.astype(jnp.bfloat16)
        low = (rest - middle.astype(jnp.float32)).astype(jnp.bfloat16)
        both = sum(jnp.dot(q, part, preferred_element_type=jnp.float32) for part in (low, middle, high))
        reads.append(jnp.where(prompt == 0, both[0:1], both[1:2]))
    reads = jnp.concatenate(reads + [jnp.zeros((6, 128), jnp.float32)], axis=0)
    top = lax.broadcasted_iota(jnp.int32, (8, 128), 0) < 4
    for i in range(16):
        a = states[0][8 * i : 8 * i + 8]
        b = states[1][8 * i : 8 * i + 8]
        for n, share in enumerate((
            jnp.where(top, a, pltpu.roll(b, 4, axis=0)), jnp.where(top, pltpu.roll(a, 4, axis=0), b)
        )):
            send_share[2 * i + n] = jnp.concatenate([share, reads], axis=0).astype(jnp.bfloat16)

    target_tp = jnp.where(is_native, tp, partner_tp)

    sent = pl.ds(0, ROWS)

    def tail(step, other):
        target = (z + step + Z) % Z * 2 + (1 - core if other else core)
        device = (target, target_tp)
        remote(
            send_share.at[target, sent], got_share.at[block, sent], tail_send, tail_recv, device
        ).start()

    far = [8]
    for s in range(7, 0, -1):
        far += [s, -s]
    for step in far:
        for other in (False, True):
            tail(step, other)
    tail(0, True)

    @pl.when(is_native)
    def _():
        pltpu.make_async_copy(send_share.at[sp, sent], got_share.at[block, sent], tail_recv).start()

    @pl.when(is_foreign)
    def _():
        tail(0, False)

    queries = query[...].astype(jnp.float32)
    dots = queries * key_new[...].astype(jnp.float32)
    news = value_new[...].astype(jnp.float32)
    own_terms = [
        jnp.sum(dots[:, h * 128 : h * 128 + 128], axis=1, keepdims=True) * news[:, h * 128 : h * 128 + 128]
        for h in range(2)
    ]

    arrived(got_share.at[:, sent], tail_recv)
    carried = [jnp.sum(got_share[16 * s : 16 * s + 16, 8:10, :].astype(jnp.float32), axis=0) for s in range(2)]
    for h in range(2):
        scaled = jnp.exp(mini_own[h : h + 1, :])
        rows = jnp.concatenate([carried[0][h : h + 1], carried[1][h : h + 1]], axis=0)
        mixed = scaled * rows + own_terms[h]
        normed = mixed * lax.rsqrt(jnp.mean(mixed * mixed, axis=1, keepdims=True) + 1e-06)
        read_out[:, h * 128 : h * 128 + 128] = normed * gain[:, h * 128 : h * 128 + 128]
    for s in range(2):
        total = jnp.zeros((8, 128), jnp.float32)
        for i in range(16):
            total = total + got_share[16 * s + i, 0:8, :].astype(jnp.float32)
        state_out[s] = total

    arrived(xbuf.at[0, pl.ds(0, 7)], link_send)
    arrived(xbuf.at[0], sib_send)

    @pl.when(is_native)
    def _():
        arrived(got_share.at[pl.ds(0, 31), sent], tail_send)

    @pl.when(is_foreign)
    def _():
        arrived(got_share.at[:, sent], tail_send)
        arrived(xbuf.at[0, 0], x_send)
        arrived(mini_own, mini_send)
        arrived(weights.at[:, pl.ds(0, 1536)], w_send)
        arrived(weights.at[0], wz_send)
        arrived(weights.at[0, pl.ds(0, 1024)], wzz_send)


def round_results(state, read, state_out, read_out):
    state_out[...] = state[...].astype(jnp.bfloat16)
    read_out[...] = read[...].astype(jnp.bfloat16)


def on_device(
    layer_input, key_weight, value_weight, decay_exponent, query_new, key_new, value_new, norm_gain
):
    inverse = (1.0 / 10000.0 ** (np.arange(64) / 63.0)).astype(np.float32)
    inverse = jnp.asarray(np.concatenate([inverse, inverse])[None, :])
    vmem = pl.BlockSpec(memory_space=pltpu.VMEM)
    anywhere = pl.BlockSpec(memory_space=pl.ANY)
    dma = pltpu.SemaphoreType.DMA
    state, read = pl.pallas_call(
        kernel,
        name="gather_project_reduce",
        out_shape=(
            pltpu.VMEM((2, 8, 128), jnp.float32),
            pltpu.VMEM((2, 256), jnp.float32),
        ),
        in_specs=[
            anywhere, anywhere, anywhere, anywhere, anywhere, anywhere, anywhere, anywhere, anywhere,
        ],
        out_specs=(vmem, vmem),
        scratch_shapes=[
            pltpu.VMEM((1, 2), jnp.float32),
            pltpu.VMEM((2, 256), jnp.bfloat16),
            pltpu.VMEM((2, 256), jnp.bfloat16),
            pltpu.VMEM((2, 256), jnp.bfloat16),
            pltpu.VMEM((1, 256), jnp.float32),
            pltpu.VMEM((1, 128), jnp.float32),
            pltpu.VMEM((2, 8, TOK, FEAT), jnp.bfloat16),
            pltpu.VMEM((2, 4096, 256), jnp.bfloat16),
            pltpu.VMEM((2, TOK, 256), jnp.float32),
            pltpu.VMEM((2, 128, 128), jnp.float32),
            pltpu.VMEM((TOK, 128), jnp.float32),
            pltpu.VMEM((TOK, 128), jnp.float32),
            pltpu.VMEM((2, TOK, 128), jnp.float32),
            pltpu.VMEM((8, 128), jnp.float32),
            pltpu.VMEM((8, 128), jnp.float32),
            pltpu.VMEM((SP, 16, 128), jnp.bfloat16),
            pltpu.VMEM((SP, 16, 128), jnp.bfloat16),
            dma((6,)), dma((8, N)), dma((N,)), dma((11,)), dma((8,)), dma((2,)), dma,
            dma, dma, dma, dma, dma, dma, dma,
            dma, dma,
            pltpu.SemaphoreType.REGULAR((5,)),
        ],
        compiler_params=pltpu.CompilerParams(collective_id=0, has_side_effects=True),
    )(
        decay_exponent[None, :], layer_input, key_weight, value_weight,
        query_new, key_new, value_new, norm_gain[None, :], inverse,
    )
    in_vmem = [pltpu.with_memory_space_constraint(result, pltpu.VMEM) for result in (state, read)]
    state, read = pl.pallas_call(
        round_results,
        name="round_results",
        out_shape=(
            jax.ShapeDtypeStruct((2, 8, 128), jnp.bfloat16),
            jax.ShapeDtypeStruct((2, 256), jnp.bfloat16),
        ),
        in_specs=[vmem, vmem],
        out_specs=(vmem, vmem),
    )(*in_vmem)
    return (state.reshape(2, 2, 4, 128), read)


def solution(mesh):
    in_specs = (
        P("sp", "tp"), P(None, "tp"), P(None, "tp"), P("tp"),
        P(None, "tp"), P(None, "tp"), P(None, "tp"), P("tp"),
    )
    out_specs = (P(None, "tp", "sp", None), P(None, "tp"))
    return jax.shard_map(
        on_device, mesh=mesh, in_specs=in_specs, out_specs=out_specs, check_vma=False
    )
```
